256 devices in a mesh: sp: 32 (over z, x), tp: 8 (over y, core).
Axes of the slice: x: 4, y: 4, z: 8, core: 2. Of those that a mesh axis runs over, the one named last changes fastest.
Arguments:
- resid: bfloat16 [8192, 4096], P('sp'), may hold values from -6 to 6
- queries: bfloat16 [8192, 3072], P('sp', 'tp'), may hold values from -1000 to 1000
- latent: bfloat16 [8192, 512], P('sp'), may hold values from -6 to 6
- rope_key: bfloat16 [8192, 64], P('sp'), may hold values from -6 to 6
- lat_gain: float32 [512], replicated, may hold values from 0.1 to 1.9
- kv_weight: bfloat16 [512, 4096], P(None, 'tp'), may hold values from -4 to 4
- out_gain: float32 [2048], P('tp'), may hold values from 0.1 to 1.9
- out_weight: bfloat16 [2048, 4096], P('tp'), may hold values from -0.125 to 0.125
- ffn_gain: float32 [4096], replicated, may hold values from 0.1 to 1.9
- gate_weight: bfloat16 [4096, 6144], P('sp', 'tp'), may hold values from -0.09375 to 0.09375
- up_weight: bfloat16 [4096, 6144], P('sp', 'tp'), may hold values from -0.09375 to 0.09375
- down_weight: bfloat16 [6144, 4096], P('tp', 'sp'), may hold values from -0.078125 to 0.078125
Outputs:
- result: bfloat16 [8192, 4096], P(('sp', 'tp'))
The draws below stay inside these ranges and needn't reach their ends.
All inputs are finite; a program needn't handle non-finite values.
Results may differ from the reference program's by a relative error of at most 0.018.
Values may be sent and summed in bfloat16 or wider, within the bound.
A program may use at most 192 MiB of HBM per device.

```python
import math
import jax
import jax.numpy as jnp
from jax import lax

D = 4096
HEADS = 16
NOPE = 128
ROPE = 64
VDIM = 128
KV_RANK = 512
FF = 6144
TOK_DEV = 256
TOKENS = 8192
N_TP = 8


def draw_pair(key):
    base = jax.random.fold_in(key, 7)
    key_one, key_two = jax.random.split(base, 2)
    width = NOPE + ROPE
    query = jax.random.truncated_normal(key_one, -6.0, 6.0, (TOKENS, HEADS, width), jnp.float32)
    rotary = jax.random.truncated_normal(key_two, -4.0, 4.0, (TOKENS, ROPE), jnp.float32)
    return (query.reshape(TOKENS, HEADS * width), rotary)


def draw_queries(key, part):
    return draw_pair(key)[0].astype(jnp.bfloat16)


def draw_rope_key(key, part):
    return draw_pair(key)[1].astype(jnp.bfloat16)


def draw_kv_weight(key, part):
    base = jax.random.fold_in(key, 11)
    shape = (KV_RANK, HEADS, NOPE + VDIM)
    matrix = jax.random.truncated_normal(base, -6.0, 6.0, shape, jnp.float32)
    ceiling = 3.0
    factor = ceiling ** (jnp.arange(HEADS, dtype=jnp.float32) / (HEADS - 1))
    scaled = jnp.concatenate([matrix[:, :, :NOPE], matrix[:, :, NOPE:] * factor[None, :, None]], axis=-1)
    return (scaled / math.sqrt(KV_RANK)).reshape(KV_RANK, HEADS * (NOPE + VDIM)).astype(jnp.bfloat16)


def shard_levels(rng, shape, pieces, low, top_value):
    level, own = 1.0, jax.random.fold_in(rng, 6)
    for dim, shards_of in pieces:
        heights = jnp.exp(jax.random.uniform(jax.random.fold_in(own, dim), (shards_of,), jnp.float32, low / len(pieces), top_value / len(pieces)))
        level = level * jnp.repeat(heights, shape[dim] // shards_of).reshape([-1 if axis == dim else 1 for axis in range(len(shape))])
    return level


def noise(own_key, dims, scale, reach, shards=(), kind=jnp.bfloat16):
    values = scale * jax.random.normal(own_key, dims, jnp.float32)
    if shards:
        values = values * shard_levels(own_key, dims, shards, -0.22, 0.18)
    return jnp.clip(values, -reach, reach).astype(kind)


def setup_inputs(seed: int = 0) -> dict:
    streams_of = jax.random.split(jax.random.key(seed), 13)
    return {
        "resid": noise(streams_of[0], (TOKENS, D), 1.0, 6.0, ((0, 32),)),
        "queries": draw_queries(jax.random.fold_in(streams_of[12], 71), 0),
        "latent": noise(streams_of[2], (TOKENS, KV_RANK), 1.0, 6.0, ((0, 32),)),
        "rope_key": draw_rope_key(jax.random.fold_in(streams_of[12], 71), 0),
        "lat_gain": jnp.clip(1.0 + 0.18 * jax.random.normal(streams_of[4], (KV_RANK,), jnp.float32), 0.1, 1.9),
        "kv_weight": draw_kv_weight(jax.random.fold_in(streams_of[12], 71), 0),
        "out_gain": jnp.clip(1.0 + 0.18 * jax.random.normal(streams_of[6], (HEADS * VDIM,), jnp.float32), 0.1, 1.9),
        "out_weight": noise(streams_of[7], (HEADS * VDIM, D), (HEADS * VDIM) ** -0.5, 0.125, ((0, 8),)),
        "ffn_gain": jnp.clip(1.0 + 0.18 * jax.random.normal(streams_of[8], (D,), jnp.float32), 0.1, 1.9),
        "gate_weight": noise(streams_of[9], (D, FF), D ** -0.5, 0.09375, ((0, 32), (1, 8))),
        "up_weight": noise(streams_of[10], (D, FF), D ** -0.5, 0.09375, ((0, 32), (1, 8))),
        "down_weight": noise(streams_of[11], (FF, D), FF ** -0.5, 0.078125, ((0, 8), (1, 32))),
    }


EPSILON = 1e-06
THETA = 10000.0

def rotate(values, places):
    half = values.shape[-1] // 2
    inverse = THETA ** (-jnp.arange(half, dtype=jnp.float32) / half)
    angle = places[..., None] * inverse
    cosine = jnp.cos(angle)
    sine = jnp.sin(angle)
    first = values[..., :half]
    second = values[..., half:]
    return jnp.concatenate([first * cosine - second * sine, first * sine + second * cosine], axis=-1)

def norm_rows(values, gain):
    wide = values.astype(jnp.float32)
    return wide * lax.rsqrt(lax.optimization_barrier(jnp.mean(wide * wide, axis=-1, keepdims=True)) + EPSILON) * gain.astype(jnp.float32)

def round_trip(values):
    return lax.optimization_barrier(values.astype(jnp.bfloat16)).astype(jnp.float32)

def reference(resid, queries, latent, rope_key, lat_gain, kv_weight, out_gain, out_weight, ffn_gain, gate_weight, up_weight, down_weight):
    total_rows = latent.shape[0]
    positions = jnp.arange(total_rows, dtype=jnp.int32)
    places = positions.astype(jnp.float32)
    normed = norm_rows(latent, lat_gain).astype(jnp.bfloat16)
    key_value = jnp.dot(normed, kv_weight, preferred_element_type=jnp.float32).astype(jnp.bfloat16)
    key_value = key_value.reshape(total_rows, HEADS, NOPE + VDIM).astype(jnp.float32)
    key_nope = key_value[:, :, :NOPE]
    values = key_value[:, :, NOPE:]
    key_rope = round_trip(rotate(rope_key.astype(jnp.float32), places))
    query = queries.reshape(total_rows, HEADS, NOPE + ROPE)
    query_nope = query[:, :, :NOPE].astype(jnp.float32)
    query_rope = round_trip(rotate(query[:, :, NOPE:].astype(jnp.float32), places[:, None]))
    scale = 1.0 / math.sqrt(NOPE + ROPE)
    blocks = total_rows // TOK_DEV

    def attend_block(index):
        first = (index * TOK_DEV).astype(jnp.int32)
        block_nope = lax.dynamic_slice_in_dim(query_nope, first, TOK_DEV, 0)
        block_rope = lax.dynamic_slice_in_dim(query_rope, first, TOK_DEV, 0)
        scores = jnp.einsum('qhd,khd->hqk', block_nope, key_nope) + jnp.einsum('qhr,kr->hqk', block_rope, key_rope)
        scores = scores * scale
        query_index = first + jnp.arange(TOK_DEV, dtype=jnp.int32)
        allowed = (positions[None, :] <= query_index[:, None])[None]
        scores = jnp.where(allowed, scores, -jnp.inf)
        highest = lax.optimization_barrier(jnp.max(scores, axis=-1, keepdims=True))
        weights = jnp.where(allowed, jnp.exp(scores - highest), 0.0)
        totals = lax.optimization_barrier(jnp.sum(weights, axis=-1))
        mixed = jnp.einsum('hqk,khd->qhd', round_trip(weights), values)
        return (mixed / jnp.transpose(totals)[:, :, None]).astype(jnp.bfloat16)
    attended = lax.map(attend_block, jnp.arange(blocks, dtype=jnp.int32))
    attended = attended.reshape(total_rows, HEADS * VDIM)
    normed_out = norm_rows(attended, out_gain).astype(jnp.bfloat16)
    group_width = HEADS * VDIM // N_TP
    attn_sum = jnp.zeros((total_rows, D), jnp.float32)
    for group in range(N_TP):
        lower = group * group_width
        part = jnp.dot(normed_out[:, lower:lower + group_width], out_weight[lower:lower + group_width], preferred_element_type=jnp.float32)
        attn_sum = attn_sum + round_trip(part)
    middle = (resid.astype(jnp.float32) + attn_sum).astype(jnp.bfloat16)
    normed_mid = norm_rows(middle, ffn_gain).astype(jnp.bfloat16)
    gate = jnp.dot(normed_mid, gate_weight, preferred_element_type=jnp.float32)
    upward = jnp.dot(normed_mid, up_weight, preferred_element_type=jnp.float32)
    hidden = (jax.nn.silu(gate) * upward).astype(jnp.bfloat16)
    group_units = FF // N_TP
    ffn_sum = jnp.zeros((total_rows, D), jnp.float32)
    for group in range(N_TP):
        lower = group * group_units
        part = jnp.dot(hidden[:, lower:lower + group_units], down_weight[lower:lower + group_units], preferred_element_type=jnp.float32)
        ffn_sum = ffn_sum + round_trip(part)
    return (middle.astype(jnp.float32) + ffn_sum).astype(jnp.bfloat16)
```

```python
import functools
import math

import jax
import jax.numpy as jnp
from jax import lax
from jax.experimental import pallas as pl
from jax.experimental.pallas import tpu as pltpu
from jax.sharding import PartitionSpec as P

HEADS = 16
NOPE = 128
ROPE = 64
VDIM = 128
NX = 4
NC = 2
CHUNKS = 2

EPSILON = 1e-06
THETA = 10000.0
LOWEST = -1e30
MESH = pl.DeviceIdType.MESH
F32 = jnp.float32
BF16 = jnp.bfloat16


def turned_gather(arrays, axis, dims):
    turned = [jnp.moveaxis(a, dim, 0) for a, dim in zip(arrays, dims)]
    both = jnp.concatenate([t.reshape(len(t), -1) for t in turned], axis=1)
    filled, at, outs = (lax.all_gather(both, axis, axis=0, tiled=True), 0, [])
    for t, dim in zip(turned, dims):
        slab = filled[:, at : at + t[0].size].reshape(-1, *t.shape[1:])
        outs.append(jnp.moveaxis(slab, 0, dim))
        at += t[0].size
    return tuple(outs)


def sent_to_all(array, axis):
    copies = jnp.broadcast_to(array, (lax.axis_size(axis), *array.shape))
    return lax.all_to_all(copies, axis, split_axis=0, concat_axis=0, tiled=True)


def over_copies(array, axis):
    return sent_to_all(array, axis).sum(axis=0)


def cut_along(array, dim, devices):
    shape = array.shape
    parts = array.reshape(*shape[:dim], devices, shape[dim] // devices, *shape[dim + 1 :])
    return jnp.moveaxis(parts, dim, 0)


def summed_on_arrival(array, axis, dim):
    parts = cut_along(array, dim, lax.axis_size(axis))
    arrived = lax.all_to_all(parts, axis, split_axis=0, concat_axis=0, tiled=True)
    return arrived.astype(jnp.float32).sum(axis=0)


def laid_out(parts, dim):
    shape = list(parts.shape[1:])
    shape[dim] *= parts.shape[0]
    return jnp.moveaxis(parts, 0, dim).reshape(shape)


def gather_directly(array, axis, dim):
    parts = sent_to_all(array, axis)
    return laid_out(parts, dim)


def norm_rows(values, gain):
    wide = values.astype(jnp.float32)
    return wide * lax.rsqrt(jnp.mean(wide * wide, axis=-1, keepdims=True) + EPSILON) * gain


def nt_dot(a, b):
    return lax.dot_general(a, b, (((1,), (1,)), ((), ())), preferred_element_type=F32)


def attention_kernel(
    nz,
    lat_ref,
    q_ref,
    wk_ref,
    wv_ref,
    out_ref,
    latbuf,
    qbuf,
    acc,
    stat_m,
    stat_l,
    osend,
    orecv,
    ssend,
    srecv,
    local_sem,
    ring_send,
    ring_recv,
    pair_send,
    pair_recv,
    q_send,
    q_recv,
    o_send,
    o_recv,
    s_send,
    s_recv,
):
    sp = lax.axis_index("sp")
    tp = lax.axis_index("tp")
    z, x = sp // NX, lax.rem(sp, NX)
    core = lax.rem(tp, NC)
    up = lax.rem(z + 1, nz) * NX + x
    down = lax.rem(z + nz - 1, nz) * NX + x
    partner = tp + 1 - 2 * core
    rows = q_ref.shape[1]
    far = nz // 2
    factor = (1.0 / math.sqrt(NOPE + ROPE)) * math.log2(math.e)

    barrier = pltpu.get_barrier_semaphore()
    peers = [(up, tp), (down, tp), (sp, partner)]
    for k in range(1, NX):
        peers.append((z * NX + lax.rem(x + k, NX), tp))
    for peer in peers:
        pl.semaphore_signal(barrier, inc=1, device_id=peer, device_id_type=MESH)
    pl.semaphore_wait(barrier, len(peers))

    def ring(src_slot, dst_slot, chunk, device):
        src = lat_ref.at[core, chunk] if src_slot is None else latbuf.at[src_slot, core, chunk]
        return pltpu.make_async_remote_copy(
            src_ref=src,
            dst_ref=latbuf.at[dst_slot, core, chunk],
            send_sem=ring_send.at[dst_slot, chunk],
            recv_sem=ring_recv.at[dst_slot, chunk],
            device_id=(device, tp),
            device_id_type=MESH,
        )

    def pair(slot, chunk):
        return pltpu.make_async_remote_copy(
            src_ref=latbuf.at[slot, core, chunk],
            dst_ref=latbuf.at[slot, core, chunk],
            send_sem=pair_send.at[slot, chunk],
            recv_sem=pair_recv.at[slot, chunk],
            device_id=(sp, partner),
            device_id_type=MESH,
        )

    def pair_in(slot, chunk):
        return pltpu.make_async_remote_copy(
            src_ref=latbuf.at[slot, 1 - core, chunk],
            dst_ref=latbuf.at[slot, 1 - core, chunk],
            send_sem=pair_send.at[slot, chunk],
            recv_sem=pair_recv.at[slot, chunk],
            device_id=(sp, partner),
            device_id_type=MESH,
        )

    def q_copy(k):
        return pltpu.make_async_remote_copy(
            src_ref=q_ref,
            dst_ref=qbuf.at[x],
            send_sem=q_send.at[k],
            recv_sem=q_recv.at[k],
            device_id=(z * NX + lax.rem(x + k, NX), tp),
            device_id_type=MESH,
        )

    for chunk in range(CHUNKS):
        ring(None, 1, chunk, up).start()
        ring(None, far + 1, chunk, down).start()
    own_lat = pltpu.make_async_copy(lat_ref, latbuf.at[0], local_sem.at[0])
    own_q = pltpu.make_async_copy(q_ref, qbuf.at[x], local_sem.at[1])
    own_lat.start()
    own_q.start()
    for k in range(1, NX):
        q_copy(k).start()

    stat_m[...] = jnp.full(stat_m.shape, LOWEST, F32)
    stat_l[...] = jnp.zeros(stat_l.shape, F32)
    acc[...] = jnp.zeros(acc.shape, F32)

    def piece(slot, diagonal):
        lat = latbuf[slot].reshape(rows, lat_ref.shape[-1])
        wide = wk_ref.shape[0]
        compressed, key_rot = lat[:, :wide], lat[:, wide:]
        keys = jnp.dot(compressed, wk_ref[...], preferred_element_type=F32).astype(BF16)
        values = nt_dot(wv_ref[...], compressed).astype(BF16)
        for h in range(2):
            key = jnp.concatenate([keys[:, h * NOPE : (h + 1) * NOPE], key_rot], axis=1)
            value = values[h * VDIM : (h + 1) * VDIM]
            for b in range(NX):
                at = pl.ds(b * rows, rows)
                scores = nt_dot(key, qbuf[b, h]) * factor
                if diagonal:
                    key_at = x * rows + lax.broadcasted_iota(jnp.int32, scores.shape, 0)
                    query_at = b * rows + lax.broadcasted_iota(jnp.int32, scores.shape, 1)
                    allowed = key_at <= query_at
                    scores = jnp.where(allowed, scores, LOWEST)
                old = stat_m[h, :, at]
                new = jnp.maximum(old, jnp.max(scores, axis=0, keepdims=True))
                weights = jnp.exp2(scores - new)
                if diagonal:
                    weights = jnp.where(allowed, weights, 0.0)
                shrink = jnp.exp2(old - new)
                stat_m[h, :, at] = new
                stat_l[h, :, at] = stat_l[h, :, at] * shrink + jnp.sum(
                    weights, axis=0, keepdims=True
                )
                acc[h, :, at] = acc[h, :, at] * shrink + jnp.dot(
                    value, weights.astype(BF16), preferred_element_type=F32
                )

    own_lat.wait()
    own_q.wait()
    for k in range(1, NX):
        q_copy(k).wait_recv()
    piece(0, True)

    def arrive(slot, forward_to, device):
        for chunk in range(CHUNKS):
            ring(None, slot, chunk, device).wait_recv()
            if forward_to is not None:
                ring(slot, forward_to, chunk, device).start()
            pair(slot, chunk).start()

    def use(slot, needed):
        for chunk in range(CHUNKS):
            pair_in(slot, chunk).wait_recv()

        @pl.when(needed)
        def _():
            piece(slot, False)

    def both(d):
        def one(i, carry):
            slot = jnp.where(i == 0, d, far + d)
            source = jnp.where(i == 0, z - d, z + d - nz)
            use(slot, source >= 0)
            return carry

        return one

    for d in range(1, far + 1):
        arrive(d, d + 1 if d < far else None, up)
        if d < far:
            arrive(far + d, far + d + 1 if d < far - 1 else None, down)
        if d > 1:
            lax.fori_loop(0, 2, both(d - 1), 0)
    use(far, z - far >= 0)

    for k in range(1, NX):
        q_copy(k).wait_send()
    for slot in range(1, nz):
        for chunk in range(CHUNKS):
            ring(None, slot, chunk, up).wait_send()
            pair(slot, chunk).wait_send()

    for b in range(NX):
        at = pl.ds(b * rows, rows)
        for h in range(2):
            total = stat_l[h, :, at]
            inverse = jnp.where(total > 0.0, 1.0 / jnp.where(total > 0.0, total, 1.0), 0.0)
            osend[b, h * VDIM : (h + 1) * VDIM] = (acc[h, :, at] * inverse).astype(BF16)
            ssend[b, h : h + 1] = stat_m[h, :, at]
            ssend[b, 2 + h : 3 + h] = total

    def o_copy(k):
        to = lax.rem(x + k, NX)
        return pltpu.make_async_remote_copy(
            src_ref=osend.at[to],
            dst_ref=orecv.at[k],
            send_sem=o_send.at[k],
            recv_sem=o_recv.at[k],
            device_id=(z * NX + to, tp),
            device_id_type=MESH,
        )

    def s_copy(k):
        to = lax.rem(x + k, NX)
        return pltpu.make_async_remote_copy(
            src_ref=ssend.at[to],
            dst_ref=srecv.at[k],
            send_sem=s_send.at[k],
            recv_sem=s_recv.at[k],
            device_id=(z * NX + to, tp),
            device_id_type=MESH,
        )

    for k in range(1, NX):
        s_copy(k).start()
        o_copy(k).start()
    for k in range(1, NX):
        s_copy(k).wait_recv()
        o_copy(k).wait_recv()
    for h in range(2):
        stats = [ssend[x]] + [srecv[k] for k in range(1, NX)]
        outs = [osend[x, h * VDIM : (h + 1) * VDIM]] + [
            orecv[k, h * VDIM : (h + 1) * VDIM] for k in range(1, NX)
        ]
        top = functools.reduce(jnp.maximum, [s[h : h + 1] for s in stats])
        shares = [s[2 + h : 3 + h] * jnp.exp2(s[h : h + 1] - top) for s in stats]
        inverse = 1.0 / sum(shares)
        mixed = sum(o.astype(F32) * (w * inverse) for o, w in zip(outs, shares))
        out_ref[:, h * VDIM : (h + 1) * VDIM] = jnp.transpose(mixed).astype(BF16)
    for k in range(1, NX):
        s_copy(k).wait_send()
        o_copy(k).wait_send()


def attention(lat, q, wk, wv):
    nz = lax.axis_size("sp") // NX
    rows, wide = lat.shape
    lat = lat.reshape(NC, CHUNKS, rows // NC // CHUNKS, wide)
    dma = pltpu.SemaphoreType.DMA
    vmem = pl.BlockSpec(memory_space=pltpu.VMEM)
    return pl.pallas_call(
        functools.partial(attention_kernel, nz),
        out_shape=jax.ShapeDtypeStruct((rows, 2 * VDIM), BF16),
        in_specs=[vmem] * 4,
        out_specs=vmem,
        scratch_shapes=[
            pltpu.VMEM((nz, *lat.shape), BF16),
            pltpu.VMEM((NX, *q.shape), BF16),
            pltpu.VMEM((2, VDIM, NX * rows), F32),
            pltpu.VMEM((2, 1, NX * rows), F32),
            pltpu.VMEM((2, 1, NX * rows), F32),
            pltpu.VMEM((NX, 2 * VDIM, rows), BF16),
            pltpu.VMEM((NX, 2 * VDIM, rows), BF16),
            pltpu.VMEM((NX, 8, rows), F32),
            pltpu.VMEM((NX, 8, rows), F32),
            dma((2,)),
            dma((nz, CHUNKS)),
            dma((nz, CHUNKS)),
            dma((nz, CHUNKS)),
            dma((nz, CHUNKS)),
            dma((NX,)),
            dma((NX,)),
            dma((NX,)),
            dma((NX,)),
            dma((NX,)),
            dma((NX,)),
        ],
        compiler_params=pltpu.CompilerParams(
            collective_id=0, has_side_effects=True, vmem_limit_bytes=40 * 1024 * 1024
        ),
        cost_estimate=pl.CostEstimate(
            flops=20_000_000_000, bytes_accessed=4_000_000, transcendentals=0
        ),
    )(lat, q, wk, wv)


def turned(values, cosine, sine):
    half = values.shape[-1] // 2
    first, second = values[..., :half], values[..., half:]
    return jnp.concatenate(
        [first * cosine - second * sine, first * sine + second * cosine], axis=-1
    )


def attended_rows(queries, latent, rope_key, lat_gain, kv_weight):
    rows = latent.shape[0]
    first_row = lax.axis_index("sp") * rows
    heads_here = queries.shape[1] // (NOPE + ROPE)
    places = (first_row + jnp.arange(rows, dtype=jnp.int32)).astype(F32)
    half = ROPE // 2
    inverse = THETA ** (-jnp.arange(half, dtype=F32) / half)
    angle = places[:, None] * inverse
    cosine, sine = jnp.cos(angle), jnp.sin(angle)
    pad = jnp.zeros((rows, NOPE - ROPE), BF16)
    key_rot = turned(rope_key.astype(F32), cosine, sine).astype(BF16)
    normed = norm_rows(latent, lat_gain).astype(BF16)
    lat = jnp.concatenate([normed, key_rot, pad], axis=1)
    query = queries.reshape(rows, heads_here, NOPE + ROPE)
    query_rot = turned(
        query[:, :, NOPE:].astype(F32), cosine[:, None], sine[:, None]
    ).astype(BF16)
    full = jnp.concatenate(
        [query[:, :, :NOPE], query_rot, jnp.broadcast_to(pad[:, None], (rows, heads_here, NOPE - ROPE))],
        axis=2,
    )
    full = jnp.transpose(full, (1, 0, 2))
    weight = kv_weight.reshape(kv_weight.shape[0], heads_here, NOPE + VDIM)
    wk = weight[:, :, :NOPE].reshape(-1, heads_here * NOPE)
    wv = jnp.transpose(weight[:, :, NOPE:].reshape(-1, heads_here * VDIM))
    return attention(lat, full, wk, wv)


def body(
    resid,
    queries,
    latent,
    rope_key,
    lat_gain,
    kv_weight,
    out_gain,
    out_weight,
    ffn_gain,
    gate_weight,
    up_weight,
    down_weight,
):
    rows_here = resid.shape[0]
    whole_gate, whole_up, whole_down = turned_gather(
        (gate_weight, up_weight, down_weight), "sp", (0, 0, 1)
    )
    attended = attended_rows(queries, latent, rope_key, lat_gain, kv_weight)
    attended_float = attended.astype(F32)
    squares = over_copies(jnp.sum(attended_float * attended_float, axis=1), "tp")
    normed_out = attended_float * lax.rsqrt(squares / (HEADS * VDIM) + EPSILON)[:, None] * out_gain
    normed_out = normed_out.astype(jnp.bfloat16)
    share = rows_here // lax.axis_size("tp")
    own_first = lax.axis_index("tp") * share
    attn_sum = summed_on_arrival(
        jnp.dot(normed_out, out_weight, preferred_element_type=jnp.float32).astype(jnp.bfloat16),
        "tp",
        0,
    )
    own_resid = lax.dynamic_slice_in_dim(resid, own_first, share, 0)
    middle = (own_resid.astype(jnp.float32) + attn_sum).astype(jnp.bfloat16)
    normed_mid = gather_directly(norm_rows(middle, ffn_gain).astype(jnp.bfloat16), "tp", 0)
    gate = jnp.dot(normed_mid, whole_gate, preferred_element_type=jnp.float32)
    upward = jnp.dot(normed_mid, whole_up, preferred_element_type=jnp.float32)
    hidden = (jax.nn.silu(gate) * upward).astype(jnp.bfloat16)
    terms = jnp.dot(hidden, whole_down, preferred_element_type=jnp.float32)
    ffn_sum = summed_on_arrival(terms.astype(jnp.bfloat16), "tp", 0)
    return (middle.astype(jnp.float32) + ffn_sum).astype(jnp.bfloat16)


def solution(mesh):
    placed = (
        P("sp", None),
        P("sp", "tp"),
        P("sp", None),
        P("sp", None),
        P(),
        P(None, "tp"),
        P("tp"),
        P("tp", None),
        P(),
        P("sp", "tp"),
        P("sp", "tp"),
        P("tp", "sp"),
    )
    return jax.shard_map(
        body, mesh=mesh, in_specs=placed, out_specs=P(("sp", "tp"), None), check_vma=False
    )
```

```python
import functools
import math

import jax
import jax.numpy as jnp
from jax import lax
from jax.experimental import pallas as pl
from jax.experimental.pallas import tpu as pltpu
from jax.sharding import PartitionSpec as P

NOPE = 128
ROPE = 64
VDIM = 128
NX = 4
NY = 4
NC = 2
NT = NY * NC
CHUNKS = 2
UNIT = 192

EPSILON = 1e-06
THETA = 10000.0
LOWEST = -1e30
MESH = pl.DeviceIdType.MESH
F32 = jnp.float32
BF16 = jnp.bfloat16


def norm_rows(values, gain):
    wide = values.astype(jnp.float32)
    return wide * lax.rsqrt(jnp.mean(wide * wide, axis=-1, keepdims=True) + EPSILON) * gain


def nt_dot(a, b):
    return lax.dot_general(a, b, (((1,), (1,)), ((), ())), preferred_element_type=F32)


def wide_dot(a, b):
    return jnp.dot(a, b, preferred_element_type=F32)


class Refs:
    def __init__(self, names, values):
        self.__dict__.update(zip(names, values, strict=True))


def remote(src, dst, send, recv, to):
    return pltpu.make_async_remote_copy(
        src_ref=src, dst_ref=dst, send_sem=send, recv_sem=recv, device_id=to, device_id_type=MESH
    )


class Gather4:
    def __init__(self, piece, send, recv, index, plus, minus):
        self.piece, self.send, self.recv, self.index = piece, send, recv, index
        self.plus, self.minus = plus, minus

    def copy(self, way, k, half):
        to = self.plus if way in (0, 2) else self.minus
        ref = self.piece(k, half)
        return remote(ref, ref, self.send.at[self.index, way], self.recv.at[self.index, way], to)

    def start(self):
        self.copy(0, 0, None).start()
        self.copy(1, 0, None).start()

    def near(self, way):
        self.copy(way, 3 if way == 0 else 1, None).wait_recv()
        self.copy(way + 2, 3 if way == 0 else 1, way).start()

    def far(self, half):
        self.copy(half + 2, 2, half).wait_recv()

    def done(self):
        self.copy(0, 0, None).wait_send()
        self.copy(1, 0, None).wait_send()
        self.copy(2, 3, 0).wait_send()
        self.copy(3, 1, 1).wait_send()


class Scatter4:
    def __init__(self, block, half_in, whole_in, send, recv, index, plus, minus):
        self.block, self.half_in, self.whole_in = block, half_in, whole_in
        self.send, self.recv, self.index = send, recv, index
        self.plus, self.minus = plus, minus

    def half(self, h):
        to = self.minus if h == 0 else self.plus
        return remote(
            self.block(2, h), self.half_in.at[h], self.send.at[self.index, h], self.recv.at[self.index, h], to
        )

    def whole(self, h):
        to, k = (self.minus, 3) if h == 0 else (self.plus, 1)
        return remote(
            self.block(k, None),
            self.whole_in.at[h],
            self.send.at[self.index, 2 + h],
            self.recv.at[self.index, 2 + h],
            to,
        )

    def start(self):
        self.half(0).start()
        self.half(1).start()

    def near(self, h):
        self.half(h).wait_recv()
        ref = self.block(3 if h == 0 else 1, h)
        ref[...] = (ref[...].astype(F32) + self.half_in[h].astype(F32)).astype(BF16)
        self.whole(h).start()

    def total(self):
        self.whole(0).wait_recv()
        self.whole(1).wait_recv()
        ref = self.block(0, None)
        return ref[...].astype(F32) + self.whole_in[0].astype(F32) + self.whole_in[1].astype(F32)

    def finish(self):
        self.block(0, None)[...] = self.total().astype(BF16)

    def done(self):
        for h in range(2):
            self.half(h).wait_send()
            self.whole(h).wait_send()


def layer_kernel(nz, names, *values):
    r = Refs(names, values)
    sp, tp = lax.axis_index("sp"), lax.axis_index("tp")
    z, x = sp // NX, lax.rem(sp, NX)
    y, core = tp // NC, lax.rem(tp, NC)
    up = (lax.rem(z + 1, nz) * NX + x, tp)
    down = (lax.rem(z + nz - 1, nz) * NX + x, tp)
    partner = (sp, tp + 1 - 2 * core)
    rows = r.q.shape[1]
    far = nz // 2
    factor = (1.0 / math.sqrt(NOPE + ROPE)) * math.log2(math.e)
    cols = r.resid.shape[1] // NT
    share = rows // NT

    def along_x(k):
        return (z * NX + lax.rem(x + k, NX), tp)

    def along_y(k, other=0):
        to_core = core if other == 0 else 1 - core
        return (sp, lax.rem(y + k, NY) * NC + to_core)

    peers = [up, down, partner]
    peers += [along_x(k) for k in range(1, NX)]
    peers += [along_y(k) for k in range(1, NY)]
    peers += [along_y(k, 1) for k in range(1, NY)]
    barrier = pltpu.get_barrier_semaphore()
    for peer in peers:
        pl.semaphore_signal(barrier, inc=1, device_id=peer, device_id_type=MESH)
    pl.semaphore_wait(barrier, len(peers))

    def ring(src_slot, dst_slot, chunk, to):
        src = r.lat.at[core, chunk] if src_slot is None else r.latbuf.at[src_slot, core, chunk]
        dst = r.latbuf.at[dst_slot, core, chunk]
        return remote(src, dst, r.ring_send.at[dst_slot, chunk], r.ring_recv.at[dst_slot, chunk], to)

    def pair(slot, chunk, side):
        ref = r.latbuf.at[slot, side, chunk]
        return remote(ref, ref, r.pair_send.at[slot, chunk], r.pair_recv.at[slot, chunk], partner)

    def q_copy(k):
        return remote(r.q, r.qbuf.at[x], r.q_send.at[k], r.q_recv.at[k], along_x(k))

    def weight_copies(k):
        to = lax.rem(x + k, NX)
        return [
            remote(r.gu.at[to], r.gubuf.at[z, x], r.wx_send.at[k, 0], r.wx_recv.at[k, 0], along_x(k)),
            remote(r.dn.at[to], r.dnbuf.at[z, x], r.wx_send.at[k, 1], r.wx_recv.at[k, 1], along_x(k)),
        ]

    def ow_copy(i):
        k, other = i // 2, i % 2
        to = along_y(k, other)
        src = r.ow.at[:, pl.ds(pl.multiple_of(to[1] * cols, cols), cols)]
        return remote(src, r.owbuf.at[tp], r.ow_send.at[i], r.ow_recv.at[i], to)

    for chunk in range(CHUNKS):
        ring(None, 1, chunk, up).start()
        ring(None, far + 1, chunk, down).start()
    own_cols = pl.ds(pl.multiple_of(tp * cols, cols), cols)
    local = [
        pltpu.make_async_copy(r.lat, r.latbuf.at[0], r.local_sem.at[0]),
        pltpu.make_async_copy(r.q, r.qbuf.at[x], r.local_sem.at[1]),
        pltpu.make_async_copy(r.gu.at[x], r.gubuf.at[z, x], r.local_sem.at[2]),
        pltpu.make_async_copy(r.dn.at[x], r.dnbuf.at[z, x], r.local_sem.at[3]),
        pltpu.make_async_copy(r.ow.at[:, own_cols], r.owbuf.at[tp], r.local_sem.at[4]),
        pltpu.make_async_copy(r.resid.at[:, own_cols], r.residbuf, r.local_sem.at[5]),
    ]
    for copy in local:
        copy.start()
    for k in range(1, NX):
        q_copy(k).start()
    for k in range(1, NX):
        for copy in weight_copies(k):
            copy.start()
    for i in range(1, NT):
        ow_copy(i).start()

    r.stat_m[...] = jnp.full(r.stat_m.shape, LOWEST, F32)
    r.stat_l[...] = jnp.zeros(r.stat_l.shape, F32)
    r.acc[...] = jnp.zeros(r.acc.shape, F32)

    def piece(slot, diagonal):
        lat = r.latbuf[slot].reshape(rows, r.lat.shape[-1])
        wide = r.wk.shape[0]
        compressed, key_rot = lat[:, :wide], lat[:, wide:]
        keys = wide_dot(compressed, r.wk[...]).astype(BF16)
        values = nt_dot(r.wv[...], compressed).astype(BF16)
        for h in range(2):
            key = jnp.concatenate([keys[:, h * NOPE : (h + 1) * NOPE], key_rot], axis=1)
            value = values[h * VDIM : (h + 1) * VDIM]
            for b in range(NX):
                at = pl.ds(b * rows, rows)
                scores = nt_dot(key, r.qbuf[b, h]) * factor
                if diagonal:
                    key_at = x * rows + lax.broadcasted_iota(jnp.int32, scores.shape, 0)
                    query_at = b * rows + lax.broadcasted_iota(jnp.int32, scores.shape, 1)
                    allowed = key_at <= query_at
                    scores = jnp.where(allowed, scores, LOWEST)
                old = r.stat_m[h, :, at]
                new = jnp.maximum(old, jnp.max(scores, axis=0, keepdims=True))
                weights = jnp.exp2(scores - new)
                if diagonal:
                    weights = jnp.where(allowed, weights, 0.0)
                shrink = jnp.exp2(old - new)
                r.stat_m[h, :, at] = new
                r.stat_l[h, :, at] = r.stat_l[h, :, at] * shrink + jnp.sum(
                    weights, axis=0, keepdims=True
                )
                r.acc[h, :, at] = r.acc[h, :, at] * shrink + wide_dot(value, weights.astype(BF16))

    for copy in local[:2]:
        copy.wait()
    for k in range(1, NX):
        q_copy(k).wait_recv()
    piece(0, True)

    def arrive(slot, forward_to, to):
        for chunk in range(CHUNKS):
            ring(None, slot, chunk, to).wait_recv()
            if forward_to is not None:
                ring(slot, forward_to, chunk, to).start()
            pair(slot, chunk, core).start()

    def use(slot, needed):
        for chunk in range(CHUNKS):
            pair(slot, chunk, 1 - core).wait_recv()

        @pl.when(needed)
        def _():
            piece(slot, False)

    def both(d):
        def one(i, carry):
            slot = jnp.where(i == 0, d, far + d)
            source = jnp.where(i == 0, z - d, z + d - nz)
            use(slot, source >= 0)
            return carry

        return one

    def hop(d, way, part):
        of = lax.rem(z - (d - 1) + nz, nz) if way == 0 else lax.rem(z + d - 1, nz)
        ref = (r.gubuf if part == 0 else r.dnbuf).at[of]
        to = up if way == 0 else down
        return remote(ref, ref, r.hop_send.at[d, way, part], r.hop_recv.at[d, way, part], to)

    def hop_in(d, way, part):
        of = lax.rem(z - d + nz, nz) if way == 0 else lax.rem(z + d, nz)
        ref = (r.gubuf if part == 0 else r.dnbuf).at[of]
        to = up if way == 0 else down
        return remote(ref, ref, r.hop_send.at[d, way, part], r.hop_recv.at[d, way, part], to)

    def in_hop(d):
        return [(way, part) for part in range(2) for way in range(2) if d < far or way == part]

    def hop_first():
        for k in range(1, NX):
            for copy in weight_copies(k):
                copy.wait_recv()
        local[2].wait()
        local[3].wait()
        for way, part in in_hop(1):
            hop(1, way, part).start()

    def hop_on(d):
        for way, part in in_hop(d):
            hop_in(d, way, part).wait_recv()
            if d < far and (way, part) in in_hop(d + 1):
                hop(d + 1, way, part).start()

    for d in range(1, far + 1):
        arrive(d, d + 1 if d < far else None, up)
        if d < far:
            arrive(far + d, far + d + 1 if d < far - 1 else None, down)
        if d == far:
            hop_first()
        if d > 1:
            lax.fori_loop(0, 2, both(d - 1), 0)
    use(far, z - far >= 0)

    for b in range(NX):
        at = pl.ds(b * rows, rows)
        for h in range(2):
            total = r.stat_l[h, :, at]
            inverse = jnp.where(total > 0.0, 1.0 / jnp.where(total > 0.0, total, 1.0), 0.0)
            r.osend[b, h * VDIM : (h + 1) * VDIM] = (r.acc[h, :, at] * inverse).astype(BF16)
            r.ssend[b, h : h + 1] = r.stat_m[h, :, at]
            r.ssend[b, 2 + h : 3 + h] = total

    def o_copy(k):
        to = lax.rem(x + k, NX)
        return remote(r.osend.at[to], r.orecv.at[k], r.o_send.at[k], r.o_recv.at[k], along_x(k))

    def s_copy(k):
        to = lax.rem(x + k, NX)
        return remote(r.ssend.at[to], r.srecv.at[k], r.s_send.at[k], r.s_recv.at[k], along_x(k))

    for k in range(1, NX):
        s_copy(k).start()
        o_copy(k).start()
    for k in range(1, NX):
        s_copy(k).wait_recv()
        o_copy(k).wait_recv()
    width = 2 * VDIM
    stats = [r.ssend[x]] + [r.srecv[k] for k in range(1, NX)]
    for h in range(2):
        outs = [r.osend[x, h * VDIM : (h + 1) * VDIM]] + [
            r.orecv[k, h * VDIM : (h + 1) * VDIM] for k in range(1, NX)
        ]
        top = functools.reduce(jnp.maximum, [s[h : h + 1] for s in stats])
        shares = [s[2 + h : 3 + h] * jnp.exp2(s[h : h + 1] - top) for s in stats]
        inverse = 1.0 / sum(shares)
        mixed = sum(o.astype(F32) * (w * inverse) for o, w in zip(outs, shares))
        at = pl.ds(pl.multiple_of(tp * width + h * VDIM, VDIM), VDIM)
        r.att[:, at] = jnp.transpose(mixed).astype(BF16)

    def att_piece(own_core):
        def ref(k, half):
            of = lax.rem(y + k, NY) * NC + own_core
            where = pl.ds(pl.multiple_of(of * width, width), width)
            at = pl.ds(0, rows) if half is None else pl.ds(half * (rows // 2), rows // 2)
            return r.att.at[at, where]

        return ref

    ga = Gather4(att_piece(core), r.ga_send, r.ga_recv, 0, along_y(1), along_y(3))

    def swap(piece, send, recv, index):
        k, half = ((0, None), (3, None), (1, None), (2, 0), (2, 1))[index]
        mine, theirs = piece(core)(k, half), piece(1 - core)(k, half)
        out = functools.partial(remote, mine, mine, send.at[index], recv.at[index], partner)
        come = functools.partial(remote, theirs, theirs, send.at[index], recv.at[index], partner)
        return out, come

    swaps = [swap(att_piece, r.sa_send.at[0], r.sa_recv.at[0], i) for i in range(5)]
    ga.start()
    swaps[0][0]().start()
    ga.near(0)
    swaps[1][0]().start()
    ga.near(1)
    swaps[2][0]().start()
    ga.far(0)
    swaps[3][0]().start()
    ga.far(1)
    swaps[4][0]().start()
    for i in range(1, NT):
        ow_copy(i).wait_recv()
    local[4].wait()
    local[5].wait()
    hop_on(1)
    for out, come in swaps:
        come().wait_recv()

    att = r.att[...]
    att_wide = att.astype(F32)
    scale = lax.rsqrt(jnp.mean(att_wide * att_wide, axis=1, keepdims=True) + EPSILON)
    attn_sum = wide_dot(att, r.owbuf[...].reshape(att.shape[1], cols)) * scale
    r.mid[x, :, own_cols] = (r.residbuf[...].astype(F32) + attn_sum).astype(BF16)

    def mid_piece(axis, at_x, at_y, own_core, first):
        def ref(k, half):
            of_x = lax.rem(x + at_x + (k if axis == 0 else 0), NX)
            of_y = lax.rem(y + at_y + (k if axis == 1 else 0), NY)
            where = pl.ds(pl.multiple_of((of_y * NC + own_core) * cols, cols), cols)
            quarter = rows // 4
            at = pl.ds(first * 2 * quarter, 2 * quarter)
            if half is not None:
                at = pl.ds((first * 2 + half) * quarter, quarter)
            return r.mid.at[of_x, at, where]

        return ref

    def plane_ring(index, axis, at_x, at_y, first):
        piece_of = functools.partial(lambda c: mid_piece(axis, at_x, at_y, c, first))
        plus, minus = (along_x(1), along_x(3)) if axis == 0 else (along_y(1), along_y(3))
        g = Gather4(piece_of(core), r.gm_send, r.gm_recv, index, plus, minus)
        return g, [swap(piece_of, r.sm_send.at[index], r.sm_recv.at[index], i) for i in range(5)]

    offsets = (0, 3, 1, 2)
    first_rings = [plane_ring(0, 0, 0, 0, 0), plane_ring(1, 1, 0, 0, 1)]
    second_rings = [
        [plane_ring(2 + i, 1, k, 0, 0), plane_ring(6 + i, 0, 0, k, 1)] for i, k in enumerate(offsets)
    ]
    for g, s in first_rings:
        g.start()
        s[0][0]().start()
    for g, s in second_rings[0]:
        g.start()
    for way in range(2):
        for i, (g, s) in enumerate(first_rings):
            g.near(way)
            second_rings[1 + way][i][0].start()
            s[1 + way][0]().start()
    for way in range(2):
        for g, s in second_rings[0]:
            g.near(way)
            s[1 + way][0]().start()
    for i, (g, s) in enumerate(first_rings):
        for half in range(2):
            g.far(half)
            s[3 + half][0]().start()
        second_rings[3][i][0].start()
    hop_on(2)
    for j in range(1, 4):
        for way in range(2):
            for g, s in second_rings[j]:
                g.near(way)
                s[1 + way][0]().start()
        for half in range(2):
            for g, s in second_rings[j - 1]:
                g.far(half)
                s[3 + half][0]().start()
        if j == 2 and far > 3:
            hop_on(3)
    for half in range(2):
        for g, s in second_rings[3]:
            g.far(half)
            s[3 + half][0]().start()
    if far == 2:
        pass
    else:
        hop_on(far)
    rings = first_rings + [pair_of for both_of in second_rings for pair_of in both_of]
    for i, (g, s) in enumerate(rings):
        for j, (out, come) in enumerate(s):
            if j > 0 or i < 2:
                come().wait_recv()

    def mixer(b, carry):
        squares = jnp.zeros((rows, 128), F32)
        for j in range(r.mid.shape[2] // 128):
            v = r.mid[b, :, j * 128 : (j + 1) * 128].astype(F32)
            squares = squares + v * v
        mean = jnp.sum(squares, axis=1, keepdims=True) / r.mid.shape[2]
        row_scale = lax.rsqrt(mean + EPSILON)
        mid = r.mid[b]
        gu = wide_dot(mid, r.gubuf[...].reshape(mid.shape[1], 2 * UNIT)) * row_scale
        gate, mixed_tile, upward = gu[:, :128], gu[:, 128:256], gu[:, 256:]
        first = gate / (1.0 + jnp.exp(-gate)) * upward
        second = (mixed_tile / (1.0 + jnp.exp(-mixed_tile)))[:, :64] * mixed_tile[:, 64:]
        hidden = jnp.concatenate([first, second], axis=1).astype(BF16)
        n = r.dnbuf.shape[-1]
        for zz in range(nz):
            w = jnp.concatenate([r.dnbuf[zz, i] for i in range(NX)], axis=1)
            terms = wide_dot(hidden, w).astype(BF16).reshape(NY, NC, share, NX * n)
            for c in range(NC):
                r.part[c, b, :, :, zz * NX * n : (zz + 1) * NX * n] = terms[:, c]
        core_copy(b).start()
        return carry

    def core_copy(b):
        return remote(r.part.at[1 - core, b], r.pairbuf.at[b], r.pc_send.at[b], r.pc_recv.at[b], partner)

    lax.fori_loop(0, NX, mixer, 0)

    def core_sum(b, carry):
        core_copy(b).wait_recv()
        for i in range(NY):
            ref = r.part.at[core, b, i]
            ref[...] = (ref[...].astype(F32) + r.pairbuf[b, i].astype(F32)).astype(BF16)
        return carry

    lax.fori_loop(0, NX, core_sum, 0)

    depth = r.part.shape[-1] // 2

    def block(axis, of_x, of_y, first):
        def ref(k, half):
            bx = lax.rem(of_x + (k if axis == 0 else 0), NX)
            by = lax.rem(of_y + (k if axis == 1 else 0), NY)
            at = pl.ds(first * depth, depth)
            if half is not None:
                at = pl.ds(first * depth + half * (depth // 2), depth // 2)
            return r.part.at[core, bx, by, :, at]

        return ref

    def scatter(index, axis, of_x, of_y, first):
        plus, minus = (along_x(1), along_x(3)) if axis == 0 else (along_y(1), along_y(3))
        return Scatter4(
            block(axis, of_x, of_y, first),
            r.half_in.at[index],
            r.whole_in.at[index],
            r.rs_send,
            r.rs_recv,
            index,
            plus,
            minus,
        )

    order = (1, 3, 2, 0)
    steps = [
        [scatter(i, 1, x + k, y, 0), scatter(4 + i, 0, x, y + k, 1)] for i, k in enumerate(order)
    ]
    ends = [scatter(8, 0, x, y, 0), scatter(9, 1, x, y, 1)]
    for both_of in steps:
        for s in both_of:
            s.start()
    for both_of in steps:
        for s in both_of:
            s.near(0)
            s.near(1)
    for j, both_of in enumerate(steps):
        for s in both_of:
            s.finish()
        if j == 2:
            for s in ends:
                s.start()
    for s in ends:
        s.near(0)
        s.near(1)
    own_rows = pl.ds(pl.multiple_of(tp * share, share), share)
    for first, s in enumerate(ends):
        at = slice(first * depth, (first + 1) * depth)
        r.out[:, at] = (s.total() + r.mid[x, own_rows, at].astype(F32)).astype(BF16)

    for k in range(1, NX):
        q_copy(k).wait_send()
        o_copy(k).wait_send()
        s_copy(k).wait_send()
        for copy in weight_copies(k):
            copy.wait_send()
    for i in range(1, NT):
        ow_copy(i).wait_send()
    for slot in range(1, nz):
        for chunk in range(CHUNKS):
            ring(None, slot, chunk, up).wait_send()
            pair(slot, chunk, core).wait_send()
    for d in range(1, far + 1):
        for way, part in in_hop(d):
            hop(d, way, part).wait_send()
    ga.done()
    for out, come in swaps:
        out().wait_send()
    for i, (g, s) in enumerate(rings):
        g.done()
        for j, (out, come) in enumerate(s):
            if j > 0 or i < 2:
                out().wait_send()
    for b in range(NX):
        core_copy(b).wait_send()
    for both_of in [*steps, ends]:
        for s in both_of:
            s.done()


def layer(lat, q, wk, wv, gu, dn, ow, resid):
    nz = lax.axis_size("sp") // NX
    rows, wide = lat.shape
    dim = resid.shape[1]
    share = rows // NT
    cols = dim // NT
    lat = lat.reshape(NC, CHUNKS, rows // NC // CHUNKS, wide)
    vmem = pl.BlockSpec(memory_space=pltpu.VMEM)
    anywhere = pl.BlockSpec(memory_space=pl.ANY)
    inputs = {
        "lat": (lat, vmem),
        "q": (q, vmem),
        "wk": (wk, vmem),
        "wv": (wv, vmem),
        "gu": (gu, anywhere),
        "dn": (dn, anywhere),
        "ow": (ow, anywhere),
        "resid": (resid, anywhere),
    }
    buffers = {
        "latbuf": ((nz, *lat.shape), BF16),
        "qbuf": ((NX, *q.shape), BF16),
        "acc": ((2, VDIM, NX * rows), F32),
        "stat_m": ((2, 1, NX * rows), F32),
        "stat_l": ((2, 1, NX * rows), F32),
        "osend": ((NX, 2 * VDIM, rows), BF16),
        "orecv": ((NX, 2 * VDIM, rows), BF16),
        "ssend": ((NX, 8, rows), F32),
        "srecv": ((NX, 8, rows), F32),
        "gubuf": ((nz, *gu.shape), BF16),
        "dnbuf": ((nz, *dn.shape), BF16),
        "owbuf": ((NT, ow.shape[0], cols), BF16),
        "residbuf": ((rows, cols), BF16),
        "att": ((rows, NT * 2 * VDIM), BF16),
        "mid": ((NX, rows, dim), BF16),
        "part": ((NC, NX, NY, share, dim), BF16),
        "pairbuf": ((NX, NY, share, dim), BF16),
        "half_in": ((10, 2, share, dim // 4), BF16),
        "whole_in": ((10, 2, share, dim // 2), BF16),
    }
    semaphores = {
        "local_sem": (6,),
        "ring_send": (nz, CHUNKS),
        "ring_recv": (nz, CHUNKS),
        "pair_send": (nz, CHUNKS),
        "pair_recv": (nz, CHUNKS),
        "q_send": (NX,),
        "q_recv": (NX,),
        "wx_send": (NX, 2),
        "wx_recv": (NX, 2),
        "ow_send": (NT,),
        "ow_recv": (NT,),
        "hop_send": (nz, 2, 2),
        "hop_recv": (nz, 2, 2),
        "o_send": (NX,),
        "o_recv": (NX,),
        "s_send": (NX,),
        "s_recv": (NX,),
        "ga_send": (1, 4),
        "ga_recv": (1, 4),
        "sa_send": (1, 5),
        "sa_recv": (1, 5),
        "gm_send": (10, 4),
        "gm_recv": (10, 4),
        "sm_send": (10, 5),
        "sm_recv": (10, 5),
        "pc_send": (NX,),
        "pc_recv": (NX,),
        "rs_send": (10, 4),
        "rs_recv": (10, 4),
    }
    names = [*inputs, "out", *buffers, *semaphores]
    return pl.pallas_call(
        functools.partial(layer_kernel, nz, names),
        out_shape=jax.ShapeDtypeStruct((share, dim), BF16),
        in_specs=[spec for _, spec in inputs.values()],
        out_specs=vmem,
        scratch_shapes=[pltpu.VMEM(*b) for b in buffers.values()]
        + [pltpu.SemaphoreType.DMA(s) for s in semaphores.values()],
        compiler_params=pltpu.CompilerParams(
            collective_id=0, has_side_effects=True, vmem_limit_bytes=62 * 1024 * 1024
        ),
    )(*[array for array, _ in inputs.values()])


def turned(values, cosine, sine):
    half = values.shape[-1] // 2
    first, second = values[..., :half], values[..., half:]
    return jnp.concatenate(
        [first * cosine - second * sine, first * sine + second * cosine], axis=-1
    )


def body(
    resid,
    queries,
    latent,
    rope_key,
    lat_gain,
    kv_weight,
    out_gain,
    out_weight,
    ffn_gain,
    gate_weight,
    up_weight,
    down_weight,
):
    rows = latent.shape[0]
    sp = lax.axis_index("sp")
    heads_here = queries.shape[1] // (NOPE + ROPE)
    places = (sp * rows + jnp.arange(rows, dtype=jnp.int32)).astype(F32)
    half = ROPE // 2
    inverse = THETA ** (-jnp.arange(half, dtype=F32) / half)
    angle = places[:, None] * inverse
    cosine, sine = jnp.cos(angle), jnp.sin(angle)
    pad = jnp.zeros((rows, NOPE - ROPE), BF16)
    key_rot = turned(rope_key.astype(F32), cosine, sine).astype(BF16)
    normed = norm_rows(latent, lat_gain).astype(BF16)
    lat = jnp.concatenate([normed, key_rot, pad], axis=1)
    query = queries.reshape(rows, heads_here, NOPE + ROPE)
    query_rot = turned(
        query[:, :, NOPE:].astype(F32), cosine[:, None], sine[:, None]
    ).astype(BF16)
    full = jnp.concatenate(
        [query[:, :, :NOPE], query_rot, jnp.broadcast_to(pad[:, None], (rows, heads_here, NOPE - ROPE))],
        axis=2,
    )
    full = jnp.transpose(full, (1, 0, 2))
    weight = kv_weight.reshape(kv_weight.shape[0], heads_here, NOPE + VDIM)
    wk = weight[:, :, :NOPE].reshape(-1, heads_here * NOPE)
    wv = jnp.transpose(weight[:, :, NOPE:].reshape(-1, heads_here * VDIM))
    depth = gate_weight.shape[0]
    gain = lax.dynamic_slice_in_dim(ffn_gain, sp * depth, depth)[:, None]
    gate = (gate_weight.astype(F32) * gain).astype(BF16)
    upward = (up_weight.astype(F32) * gain).astype(BF16)
    gu = jnp.stack(
        [
            jnp.concatenate(
                [
                    gate[:, i * UNIT : i * UNIT + 128],
                    gate[:, i * UNIT + 128 : (i + 1) * UNIT],
                    upward[:, i * UNIT + 128 : (i + 1) * UNIT],
                    upward[:, i * UNIT : i * UNIT + 128],
                ],
                axis=1,
            )
            for i in range(NX)
        ]
    )
    dn = down_weight.reshape(NX, UNIT, down_weight.shape[1])
    ow = (out_weight.astype(F32) * out_gain[:, None]).astype(BF16)
    return layer(lat, full, wk, wv, gu, dn, ow, resid)


def solution(mesh):
    placed = (
        P("sp", None),
        P("sp", "tp"),
        P("sp", None),
        P("sp", None),
        P(),
        P(None, "tp"),
        P("tp"),
        P("tp", None),
        P(),
        P("sp", "tp"),
        P("sp", "tp"),
        P("tp", "sp"),
    )
    return jax.shard_map(
        body, mesh=mesh, in_specs=placed, out_specs=P(("sp", "tp"), None), check_vma=False
    )
```

```python
import functools
import math

import jax
import jax.numpy as jnp
import numpy as np
from jax import lax
from jax.experimental import pallas as pl
from jax.experimental.pallas import tpu as pltpu
from jax.sharding import PartitionSpec as P

NOPE = 128
ROPE = 64
VDIM = 128
NX = 4
NY = 4
NC = 2
NT = NY * NC
CHUNKS = 2
UNIT = 192

EPSILON = 1e-06
THETA = 10000.0
LOWEST = -1e30
MESH = pl.DeviceIdType.MESH
F32 = jnp.float32
BF16 = jnp.bfloat16


def norm_rows(values, gain):
    wide = values.astype(F32)
    return wide * lax.rsqrt(jnp.mean(wide * wide, axis=-1, keepdims=True) + EPSILON) * gain


def column(row):
    return jnp.transpose(jnp.broadcast_to(row, (128, row.shape[1])))[:, :1]


def turned(values, cosine, sine):
    half = values.shape[-1] // 2
    first, second = values[:, :half], values[:, half:]
    return jnp.concatenate(
        [first * cosine - second * sine, first * sine + second * cosine], axis=1
    )


def nt_dot(a, b):
    return lax.dot_general(a, b, (((1,), (1,)), ((), ())), preferred_element_type=F32)


def wide_dot(a, b):
    return jnp.dot(a, b, preferred_element_type=F32)


class Refs:
    def __init__(self, names, values):
        self.__dict__.update(zip(names, values, strict=True))


def remote(src, dst, send, recv, to):
    return pltpu.make_async_remote_copy(
        src_ref=src, dst_ref=dst, send_sem=send, recv_sem=recv, device_id=to, device_id_type=MESH
    )


class Gather4:
    def __init__(self, piece, send, recv, index, plus, minus):
        self.piece, self.send, self.recv, self.index = piece, send, recv, index
        self.plus, self.minus = plus, minus

    def copy(self, way, k, half):
        to = self.plus if way in (0, 2) else self.minus
        ref = self.piece(k, half)
        return remote(ref, ref, self.send.at[self.index, way], self.recv.at[self.index, way], to)

    def start(self):
        self.copy(0, 0, None).start()
        self.copy(1, 0, None).start()

    def near(self, way):
        self.copy(way, 3 if way == 0 else 1, None).wait_recv()
        self.copy(way + 2, 3 if way == 0 else 1, way).start()

    def far(self, half):
        self.copy(half + 2, 2, half).wait_recv()

    def done(self):
        self.copy(0, 0, None).wait_send()
        self.copy(1, 0, None).wait_send()
        self.copy(2, 3, 0).wait_send()
        self.copy(3, 1, 1).wait_send()


class Scatter4:
    def __init__(self, block, half_in, whole_in, send, recv, index, plus, minus):
        self.block, self.half_in, self.whole_in = block, half_in, whole_in
        self.send, self.recv, self.index = send, recv, index
        self.plus, self.minus = plus, minus

    def half(self, h):
        to = self.minus if h == 0 else self.plus
        return remote(
            self.block(2, h), self.half_in.at[h], self.send.at[self.index, h], self.recv.at[self.index, h], to
        )

    def whole(self, h):
        to, k = (self.minus, 3) if h == 0 else (self.plus, 1)
        return remote(
            self.block(k, None),
            self.whole_in.at[h],
            self.send.at[self.index, 2 + h],
            self.recv.at[self.index, 2 + h],
            to,
        )

    def start(self):
        self.half(0).start()
        self.half(1).start()

    def near(self, h):
        self.half(h).wait_recv()
        ref = self.block(3 if h == 0 else 1, h)
        ref[...] = (ref[...].astype(F32) + self.half_in[h].astype(F32)).astype(BF16)
        self.whole(h).start()

    def total(self):
        self.whole(0).wait_recv()
        self.whole(1).wait_recv()
        ref = self.block(0, None)
        return ref[...].astype(F32) + self.whole_in[0].astype(F32) + self.whole_in[1].astype(F32)

    def finish(self):
        self.block(0, None)[...] = self.total().astype(BF16)

    def done(self):
        for h in range(2):
            self.half(h).wait_send()
            self.whole(h).wait_send()


def layer_kernel(nz, names, *values):
    r = Refs(names, values)
    sp, tp = lax.axis_index("sp"), lax.axis_index("tp")
    z, x = sp // NX, lax.rem(sp, NX)
    y, core = tp // NC, lax.rem(tp, NC)
    up = (lax.rem(z + 1, nz) * NX + x, tp)
    down = (lax.rem(z + nz - 1, nz) * NX + x, tp)
    partner = (sp, tp + 1 - 2 * core)
    rows = r.latent.shape[0]
    far = nz // 2
    factor = (1.0 / math.sqrt(NOPE + ROPE)) * math.log2(math.e)
    dim = r.resid.shape[1]
    cols = dim // NT
    share = rows // NT

    def along_x(k):
        return (z * NX + lax.rem(x + k, NX), tp)

    def along_y(k, other=0):
        to_core = core if other == 0 else 1 - core
        return (sp, lax.rem(y + k, NY) * NC + to_core)

    peers = [up, down, partner]
    peers += [along_x(k) for k in range(1, NX)]
    peers += [along_y(k) for k in range(1, NY)]
    peers += [along_y(k, 1) for k in range(1, NY)]
    barrier = pltpu.get_barrier_semaphore()
    for peer in peers:
        pl.semaphore_signal(barrier, inc=1, device_id=peer, device_id_type=MESH)

    own_cols = pl.ds(pl.multiple_of(tp * cols, cols), cols)
    local = [
        pltpu.make_async_copy(r.ow, r.owstage, r.local_sem.at[0]),
        pltpu.make_async_copy(r.dn.at[x], r.dnbuf.at[z, x], r.local_sem.at[1]),
        pltpu.make_async_copy(r.resid.at[:, own_cols], r.residbuf, r.local_sem.at[2]),
        pltpu.make_async_copy(r.gustage.at[x], r.gubuf.at[z, x], r.local_sem.at[3]),
        pltpu.make_async_copy(r.owstage.at[:, own_cols], r.owbuf.at[tp], r.local_sem.at[4]),
    ]
    for copy in local[:3]:
        copy.start()

    half = ROPE // 2
    base, step = r.first_turn[pl.ds(sp, 1), :], r.row_turn[...]
    base_cos, base_sin = base[:, :half], base[:, half:]
    step_cos, step_sin = step[:, :half], step[:, half:]
    cosine = base_cos * step_cos - base_sin * step_sin
    sine = base_sin * step_cos + base_cos * step_sin
    key_rot = turned(r.rope_key[...].astype(F32), cosine, sine)
    lat = jnp.concatenate([norm_rows(r.latent[...], r.lat_gain[...]), key_rot, key_rot], axis=1)
    r.latbuf[0] = lat.astype(BF16).reshape(r.latbuf.shape[1:])
    query = r.queries[...].astype(F32)
    one = NOPE + ROPE
    parts = [query[:, h * one : h * one + NOPE] for h in range(2)]
    parts += [turned(query[:, h * one + NOPE : (h + 1) * one], cosine, sine) for h in range(2)]
    r.qbuf[x] = jnp.concatenate(parts, axis=1).astype(BF16)
    pl.semaphore_wait(barrier, len(peers))

    def ring(src_slot, dst_slot, chunk, to):
        src = r.latbuf.at[src_slot, core, chunk]
        dst = r.latbuf.at[dst_slot, core, chunk]
        return remote(src, dst, r.ring_send.at[dst_slot, chunk], r.ring_recv.at[dst_slot, chunk], to)

    def pair(slot, chunk, side):
        ref = r.latbuf.at[slot, side, chunk]
        return remote(ref, ref, r.pair_send.at[slot, chunk], r.pair_recv.at[slot, chunk], partner)

    def q_piece(k, half):
        at = pl.ds(0, rows) if half is None else pl.ds(half * (rows // 2), rows // 2)
        return r.qbuf.at[lax.rem(x + k, NX), at]

    gq = Gather4(q_piece, r.gq_send, r.gq_recv, 0, along_x(1), along_x(3))

    def weight_copies(k):
        to = lax.rem(x + k, NX)
        return [
            remote(r.gustage.at[to], r.gubuf.at[z, x], r.wx_send.at[k, 0], r.wx_recv.at[k, 0], along_x(k)),
            remote(r.dn.at[to], r.dnbuf.at[z, x], r.wx_send.at[k, 1], r.wx_recv.at[k, 1], along_x(k)),
        ]

    def ow_copy(i):
        k, other = i // 2, i % 2
        to = along_y(k, other)
        src = r.owstage.at[:, pl.ds(pl.multiple_of(to[1] * cols, cols), cols)]
        return remote(src, r.owbuf.at[tp], r.ow_send.at[i], r.ow_recv.at[i], to)

    for chunk in range(CHUNKS):
        ring(0, 1, chunk, up).start()
        ring(0, far + 1, chunk, down).start()
    gq.start()

    gain = column(r.ffn_gain[pl.ds(sp, 1), :])
    gate, upward = r.gate[...].astype(F32) * gain, r.upward[...].astype(F32) * gain
    for i in range(NX):
        lo, mid_lo, hi = i * UNIT, i * UNIT + 128, (i + 1) * UNIT
        tiles = [gate[:, lo:mid_lo], gate[:, mid_lo:hi], upward[:, mid_lo:hi], upward[:, lo:mid_lo]]
        r.gustage[i] = jnp.concatenate(tiles, axis=1).astype(BF16)
    local[3].start()
    for k in (2, 1, 3):
        for copy in weight_copies(k):
            copy.start()
    for h in range(2):
        at = 2 * h * NOPE
        r.wk[:, h * NOPE : (h + 1) * NOPE] = r.kv_weight[:, at : at + NOPE]
        value_weight = r.kv_weight[:, at + NOPE : at + NOPE + VDIM].astype(F32)
        r.wv[h * VDIM : (h + 1) * VDIM, :] = jnp.transpose(value_weight).astype(BF16)
    local[0].wait()
    gain = column(r.out_gain[...])

    def scale_ow(j, carry):
        at = pl.ds(pl.multiple_of(j * cols, cols), cols)
        r.owstage[:, at] = (r.owstage[:, at].astype(F32) * gain).astype(BF16)
        return carry

    lax.fori_loop(0, NT, scale_ow, 0)
    local[4].start()
    for i in range(1, NT):
        ow_copy(i).start()

    r.stat_m[...] = jnp.full(r.stat_m.shape, LOWEST, F32)
    r.stat_l[...] = jnp.zeros(r.stat_l.shape, F32)
    r.acc[...] = jnp.zeros(r.acc.shape, F32)

    def piece(slot, diagonal):
        lat = r.latbuf[slot].reshape(rows, r.latbuf.shape[-1])
        wide = r.wk.shape[0]
        compressed, both_rot = lat[:, :wide], lat[:, wide:]
        lane = lax.broadcasted_iota(jnp.int32, both_rot.shape, 1)
        keys = wide_dot(compressed, r.wk[...]).astype(BF16)
        values = nt_dot(r.wv[...], compressed).astype(BF16)
        for h in range(2):
            own_half = lane < ROPE if h == 0 else lane >= ROPE
            key_rot = jnp.where(own_half, both_rot.astype(F32), 0.0).astype(BF16)
            key = jnp.concatenate([keys[:, h * NOPE : (h + 1) * NOPE], key_rot], axis=1)
            value = values[h * VDIM : (h + 1) * VDIM]
            for b in range(NX):
                at = pl.ds(b * rows, rows)
                here = r.qbuf[b, :, h * NOPE : (h + 1) * NOPE]
                turned_here = r.qbuf[b, :, 2 * NOPE :]
                scores = nt_dot(key, jnp.concatenate([here, turned_here], axis=1)) * factor
                if diagonal:
                    key_at = x * rows + lax.broadcasted_iota(jnp.int32, scores.shape, 0)
                    query_at = b * rows + lax.broadcasted_iota(jnp.int32, scores.shape, 1)
                    allowed = key_at <= query_at
                    scores = jnp.where(allowed, scores, LOWEST)
                old = r.stat_m[h, :, at]
                new = jnp.maximum(old, jnp.max(scores, axis=0, keepdims=True))
                weights = jnp.exp2(scores - new)
                if diagonal:
                    weights = jnp.where(allowed, weights, 0.0)
                shrink = jnp.exp2(old - new)
                r.stat_m[h, :, at] = new
                r.stat_l[h, :, at] = r.stat_l[h, :, at] * shrink + jnp.sum(
                    weights, axis=0, keepdims=True
                )
                r.acc[h, :, at] = r.acc[h, :, at] * shrink + wide_dot(value, weights.astype(BF16))

    def arrive(slot, forward_to, to):
        for chunk in range(CHUNKS):
            ring(0, slot, chunk, to).wait_recv()
            if forward_to is not None:
                ring(slot, forward_to, chunk, to).start()
            pair(slot, chunk, core).start()

    def use(slot, needed):
        for chunk in range(CHUNKS):
            pair(slot, chunk, 1 - core).wait_recv()

        @pl.when(needed)
        def _():
            piece(slot, False)

    def both(d):
        def one(i, carry):
            slot = jnp.where(i == 0, d, far + d)
            source = jnp.where(i == 0, z - d, z + d - nz)
            use(slot, source >= 0)
            return carry

        return one

    def hop(d, way, part):
        of = lax.rem(z - (d - 1) + nz, nz) if way == 0 else lax.rem(z + d - 1, nz)
        ref = (r.gubuf if part == 0 else r.dnbuf).at[of]
        to = up if way == 0 else down
        return remote(ref, ref, r.hop_send.at[d, way, part], r.hop_recv.at[d, way, part], to)

    def hop_in(d, way, part):
        of = lax.rem(z - d + nz, nz) if way == 0 else lax.rem(z + d, nz)
        ref = (r.gubuf if part == 0 else r.dnbuf).at[of]
        to = up if way == 0 else down
        return remote(ref, ref, r.hop_send.at[d, way, part], r.hop_recv.at[d, way, part], to)

    def in_hop(d):
        return [(way, part) for part in range(2) for way in range(2) if d < far or way == part]

    def hop_first():
        for k in range(1, NX):
            for copy in weight_copies(k):
                copy.wait_recv()
        local[1].wait()
        local[3].wait()
        for way, part in in_hop(1):
            hop(1, way, part).start()

    def hop_on(d):
        for way, part in in_hop(d):
            hop_in(d, way, part).wait_recv()
            if d < far and (way, part) in in_hop(d + 1):
                hop(d + 1, way, part).start()

    def hop_latent(d):
        arrive(d, d + 1 if d < far else None, up)
        if d < far:
            arrive(far + d, far + d + 1 if d < far - 1 else None, down)

    hop_latent(1)
    gq.near(0)
    gq.near(1)
    hop_latent(2)
    gq.far(0)
    gq.far(1)
    piece(0, True)
    if far > 2:
        lax.fori_loop(0, 2, both(1), 0)
        hop_latent(3)
    for d in range(2, far - 1):
        lax.fori_loop(0, 2, both(d), 0)
    hop_first()
    if far > 3:
        hop_latent(4)
    lax.fori_loop(0, 2, both(far - 1), 0)
    use(far, z - far >= 0)

    for b in range(NX):
        at = pl.ds(b * rows, rows)
        for h in range(2):
            total = r.stat_l[h, :, at]
            inverse = jnp.where(total > 0.0, 1.0 / jnp.where(total > 0.0, total, 1.0), 0.0)
            r.osend[b, h * VDIM : (h + 1) * VDIM] = (r.acc[h, :, at] * inverse).astype(BF16)
            r.ssend[b, h : h + 1] = r.stat_m[h, :, at]
            r.ssend[b, 2 + h : 3 + h] = total

    def o_copy(k):
        to = lax.rem(x + k, NX)
        return remote(r.osend.at[to], r.orecv.at[k], r.o_send.at[k], r.o_recv.at[k], along_x(k))

    def s_copy(k):
        to = lax.rem(x + k, NX)
        return remote(r.ssend.at[to], r.srecv.at[k], r.s_send.at[k], r.s_recv.at[k], along_x(k))

    for k in range(1, NX):
        s_copy(k).start()
        o_copy(k).start()
    for k in range(1, NX):
        s_copy(k).wait_recv()
        o_copy(k).wait_recv()
    width = 2 * VDIM
    stats = [r.ssend[x]] + [r.srecv[k] for k in range(1, NX)]
    for h in range(2):
        outs = [r.osend[x, h * VDIM : (h + 1) * VDIM]] + [
            r.orecv[k, h * VDIM : (h + 1) * VDIM] for k in range(1, NX)
        ]
        top = functools.reduce(jnp.maximum, [s[h : h + 1] for s in stats])
        shares = [s[2 + h : 3 + h] * jnp.exp2(s[h : h + 1] - top) for s in stats]
        inverse = 1.0 / sum(shares)
        mixed = sum(o.astype(F32) * (w * inverse) for o, w in zip(outs, shares))
        at = pl.ds(pl.multiple_of(tp * width + h * VDIM, VDIM), VDIM)
        r.att[:, at] = jnp.transpose(mixed).astype(BF16)

    def att_piece(own_core):
        def ref(k, half):
            of = lax.rem(y + k, NY) * NC + own_core
            where = pl.ds(pl.multiple_of(of * width, width), width)
            at = pl.ds(0, rows) if half is None else pl.ds(half * (rows // 2), rows // 2)
            return r.att.at[at, where]

        return ref

    ga = Gather4(att_piece(core), r.ga_send, r.ga_recv, 0, along_y(1), along_y(3))

    def swap(piece, send, recv, index):
        k, half = ((0, None), (3, None), (1, None), (2, 0), (2, 1))[index]
        mine, theirs = piece(core)(k, half), piece(1 - core)(k, half)
        out = functools.partial(remote, mine, mine, send.at[index], recv.at[index], partner)
        come = functools.partial(remote, theirs, theirs, send.at[index], recv.at[index], partner)
        return out, come

    swaps = [swap(att_piece, r.sa_send.at[0], r.sa_recv.at[0], i) for i in range(5)]
    ga.start()
    swaps[0][0]().start()
    ga.near(0)
    swaps[1][0]().start()
    ga.near(1)
    swaps[2][0]().start()
    hop_on(1)
    ga.far(0)
    swaps[3][0]().start()
    ga.far(1)
    swaps[4][0]().start()
    for i in range(1, NT):
        ow_copy(i).wait_recv()
    local[4].wait()
    local[2].wait()
    for out, come in swaps:
        come().wait_recv()

    att = r.att[...]
    att_wide = att.astype(F32)
    scale = lax.rsqrt(jnp.mean(att_wide * att_wide, axis=1, keepdims=True) + EPSILON)
    attn_sum = wide_dot(att, r.owbuf[...].reshape(att.shape[1], cols)) * scale
    r.mid[x, :, own_cols] = (r.residbuf[...].astype(F32) + attn_sum).astype(BF16)

    def mid_piece(axis, at_x, at_y, own_core, first):
        def ref(k, half):
            of_x = lax.rem(x + at_x + (k if axis == 0 else 0), NX)
            of_y = lax.rem(y + at_y + (k if axis == 1 else 0), NY)
            where = pl.ds(pl.multiple_of((of_y * NC + own_core) * cols, cols), cols)
            quarter = rows // 4
            at = pl.ds(first * 2 * quarter, 2 * quarter)
            if half is not None:
                at = pl.ds((first * 2 + half) * quarter, quarter)
            return r.mid.at[of_x, at, where]

        return ref

    def plane_ring(index, axis, at_x, at_y, first):
        piece_of = functools.partial(lambda c: mid_piece(axis, at_x, at_y, c, first))
        plus, minus = (along_x(1), along_x(3)) if axis == 0 else (along_y(1), along_y(3))
        g = Gather4(piece_of(core), r.gm_send, r.gm_recv, index, plus, minus)
        return g, [swap(piece_of, r.sm_send.at[index], r.sm_recv.at[index], i) for i in range(5)]

    offsets = (0, 3, 1, 2)
    first_rings = [plane_ring(0, 0, 0, 0, 0), plane_ring(1, 1, 0, 0, 1)]
    second_rings = [
        [plane_ring(2 + i, 1, k, 0, 0), plane_ring(6 + i, 0, 0, k, 1)] for i, k in enumerate(offsets)
    ]
    for g, s in first_rings:
        g.start()
        s[0][0]().start()
    for g, s in second_rings[0]:
        g.start()
    for way in range(2):
        for i, (g, s) in enumerate(first_rings):
            g.near(way)
            second_rings[1 + way][i][0].start()
            s[1 + way][0]().start()
    for way in range(2):
        for g, s in second_rings[0]:
            g.near(way)
            s[1 + way][0]().start()
    for i, (g, s) in enumerate(first_rings):
        for half in range(2):
            g.far(half)
            s[3 + half][0]().start()
        second_rings[3][i][0].start()
    hop_on(2)
    for j in range(1, 4):
        for way in range(2):
            for g, s in second_rings[j]:
                g.near(way)
                s[1 + way][0]().start()
        for half in range(2):
            for g, s in second_rings[j - 1]:
                g.far(half)
                s[3 + half][0]().start()
        if j == 2 and far > 3:
            hop_on(3)
    for half in range(2):
        for g, s in second_rings[3]:
            g.far(half)
            s[3 + half][0]().start()
    if far == 2:
        pass
    else:
        hop_on(far)
    rings = first_rings + [pair_of for both_of in second_rings for pair_of in both_of]
    for i, (g, s) in enumerate(rings):
        for j, (out, come) in enumerate(s):
            if j > 0 or i < 2:
                come().wait_recv()

    def mixer(b, carry):
        squares = jnp.zeros((rows, 128), F32)
        for j in range(r.mid.shape[2] // 128):
            v = r.mid[b, :, j * 128 : (j + 1) * 128].astype(F32)
            squares = squares + v * v
        mean = jnp.sum(squares, axis=1, keepdims=True) / r.mid.shape[2]
        row_scale = lax.rsqrt(mean + EPSILON)
        mid = r.mid[b]
        gu = wide_dot(mid, r.gubuf[...].reshape(mid.shape[1], 2 * UNIT)) * row_scale
        gate, mixed_tile, upward = gu[:, :128], gu[:, 128:256], gu[:, 256:]
        first = gate / (1.0 + jnp.exp(-gate)) * upward
        second = (mixed_tile / (1.0 + jnp.exp(-mixed_tile)))[:, :64] * mixed_tile[:, 64:]
        hidden = jnp.concatenate([first, second], axis=1).astype(BF16)
        n = r.dnbuf.shape[-1]
        for zz in range(nz):
            w = jnp.concatenate([r.dnbuf[zz, i] for i in range(NX)], axis=1)
            terms = wide_dot(hidden, w).astype(BF16).reshape(NY, NC, share, NX * n)
            for c in range(NC):
                r.part[c, b, :, :, zz * NX * n : (zz + 1) * NX * n] = terms[:, c]
        core_copy(b).start()
        return carry

    def core_copy(b):
        return remote(r.part.at[1 - core, b], r.pairbuf.at[b], r.pc_send.at[b], r.pc_recv.at[b], partner)

    lax.fori_loop(0, NX, mixer, 0)

    def core_sum(b, carry):
        core_copy(b).wait_recv()
        for i in range(NY):
            ref = r.part.at[core, b, i]
            ref[...] = (ref[...].astype(F32) + r.pairbuf[b, i].astype(F32)).astype(BF16)
        return carry

    lax.fori_loop(0, NX, core_sum, 0)

    depth = r.part.shape[-1] // 2

    def block(axis, of_x, of_y, first):
        def ref(k, half):
            bx = lax.rem(of_x + (k if axis == 0 else 0), NX)
            by = lax.rem(of_y + (k if axis == 1 else 0), NY)
            at = pl.ds(first * depth, depth)
            if half is not None:
                at = pl.ds(first * depth + half * (depth // 2), depth // 2)
            return r.part.at[core, bx, by, :, at]

        return ref

    def scatter(index, axis, of_x, of_y, first):
        plus, minus = (along_x(1), along_x(3)) if axis == 0 else (along_y(1), along_y(3))
        return Scatter4(
            block(axis, of_x, of_y, first),
            r.half_in.at[index],
            r.whole_in.at[index],
            r.rs_send,
            r.rs_recv,
            index,
            plus,
            minus,
        )

    order = (1, 3, 2, 0)
    steps = [
        [scatter(i, 1, x + k, y, 0), scatter(4 + i, 0, x, y + k, 1)] for i, k in enumerate(order)
    ]
    ends = [scatter(8, 0, x, y, 0), scatter(9, 1, x, y, 1)]
    for both_of in steps:
        for s in both_of:
            s.start()
    for both_of in steps:
        for s in both_of:
            s.near(0)
            s.near(1)
    for j, both_of in enumerate(steps):
        for s in both_of:
            s.finish()
        if j == 2:
            for s in ends:
                s.start()
    for s in ends:
        s.near(0)
        s.near(1)
    own_rows = pl.ds(pl.multiple_of(tp * share, share), share)
    for first, s in enumerate(ends):
        at = slice(first * depth, (first + 1) * depth)
        r.out[:, at] = (s.total() + r.mid[x, own_rows, at].astype(F32)).astype(BF16)

    for k in range(1, NX):
        o_copy(k).wait_send()
        s_copy(k).wait_send()
        for copy in weight_copies(k):
            copy.wait_send()
    for i in range(1, NT):
        ow_copy(i).wait_send()
    for slot in range(1, nz):
        for chunk in range(CHUNKS):
            ring(0, slot, chunk, up).wait_send()
            pair(slot, chunk, core).wait_send()
    for d in range(1, far + 1):
        for way, part in in_hop(d):
            hop(d, way, part).wait_send()
    gq.done()
    ga.done()
    for out, come in swaps:
        out().wait_send()
    for i, (g, s) in enumerate(rings):
        g.done()
        for j, (out, come) in enumerate(s):
            if j > 0 or i < 2:
                out().wait_send()
    for b in range(NX):
        core_copy(b).wait_send()
    for both_of in [*steps, ends]:
        for s in both_of:
            s.done()


def layer(inputs, whole):
    nz = lax.axis_size("sp") // NX
    vmem = pl.BlockSpec(memory_space=pltpu.VMEM)
    anywhere = pl.BlockSpec(memory_space=pl.ANY)
    rows, wide = inputs["latent"].shape
    depth = inputs["gate"].shape[0]
    n = inputs["dn"].shape[-1]
    dim = inputs["resid"].shape[1]
    share = rows // NT
    cols = dim // NT
    lat = (NC, CHUNKS, rows // NC // CHUNKS, wide + 2 * ROPE)
    gu, dn = (NX, depth, 2 * UNIT), (NX, UNIT, n)
    heads = 2 * VDIM
    buffers = {
        "latbuf": ((nz, *lat), BF16),
        "qbuf": ((NX, rows, 2 * (NOPE + ROPE)), BF16),
        "wk": ((wide, 2 * NOPE), BF16),
        "wv": ((heads, wide), BF16),
        "gustage": (gu, BF16),
        "owstage": ((heads, dim), BF16),
        "acc": ((2, VDIM, NX * rows), F32),
        "stat_m": ((2, 1, NX * rows), F32),
        "stat_l": ((2, 1, NX * rows), F32),
        "osend": ((NX, 2 * VDIM, rows), BF16),
        "orecv": ((NX, 2 * VDIM, rows), BF16),
        "ssend": ((NX, 8, rows), F32),
        "srecv": ((NX, 8, rows), F32),
        "gubuf": ((nz, *gu), BF16),
        "dnbuf": ((nz, *dn), BF16),
        "owbuf": ((NT, heads, cols), BF16),
        "residbuf": ((rows, cols), BF16),
        "att": ((rows, NT * 2 * VDIM), BF16),
        "mid": ((NX, rows, dim), BF16),
        "part": ((NC, NX, NY, share, dim), BF16),
        "pairbuf": ((NX, NY, share, dim), BF16),
        "half_in": ((10, 2, share, dim // 4), BF16),
        "whole_in": ((10, 2, share, dim // 2), BF16),
    }
    semaphores = {
        "local_sem": (5,),
        "ring_send": (nz, CHUNKS),
        "ring_recv": (nz, CHUNKS),
        "pair_send": (nz, CHUNKS),
        "pair_recv": (nz, CHUNKS),
        "gq_send": (1, 4),
        "gq_recv": (1, 4),
        "wx_send": (NX, 2),
        "wx_recv": (NX, 2),
        "ow_send": (NT,),
        "ow_recv": (NT,),
        "hop_send": (nz, 2, 2),
        "hop_recv": (nz, 2, 2),
        "o_send": (NX,),
        "o_recv": (NX,),
        "s_send": (NX,),
        "s_recv": (NX,),
        "ga_send": (1, 4),
        "ga_recv": (1, 4),
        "sa_send": (1, 5),
        "sa_recv": (1, 5),
        "gm_send": (10, 4),
        "gm_recv": (10, 4),
        "sm_send": (10, 5),
        "sm_recv": (10, 5),
        "pc_send": (NX,),
        "pc_recv": (NX,),
        "rs_send": (10, 4),
        "rs_recv": (10, 4),
    }
    names = [*inputs, "out", *buffers, *semaphores]
    return pl.pallas_call(
        functools.partial(layer_kernel, nz, names),
        out_shape=jax.ShapeDtypeStruct((share, dim), BF16),
        in_specs=[anywhere if name in whole else vmem for name in inputs],
        out_specs=vmem,
        scratch_shapes=[pltpu.VMEM(*b) for b in buffers.values()]
        + [pltpu.SemaphoreType.DMA(s) for s in semaphores.values()],
        compiler_params=pltpu.CompilerParams(
            collective_id=0, has_side_effects=True, vmem_limit_bytes=62 * 1024 * 1024
        ),
    )(*inputs.values())


def body(
    resid,
    queries,
    latent,
    rope_key,
    lat_gain,
    kv_weight,
    out_gain,
    out_weight,
    ffn_gain,
    gate_weight,
    up_weight,
    down_weight,
):
    rows = latent.shape[0]
    half = ROPE // 2
    frequency = THETA ** (-np.arange(half) / half)

    def turns(places):
        angle = places[:, None] * frequency
        return jnp.asarray(np.concatenate([np.cos(angle), np.sin(angle)], axis=1), F32)

    inputs = {
        "latent": latent,
        "rope_key": rope_key,
        "queries": queries,
        "lat_gain": lat_gain[None, :],
        "kv_weight": kv_weight,
        "gate": gate_weight,
        "upward": up_weight,
        "ffn_gain": ffn_gain.reshape(-1, gate_weight.shape[0]),
        "out_gain": out_gain[None, :],
        "first_turn": turns(np.arange(lax.axis_size("sp")) * rows),
        "row_turn": turns(np.arange(rows)),
        "dn": down_weight.reshape(NX, UNIT, down_weight.shape[1]),
        "ow": out_weight,
        "resid": resid,
    }
    return layer(inputs, ("dn", "ow", "resid"))


def solution(mesh):
    placed = (
        P("sp", None),
        P("sp", "tp"),
        P("sp", None),
        P("sp", None),
        P(),
        P(None, "tp"),
        P("tp"),
        P("tp", None),
        P(),
        P("sp", "tp"),
        P("sp", "tp"),
        P("tp", "sp"),
    )
    return jax.shard_map(
        body, mesh=mesh, in_specs=placed, out_specs=P(("sp", "tp"), None), check_vma=False
    )
```

```python
import functools
import math

import jax
import jax.numpy as jnp
import numpy as np
from jax import lax
from jax.experimental import pallas as pl
from jax.experimental.pallas import tpu as pltpu
from jax.sharding import PartitionSpec as P

NOPE = 128
ROPE = 64
VDIM = 128
NX = 4
NY = 4
NC = 2
NT = NY * NC
CHUNKS = 2
UNIT = 192

EPSILON = 1e-06
THETA = 10000.0
LOWEST = -1e30
MESH = pl.DeviceIdType.MESH
F32 = jnp.float32
BF16 = jnp.bfloat16


def norm_rows(values, gain):
    wide = values.astype(F32)
    return wide * lax.rsqrt(jnp.mean(wide * wide, axis=-1, keepdims=True) + EPSILON) * gain


def column(row):
    return jnp.transpose(jnp.broadcast_to(row, (128, row.shape[1])))[:, :1]


def turned(values, cosine, sine):
    half = values.shape[-1] // 2
    first, second = values[:, :half], values[:, half:]
    return jnp.concatenate(
        [first * cosine - second * sine, first * sine + second * cosine], axis=1
    )


def nt_dot(a, b):
    return lax.dot_general(a, b, (((1,), (1,)), ((), ())), preferred_element_type=F32)


def wide_dot(a, b):
    return jnp.dot(a, b, preferred_element_type=F32)


class Refs:
    def __init__(self, names, values):
        self.__dict__.update(zip(names, values, strict=True))


def remote(src, dst, send, recv, to):
    return pltpu.make_async_remote_copy(
        src_ref=src, dst_ref=dst, send_sem=send, recv_sem=recv, device_id=to, device_id_type=MESH
    )


class Gather4:
    def __init__(self, piece, send, recv, index, plus, minus):
        self.piece, self.send, self.recv, self.index = piece, send, recv, index
        self.plus, self.minus = plus, minus

    def copy(self, way, k, half):
        to = self.plus if way in (0, 2) else self.minus
        ref = self.piece(k, half)
        return remote(ref, ref, self.send.at[self.index, way], self.recv.at[self.index, way], to)

    def start(self):
        self.copy(0, 0, None).start()
        self.copy(1, 0, None).start()

    def near(self, way):
        self.copy(way, 3 if way == 0 else 1, None).wait_recv()
        self.copy(way + 2, 3 if way == 0 else 1, way).start()

    def far(self, half):
        self.copy(half + 2, 2, half).wait_recv()

    def done(self):
        self.copy(0, 0, None).wait_send()
        self.copy(1, 0, None).wait_send()
        self.copy(2, 3, 0).wait_send()
        self.copy(3, 1, 1).wait_send()


class Scatter4:
    def __init__(self, block, half_in, whole_in, send, recv, index, plus, minus):
        self.block, self.half_in, self.whole_in = block, half_in, whole_in
        self.send, self.recv, self.index = send, recv, index
        self.plus, self.minus = plus, minus

    def half(self, h):
        to = self.minus if h == 0 else self.plus
        return remote(
            self.block(2, h), self.half_in.at[h], self.send.at[self.index, h], self.recv.at[self.index, h], to
        )

    def whole(self, h):
        to, k = (self.minus, 3) if h == 0 else (self.plus, 1)
        return remote(
            self.block(k, None),
            self.whole_in.at[h],
            self.send.at[self.index, 2 + h],
            self.recv.at[self.index, 2 + h],
            to,
        )

    def start(self):
        self.half(0).start()
        self.half(1).start()

    def near(self, h):
        self.half(h).wait_recv()
        ref = self.block(3 if h == 0 else 1, h)
        ref[...] = (ref[...].astype(F32) + self.half_in[h].astype(F32)).astype(BF16)
        self.whole(h).start()

    def total(self):
        self.whole(0).wait_recv()
        self.whole(1).wait_recv()
        ref = self.block(0, None)
        return ref[...].astype(F32) + self.whole_in[0].astype(F32) + self.whole_in[1].astype(F32)

    def finish(self):
        self.block(0, None)[...] = self.total().astype(BF16)

    def done(self):
        for h in range(2):
            self.half(h).wait_send()
            self.whole(h).wait_send()


def layer_kernel(nz, names, *values):
    r = Refs(names, values)
    sp, tp = lax.axis_index("sp"), lax.axis_index("tp")
    z, x = sp // NX, lax.rem(sp, NX)
    y, core = tp // NC, lax.rem(tp, NC)
    up = (lax.rem(z + 1, nz) * NX + x, tp)
    down = (lax.rem(z + nz - 1, nz) * NX + x, tp)
    partner = (sp, tp + 1 - 2 * core)
    rows = r.latent.shape[0]
    far = nz // 2
    factor = (1.0 / math.sqrt(NOPE + ROPE)) * math.log2(math.e)
    dim = r.resid.shape[1]
    cols = dim // NT
    share = rows // NT

    def along_x(k):
        return (z * NX + lax.rem(x + k, NX), tp)

    def along_y(k, other=0):
        to_core = core if other == 0 else 1 - core
        return (sp, lax.rem(y + k, NY) * NC + to_core)

    peers = [up, down, partner]
    peers += [along_x(k) for k in range(1, NX)]
    peers += [along_y(k) for k in range(1, NY)]
    peers += [along_y(k, 1) for k in range(1, NY)]
    barrier = pltpu.get_barrier_semaphore()
    for peer in peers:
        pl.semaphore_signal(barrier, inc=1, device_id=peer, device_id_type=MESH)

    own_cols = pl.ds(pl.multiple_of(tp * cols, cols), cols)
    local = [
        pltpu.make_async_copy(r.ow, r.owstage, r.local_sem.at[0]),
        pltpu.make_async_copy(r.dn.at[x], r.dnbuf.at[z, x], r.local_sem.at[1]),
        pltpu.make_async_copy(r.resid.at[:, own_cols], r.residbuf, r.local_sem.at[2]),
        pltpu.make_async_copy(r.gustage.at[x], r.gubuf.at[z, x], r.local_sem.at[3]),
        pltpu.make_async_copy(r.owstage.at[:, own_cols], r.owbuf.at[tp], r.local_sem.at[4]),
    ]
    for copy in local[:3]:
        copy.start()

    half = ROPE // 2
    base, step = r.first_turn[pl.ds(sp, 1), :], r.row_turn[...]
    base_cos, base_sin = base[:, :half], base[:, half:]
    step_cos, step_sin = step[:, :half], step[:, half:]
    cosine = base_cos * step_cos - base_sin * step_sin
    sine = base_sin * step_cos + base_cos * step_sin
    key_rot = turned(r.rope_key[...].astype(F32), cosine, sine)
    lat = jnp.concatenate([norm_rows(r.latent[...], r.lat_gain[...]), key_rot, key_rot], axis=1)
    r.latbuf[0] = lat.astype(BF16).reshape(r.latbuf.shape[1:])
    query = r.queries[...].astype(F32)
    one = NOPE + ROPE
    parts = [query[:, h * one : h * one + NOPE] for h in range(2)]
    parts += [turned(query[:, h * one + NOPE : (h + 1) * one], cosine, sine) for h in range(2)]
    own_rows_at = pl.ds(pl.multiple_of(x * rows, rows), rows)
    r.qbuf[:, own_rows_at] = jnp.transpose(jnp.concatenate(parts, axis=1)).astype(BF16)
    pl.semaphore_wait(barrier, len(peers))

    def ring(src_slot, dst_slot, chunk, to):
        src = r.latbuf.at[src_slot, core, chunk]
        dst = r.latbuf.at[dst_slot, core, chunk]
        return remote(src, dst, r.ring_send.at[dst_slot, chunk], r.ring_recv.at[dst_slot, chunk], to)

    def pair(slot, chunk, side):
        ref = r.latbuf.at[slot, side, chunk]
        return remote(ref, ref, r.pair_send.at[slot, chunk], r.pair_recv.at[slot, chunk], partner)

    def q_piece(k, half):
        channels = r.qbuf.shape[0]
        at = pl.ds(0, channels) if half is None else pl.ds(half * (channels // 2), channels // 2)
        return r.qbuf.at[at, pl.ds(pl.multiple_of(lax.rem(x + k, NX) * rows, rows), rows)]

    gq = Gather4(q_piece, r.gq_send, r.gq_recv, 0, along_x(1), along_x(3))

    def weight_copies(k):
        to = lax.rem(x + k, NX)
        return [
            remote(r.gustage.at[to], r.gubuf.at[z, x], r.wx_send.at[k, 0], r.wx_recv.at[k, 0], along_x(k)),
            remote(r.dn.at[to], r.dnbuf.at[z, x], r.wx_send.at[k, 1], r.wx_recv.at[k, 1], along_x(k)),
        ]

    def ow_copy(i):
        k, other = i // 2, i % 2
        to = along_y(k, other)
        src = r.owstage.at[:, pl.ds(pl.multiple_of(to[1] * cols, cols), cols)]
        return remote(src, r.owbuf.at[tp], r.ow_send.at[i], r.ow_recv.at[i], to)

    for chunk in range(CHUNKS):
        ring(0, 1, chunk, up).start()
        ring(0, far + 1, chunk, down).start()
    gq.start()

    gain = column(r.ffn_gain[pl.ds(sp, 1), :])
    gate, upward = r.gate[...].astype(F32) * gain, r.upward[...].astype(F32) * gain
    for i in range(NX):
        lo, mid_lo, hi = i * UNIT, i * UNIT + 128, (i + 1) * UNIT
        tiles = [gate[:, lo:mid_lo], gate[:, mid_lo:hi], upward[:, mid_lo:hi], upward[:, lo:mid_lo]]
        r.gustage[i] = jnp.concatenate(tiles, axis=1).astype(BF16)
    local[3].start()
    for k in (1, 3):
        for copy in weight_copies(k):
            copy.start()
    for h in range(2):
        at = 2 * h * NOPE
        r.wk[:, h * NOPE : (h + 1) * NOPE] = r.kv_weight[:, at : at + NOPE]
        value_weight = r.kv_weight[:, at + NOPE : at + NOPE + VDIM].astype(F32)
        r.wv[h * VDIM : (h + 1) * VDIM, :] = jnp.transpose(value_weight).astype(BF16)
    local[0].wait()
    gain = column(r.out_gain[...])

    def scale_ow(j, carry):
        at = pl.ds(pl.multiple_of(j * cols, cols), cols)
        r.owstage[:, at] = (r.owstage[:, at].astype(F32) * gain).astype(BF16)
        return carry

    lax.fori_loop(0, NT, scale_ow, 0)
    local[4].start()
    for i in range(1, NT):
        ow_copy(i).start()

    r.stat_m[...] = jnp.full(r.stat_m.shape, LOWEST, F32)
    r.stat_l[...] = jnp.zeros(r.stat_l.shape, F32)
    r.acc[...] = jnp.zeros(r.acc.shape, F32)

    def piece(slot, diagonal):
        lat = r.latbuf[slot].reshape(rows, r.latbuf.shape[-1])
        wide = r.wk.shape[0]
        compressed, both_rot = lat[:, :wide], lat[:, wide:]
        lane = lax.broadcasted_iota(jnp.int32, both_rot.shape, 1)
        keys = wide_dot(compressed, r.wk[...]).astype(BF16)
        values = nt_dot(r.wv[...], compressed).astype(BF16)
        for h in range(2):
            own_half = lane < ROPE if h == 0 else lane >= ROPE
            key_rot = jnp.where(own_half, both_rot.astype(F32), 0.0).astype(BF16)
            key = jnp.concatenate([keys[:, h * NOPE : (h + 1) * NOPE], key_rot], axis=1)
            query = jnp.concatenate(
                [r.qbuf[h * NOPE : (h + 1) * NOPE], r.qbuf[2 * NOPE :]], axis=0
            )
            r.scores[h] = wide_dot(key, query)
        for h in range(2):
            for b in range(NX * rows // 128):
                at = pl.ds(b * 128, 128)
                scores = r.scores[h, :, at] * factor
                if diagonal:
                    key_at = x * rows + lax.broadcasted_iota(jnp.int32, scores.shape, 0)
                    query_at = b * 128 + lax.broadcasted_iota(jnp.int32, scores.shape, 1)
                    allowed = key_at <= query_at
                    scores = jnp.where(allowed, scores, LOWEST)
                old = r.stat_m[h, :, at]
                new = jnp.maximum(old, jnp.max(scores, axis=0, keepdims=True))
                weights = jnp.exp2(scores - new)
                if diagonal:
                    weights = jnp.where(allowed, weights, 0.0)
                shrink = jnp.exp2(old - new)
                r.stat_m[h, :, at] = new
                r.stat_a[h, :, at] = shrink
                r.stat_l[h, :, at] = r.stat_l[h, :, at] * shrink + jnp.sum(
                    weights, axis=0, keepdims=True
                )
                r.weights[h, :, at] = weights.astype(BF16)
            value = values[h * VDIM : (h + 1) * VDIM]
            r.acc[h] = r.acc[h] * r.stat_a[h] + wide_dot(value, r.weights[h])

    def arrive(slot, forward_to, to):
        for chunk in range(CHUNKS):
            ring(0, slot, chunk, to).wait_recv()
            if forward_to is not None:
                ring(slot, forward_to, chunk, to).start()
            pair(slot, chunk, core).start()

    def use(slot, needed):
        for chunk in range(CHUNKS):
            pair(slot, chunk, 1 - core).wait_recv()

        @pl.when(needed)
        def _():
            piece(slot, False)

    def both(d):
        def one(i, carry):
            slot = jnp.where(i == 0, d, far + d)
            source = jnp.where(i == 0, z - d, z + d - nz)
            use(slot, source >= 0)
            return carry

        return one

    def hop(d, way, part):
        of = lax.rem(z - (d - 1) + nz, nz) if way == 0 else lax.rem(z + d - 1, nz)
        ref = (r.gubuf if part == 0 else r.dnbuf).at[of]
        to = up if way == 0 else down
        return remote(ref, ref, r.hop_send.at[d, way, part], r.hop_recv.at[d, way, part], to)

    def hop_in(d, way, part):
        of = lax.rem(z - d + nz, nz) if way == 0 else lax.rem(z + d, nz)
        ref = (r.gubuf if part == 0 else r.dnbuf).at[of]
        to = up if way == 0 else down
        return remote(ref, ref, r.hop_send.at[d, way, part], r.hop_recv.at[d, way, part], to)

    def in_hop(d):
        return [(way, part) for part in range(2) for way in range(2) if d < far or way == part]

    def hop_first():
        for k in range(1, NX):
            for copy in weight_copies(k):
                copy.wait_recv()
        local[1].wait()
        local[3].wait()
        for way, part in in_hop(1):
            hop(1, way, part).start()

    def hop_on(d, only=None):
        for way, part in in_hop(d):
            if only is not None and part != only:
                continue
            hop_in(d, way, part).wait_recv()
            if d < far and (way, part) in in_hop(d + 1):
                hop(d + 1, way, part).start()

    def hop_latent(d):
        arrive(d, d + 1 if d < far else None, up)
        if d < far:
            arrive(far + d, far + d + 1 if d < far - 1 else None, down)

    hop_latent(1)
    gq.near(0)
    gq.near(1)
    for copy in weight_copies(2):
        copy.start()
    hop_latent(2)
    gq.far(0)
    gq.far(1)
    piece(0, True)
    if far > 2:
        lax.fori_loop(0, 2, both(1), 0)
        hop_latent(3)
    for d in range(2, far - 1):
        lax.fori_loop(0, 2, both(d), 0)
    hop_first()
    if far > 3:
        hop_latent(4)
    lax.fori_loop(0, 2, both(far - 1), 0)
    use(far, z - far >= 0)

    for b in range(NX):
        at = pl.ds(b * rows, rows)
        for h in range(2):
            total = r.stat_l[h, :, at]
            inverse = jnp.where(total > 0.0, 1.0 / jnp.where(total > 0.0, total, 1.0), 0.0)
            r.osend[b, h * VDIM : (h + 1) * VDIM] = (r.acc[h, :, at] * inverse).astype(BF16)
            r.ssend[b, h : h + 1] = r.stat_m[h, :, at]
            r.ssend[b, 2 + h : 3 + h] = total

    def o_copy(k):
        to = lax.rem(x + k, NX)
        return remote(r.osend.at[to], r.orecv.at[k], r.o_send.at[k], r.o_recv.at[k], along_x(k))

    def s_copy(k):
        to = lax.rem(x + k, NX)
        return remote(r.ssend.at[to], r.srecv.at[k], r.s_send.at[k], r.s_recv.at[k], along_x(k))

    for k in range(1, NX):
        s_copy(k).start()
        o_copy(k).start()
    for k in range(1, NX):
        s_copy(k).wait_recv()
        o_copy(k).wait_recv()
    width = 2 * VDIM
    stats = [r.ssend[x]] + [r.srecv[k] for k in range(1, NX)]
    for h in range(2):
        outs = [r.osend[x, h * VDIM : (h + 1) * VDIM]] + [
            r.orecv[k, h * VDIM : (h + 1) * VDIM] for k in range(1, NX)
        ]
        top = functools.reduce(jnp.maximum, [s[h : h + 1] for s in stats])
        shares = [s[2 + h : 3 + h] * jnp.exp2(s[h : h + 1] - top) for s in stats]
        inverse = 1.0 / sum(shares)
        mixed = sum(o.astype(F32) * (w * inverse) for o, w in zip(outs, shares))
        at = pl.ds(pl.multiple_of(tp * width + h * VDIM, VDIM), VDIM)
        r.att[:, at] = jnp.transpose(mixed).astype(BF16)

    def att_piece(own_core):
        def ref(k, half):
            of = lax.rem(y + k, NY) * NC + own_core
            where = pl.ds(pl.multiple_of(of * width, width), width)
            at = pl.ds(0, rows) if half is None else pl.ds(half * (rows // 2), rows // 2)
            return r.att.at[at, where]

        return ref

    hop_on(1, 0)
    ga = Gather4(att_piece(core), r.ga_send, r.ga_recv, 0, along_y(1), along_y(3))

    def swap(piece, send, recv, index):
        k, half = ((0, None), (3, None), (1, None), (2, 0), (2, 1))[index]
        mine, theirs = piece(core)(k, half), piece(1 - core)(k, half)
        out = functools.partial(remote, mine, mine, send.at[index], recv.at[index], partner)
        come = functools.partial(remote, theirs, theirs, send.at[index], recv.at[index], partner)
        return out, come

    swaps = [swap(att_piece, r.sa_send.at[0], r.sa_recv.at[0], i) for i in range(5)]
    ga.start()
    swaps[0][0]().start()
    ga.near(0)
    swaps[1][0]().start()
    ga.near(1)
    swaps[2][0]().start()
    hop_on(1, 1)
    ga.far(0)
    swaps[3][0]().start()
    ga.far(1)
    swaps[4][0]().start()
    for i in range(1, NT):
        ow_copy(i).wait_recv()
    local[4].wait()
    local[2].wait()
    for out, come in swaps:
        come().wait_recv()

    att = r.att[...]
    att_wide = att.astype(F32)
    scale = lax.rsqrt(jnp.mean(att_wide * att_wide, axis=1, keepdims=True) + EPSILON)
    attn_sum = wide_dot(att, r.owbuf[...].reshape(att.shape[1], cols)) * scale
    r.mid[x, :, own_cols] = (r.residbuf[...].astype(F32) + attn_sum).astype(BF16)

    def mid_piece(axis, at_x, at_y, own_core, first):
        def ref(k, half):
            of_x = lax.rem(x + at_x + (k if axis == 0 else 0), NX)
            of_y = lax.rem(y + at_y + (k if axis == 1 else 0), NY)
            where = pl.ds(pl.multiple_of((of_y * NC + own_core) * cols, cols), cols)
            quarter = rows // 4
            at = pl.ds(first * 2 * quarter, 2 * quarter)
            if half is not None:
                at = pl.ds((first * 2 + half) * quarter, quarter)
            return r.mid.at[of_x, at, where]

        return ref

    def plane_ring(index, axis, at_x, at_y, first):
        piece_of = functools.partial(lambda c: mid_piece(axis, at_x, at_y, c, first))
        plus, minus = (along_x(1), along_x(3)) if axis == 0 else (along_y(1), along_y(3))
        g = Gather4(piece_of(core), r.gm_send, r.gm_recv, index, plus, minus)
        return g, [swap(piece_of, r.sm_send.at[index], r.sm_recv.at[index], i) for i in range(5)]

    offsets = (0, 3, 1, 2)
    first_rings = [plane_ring(0, 0, 0, 0, 0), plane_ring(1, 1, 0, 0, 1)]
    second_rings = [
        [plane_ring(2 + i, 1, k, 0, 0), plane_ring(6 + i, 0, 0, k, 1)] for i, k in enumerate(offsets)
    ]
    for g, s in first_rings:
        g.start()
        s[0][0]().start()
    for g, s in second_rings[0]:
        g.start()
    for way in range(2):
        for i, (g, s) in enumerate(first_rings):
            g.near(way)
            second_rings[1 + way][i][0].start()
            s[1 + way][0]().start()
    hop_on(2, 0)
    for way in range(2):
        for g, s in second_rings[0]:
            g.near(way)
            s[1 + way][0]().start()
    hop_on(2, 1)
    for i, (g, s) in enumerate(first_rings):
        for half in range(2):
            g.far(half)
            s[3 + half][0]().start()
        second_rings[3][i][0].start()
    for j in range(1, 4):
        for way in range(2):
            for g, s in second_rings[j]:
                g.near(way)
                s[1 + way][0]().start()
        for half in range(2):
            for g, s in second_rings[j - 1]:
                g.far(half)
                s[3 + half][0]().start()
        if j == 1 and far > 3:
            hop_on(3, 0)
        if j == 2 and far > 3:
            hop_on(3, 1)
    for half in range(2):
        for g, s in second_rings[3]:
            g.far(half)
            s[3 + half][0]().start()
    if far == 2:
        pass
    else:
        hop_on(far)
    rings = first_rings + [pair_of for both_of in second_rings for pair_of in both_of]
    for i, (g, s) in enumerate(rings):
        for j, (out, come) in enumerate(s):
            if j > 0 or i < 2:
                come().wait_recv()

    def mixer(j):
        b = lax.rem(x + ahead(j), NX)
        squares = jnp.zeros((rows, 128), F32)
        for i in range(r.mid.shape[2] // 128):
            v = r.mid[b, :, i * 128 : (i + 1) * 128].astype(F32)
            squares = squares + v * v
        mean = jnp.sum(squares, axis=1, keepdims=True) / r.mid.shape[2]
        row_scale = lax.rsqrt(mean + EPSILON)
        mid = r.mid[b]
        gu = wide_dot(mid, r.gubuf[...].reshape(mid.shape[1], 2 * UNIT)) * row_scale
        gate, mixed_tile, upward = gu[:, :128], gu[:, 128:256], gu[:, 256:]
        first = gate / (1.0 + jnp.exp(-gate)) * upward
        second = (mixed_tile / (1.0 + jnp.exp(-mixed_tile)))[:, :64] * mixed_tile[:, 64:]
        hidden = jnp.concatenate([first, second], axis=1).astype(BF16)
        n = r.dnbuf.shape[-1]
        for zz in range(nz):
            w = jnp.concatenate([r.dnbuf[zz, i] for i in range(NX)], axis=1)
            terms = wide_dot(hidden, w).astype(BF16).reshape(NY, NC, share, NX * n)
            for c in range(NC):
                r.part[c, b, :, :, zz * NX * n : (zz + 1) * NX * n] = terms[:, c]
        core_copy(j).start()

    def ahead(j):
        return jnp.where(j == 0, 2, jnp.where(j == 1, 1, jnp.where(j == 2, 3, 0)))

    def core_copy(j):
        b = lax.rem(x + ahead(j), NX)
        return remote(r.part.at[1 - core, b], r.pairbuf.at[b], r.pc_send.at[j], r.pc_recv.at[j], partner)

    def core_sum(j):
        b = lax.rem(x + ahead(j), NX)
        core_copy(j).wait_recv()
        for i in range(NY):
            ref = r.part.at[core, b, i]
            ref[...] = (ref[...].astype(F32) + r.pairbuf[b, i].astype(F32)).astype(BF16)

    depth = r.part.shape[-1] // 2

    def block(axis, of_x, of_y, first):
        def ref(k, half):
            bx = lax.rem(of_x + (k if axis == 0 else 0), NX)
            by = lax.rem(of_y + (k if axis == 1 else 0), NY)
            at = pl.ds(first * depth, depth)
            if half is not None:
                at = pl.ds(first * depth + half * (depth // 2), depth // 2)
            return r.part.at[core, bx, by, :, at]

        return ref

    def scatter(index, axis, of_x, of_y, first):
        plus, minus = (along_x(1), along_x(3)) if axis == 0 else (along_y(1), along_y(3))
        return Scatter4(
            block(axis, of_x, of_y, first),
            r.half_in.at[index],
            r.whole_in.at[index],
            r.rs_send,
            r.rs_recv,
            index,
            plus,
            minus,
        )

    def first_along_y(j):
        return scatter(j, 1, x + ahead(j), y, 0)

    def first_along_x(j):
        return scatter(4 + j, 0, x, y + ahead(j), 1)

    def stage(j, carry):
        @pl.when(j < NX)
        def _():
            mixer(j)

        @pl.when(j >= 1)
        def _():
            core_sum(j - 1)
            first_along_y(j - 1).start()

        @pl.when(j == 1)
        def _():
            for i in range(NY):
                first_along_x(i).start()

        @pl.when(j >= 2)
        def _():
            first_along_y(j - 2).near(0)
            first_along_y(j - 2).near(1)

        @pl.when(j == NX - 1)
        def _():
            for i in range(NY):
                first_along_x(i).near(0)
                first_along_x(i).near(1)

        return carry

    lax.fori_loop(0, NX + 1, stage, 0)
    steps = [[first_along_y(j), first_along_x(j)] for j in range(NX)]
    ends = [scatter(8, 0, x, y, 0), scatter(9, 1, x, y, 1)]
    first_along_y(NX - 1).near(0)
    first_along_y(NX - 1).near(1)
    for j, both_of in enumerate(steps):
        for s in both_of:
            s.finish()
        if j == 0:
            for s in ends:
                s.start()
    for s in ends:
        s.near(0)
        s.near(1)
    own_rows = pl.ds(pl.multiple_of(tp * share, share), share)
    for first, s in enumerate(ends):
        at = slice(first * depth, (first + 1) * depth)
        r.out[:, at] = (s.total() + r.mid[x, own_rows, at].astype(F32)).astype(BF16)

    for k in range(1, NX):
        o_copy(k).wait_send()
        s_copy(k).wait_send()
        for copy in weight_copies(k):
            copy.wait_send()
    for i in range(1, NT):
        ow_copy(i).wait_send()
    for slot in range(1, nz):
        for chunk in range(CHUNKS):
            ring(0, slot, chunk, up).wait_send()
            pair(slot, chunk, core).wait_send()
    for d in range(1, far + 1):
        for way, part in in_hop(d):
            hop(d, way, part).wait_send()
    gq.done()
    ga.done()
    for out, come in swaps:
        out().wait_send()
    for i, (g, s) in enumerate(rings):
        g.done()
        for j, (out, come) in enumerate(s):
            if j > 0 or i < 2:
                out().wait_send()
    for j in range(NX):
        core_copy(j).wait_send()
    for both_of in [*steps, ends]:
        for s in both_of:
            s.done()


def layer(inputs, whole):
    nz = lax.axis_size("sp") // NX
    vmem = pl.BlockSpec(memory_space=pltpu.VMEM)
    anywhere = pl.BlockSpec(memory_space=pl.ANY)
    rows, wide = inputs["latent"].shape
    depth = inputs["gate"].shape[0]
    n = inputs["dn"].shape[-1]
    dim = inputs["resid"].shape[1]
    share = rows // NT
    cols = dim // NT
    lat = (NC, CHUNKS, rows // NC // CHUNKS, wide + 2 * ROPE)
    gu, dn = (NX, depth, 2 * UNIT), (NX, UNIT, n)
    heads = 2 * VDIM
    buffers = {
        "latbuf": ((nz, *lat), BF16),
        "qbuf": ((2 * (NOPE + ROPE), NX * rows), BF16),
        "scores": ((2, rows, NX * rows), F32),
        "weights": ((2, rows, NX * rows), BF16),
        "stat_a": ((2, 1, NX * rows), F32),
        "wk": ((wide, 2 * NOPE), BF16),
        "wv": ((heads, wide), BF16),
        "gustage": (gu, BF16),
        "owstage": ((heads, dim), BF16),
        "acc": ((2, VDIM, NX * rows), F32),
        "stat_m": ((2, 1, NX * rows), F32),
        "stat_l": ((2, 1, NX * rows), F32),
        "osend": ((NX, 2 * VDIM, rows), BF16),
        "orecv": ((NX, 2 * VDIM, rows), BF16),
        "ssend": ((NX, 8, rows), F32),
        "srecv": ((NX, 8, rows), F32),
        "gubuf": ((nz, *gu), BF16),
        "dnbuf": ((nz, *dn), BF16),
        "owbuf": ((NT, heads, cols), BF16),
        "residbuf": ((rows, cols), BF16),
        "att": ((rows, NT * 2 * VDIM), BF16),
        "mid": ((NX, rows, dim), BF16),
        "part": ((NC, NX, NY, share, dim), BF16),
        "pairbuf": ((NX, NY, share, dim), BF16),
        "half_in": ((10, 2, share, dim // 4), BF16),
        "whole_in": ((10, 2, share, dim // 2), BF16),
    }
    semaphores = {
        "local_sem": (5,),
        "ring_send": (nz, CHUNKS),
        "ring_recv": (nz, CHUNKS),
        "pair_send": (nz, CHUNKS),
        "pair_recv": (nz, CHUNKS),
        "gq_send": (1, 4),
        "gq_recv": (1, 4),
        "wx_send": (NX, 2),
        "wx_recv": (NX, 2),
        "ow_send": (NT,),
        "ow_recv": (NT,),
        "hop_send": (nz, 2, 2),
        "hop_recv": (nz, 2, 2),
        "o_send": (NX,),
        "o_recv": (NX,),
        "s_send": (NX,),
        "s_recv": (NX,),
        "ga_send": (1, 4),
        "ga_recv": (1, 4),
        "sa_send": (1, 5),
        "sa_recv": (1, 5),
        "gm_send": (10, 4),
        "gm_recv": (10, 4),
        "sm_send": (10, 5),
        "sm_recv": (10, 5),
        "pc_send": (NX,),
        "pc_recv": (NX,),
        "rs_send": (10, 4),
        "rs_recv": (10, 4),
    }
    names = [*inputs, "out", *buffers, *semaphores]
    return pl.pallas_call(
        functools.partial(layer_kernel, nz, names),
        out_shape=jax.ShapeDtypeStruct((share, dim), BF16),
        in_specs=[anywhere if name in whole else vmem for name in inputs],
        out_specs=vmem,
        scratch_shapes=[pltpu.VMEM(*b) for b in buffers.values()]
        + [pltpu.SemaphoreType.DMA(s) for s in semaphores.values()],
        compiler_params=pltpu.CompilerParams(
            collective_id=0, has_side_effects=True, vmem_limit_bytes=62 * 1024 * 1024
        ),
    )(*inputs.values())


def body(
    resid,
    queries,
    latent,
    rope_key,
    lat_gain,
    kv_weight,
    out_gain,
    out_weight,
    ffn_gain,
    gate_weight,
    up_weight,
    down_weight,
):
    rows = latent.shape[0]
    half = ROPE // 2
    frequency = THETA ** (-np.arange(half) / half)

    def turns(places):
        angle = places[:, None] * frequency
        return jnp.asarray(np.concatenate([np.cos(angle), np.sin(angle)], axis=1), F32)

    inputs = {
        "latent": latent,
        "rope_key": rope_key,
        "queries": queries,
        "lat_gain": lat_gain[None, :],
        "kv_weight": kv_weight,
        "gate": gate_weight,
        "upward": up_weight,
        "ffn_gain": ffn_gain.reshape(-1, gate_weight.shape[0]),
        "out_gain": out_gain[None, :],
        "first_turn": turns(np.arange(lax.axis_size("sp")) * rows),
        "row_turn": turns(np.arange(rows)),
        "dn": down_weight.reshape(NX, UNIT, down_weight.shape[1]),
        "ow": out_weight,
        "resid": resid,
    }
    return layer(inputs, ("dn", "ow", "resid"))


def solution(mesh):
    placed = (
        P("sp", None),
        P("sp", "tp"),
        P("sp", None),
        P("sp", None),
        P(),
        P(None, "tp"),
        P("tp"),
        P("tp", None),
        P(),
        P("sp", "tp"),
        P("sp", "tp"),
        P("tp", "sp"),
    )
    return jax.shard_map(
        body, mesh=mesh, in_specs=placed, out_specs=P(("sp", "tp"), None), check_vma=False
    )
```

```python
import functools
import math

import jax
import jax.numpy as jnp
import numpy as np
from jax import lax
from jax.experimental import pallas as pl
from jax.experimental.pallas import tpu as pltpu
from jax.sharding import PartitionSpec as P

NOPE = 128
ROPE = 64
VDIM = 128
NX = 4
NY = 4
NC = 2
NT = NY * NC
CHUNKS = 4
EARLY = 1
UNIT = 192

EPSILON = 1e-06
THETA = 10000.0
LOWEST = -1e30
MESH = pl.DeviceIdType.MESH
F32 = jnp.float32
BF16 = jnp.bfloat16


def norm_rows(values, gain):
    wide = values.astype(F32)
    return wide * lax.rsqrt(jnp.mean(wide * wide, axis=-1, keepdims=True) + EPSILON) * gain


def column(row):
    return jnp.transpose(jnp.broadcast_to(row, (128, row.shape[1])))[:, :1]


def turned(values, cosine, sine):
    half = values.shape[-1] // 2
    first, second = values[:, :half], values[:, half:]
    return jnp.concatenate(
        [first * cosine - second * sine, first * sine + second * cosine], axis=1
    )


def nt_dot(a, b):
    return lax.dot_general(a, b, (((1,), (1,)), ((), ())), preferred_element_type=F32)


def wide_dot(a, b):
    return jnp.dot(a, b, preferred_element_type=F32)


class Refs:
    def __init__(self, names, values):
        self.__dict__.update(zip(names, values, strict=True))


def remote(src, dst, send, recv, to):
    return pltpu.make_async_remote_copy(
        src_ref=src, dst_ref=dst, send_sem=send, recv_sem=recv, device_id=to, device_id_type=MESH
    )


class Gather4:
    def __init__(self, piece, send, recv, index, plus, minus):
        self.piece, self.send, self.recv, self.index = piece, send, recv, index
        self.plus, self.minus = plus, minus

    def copy(self, way, k, half):
        to = self.plus if way in (0, 2) else self.minus
        ref = self.piece(k, half)
        return remote(ref, ref, self.send.at[self.index, way], self.recv.at[self.index, way], to)

    def start(self):
        self.copy(0, 0, None).start()
        self.copy(1, 0, None).start()

    def near(self, way):
        self.copy(way, 3 if way == 0 else 1, None).wait_recv()
        self.copy(way + 2, 3 if way == 0 else 1, way).start()

    def far(self, half):
        self.copy(half + 2, 2, half).wait_recv()

    def done(self):
        self.copy(0, 0, None).wait_send()
        self.copy(1, 0, None).wait_send()
        self.copy(2, 3, 0).wait_send()
        self.copy(3, 1, 1).wait_send()


class Scatter4:
    def __init__(self, block, half_in, whole_in, send, recv, index, plus, minus):
        self.block, self.half_in, self.whole_in = block, half_in, whole_in
        self.send, self.recv, self.index = send, recv, index
        self.plus, self.minus = plus, minus

    def half(self, h):
        to = self.minus if h == 0 else self.plus
        return remote(
            self.block(2, h), self.half_in.at[h], self.send.at[self.index, h], self.recv.at[self.index, h], to
        )

    def whole(self, h):
        to, k = (self.minus, 3) if h == 0 else (self.plus, 1)
        return remote(
            self.block(k, None),
            self.whole_in.at[h],
            self.send.at[self.index, 2 + h],
            self.recv.at[self.index, 2 + h],
            to,
        )

    def start(self):
        self.half(0).start()
        self.half(1).start()

    def near(self, h):
        self.half(h).wait_recv()
        ref = self.block(3 if h == 0 else 1, h)
        ref[...] = (ref[...].astype(F32) + self.half_in[h].astype(F32)).astype(BF16)
        self.whole(h).start()

    def total(self):
        self.whole(0).wait_recv()
        self.whole(1).wait_recv()
        ref = self.block(0, None)
        return ref[...].astype(F32) + self.whole_in[0].astype(F32) + self.whole_in[1].astype(F32)

    def finish(self):
        self.block(0, None)[...] = self.total().astype(BF16)

    def done(self):
        for h in range(2):
            self.half(h).wait_send()
            self.whole(h).wait_send()


def layer_kernel(nz, names, *values):
    r = Refs(names, values)
    sp, tp = lax.axis_index("sp"), lax.axis_index("tp")
    z, x = sp // NX, lax.rem(sp, NX)
    y, core = tp // NC, lax.rem(tp, NC)
    up = (lax.rem(z + 1, nz) * NX + x, tp)
    down = (lax.rem(z + nz - 1, nz) * NX + x, tp)
    partner = (sp, tp + 1 - 2 * core)
    rows = r.latent.shape[0]
    far = nz // 2
    factor = (1.0 / math.sqrt(NOPE + ROPE)) * math.log2(math.e)
    dim = r.resid.shape[1]
    cols = dim // NT
    share = rows // NT

    def along_x(k):
        return (z * NX + lax.rem(x + k, NX), tp)

    def along_y(k, other=0):
        to_core = core if other == 0 else 1 - core
        return (sp, lax.rem(y + k, NY) * NC + to_core)

    peers = [up, down, partner]
    peers += [along_x(k) for k in range(1, NX)]
    peers += [along_y(k) for k in range(1, NY)]
    peers += [along_y(k, 1) for k in range(1, NY)]
    barrier = pltpu.get_barrier_semaphore()
    for peer in peers:
        pl.semaphore_signal(barrier, inc=1, device_id=peer, device_id_type=MESH)

    own_cols = pl.ds(pl.multiple_of(tp * cols, cols), cols)

    def place(t, at_z):
        return lax.rem(t - at_z + far + nz, nz)

    def channels(t):
        return pl.ds(pl.multiple_of(place(t, z) * cols, cols), cols)

    local = [
        pltpu.make_async_copy(r.ow, r.owstage, r.local_sem.at[0]),
        pltpu.make_async_copy(r.dn.at[x], r.dnbuf.at[z, x], r.local_sem.at[1]),
        pltpu.make_async_copy(r.resid.at[:, own_cols], r.residbuf, r.local_sem.at[2]),
        pltpu.make_async_copy(r.gustage.at[x], r.gubuf.at[far, x], r.local_sem.at[3]),
        pltpu.make_async_copy(r.owstage.at[:, own_cols], r.owbuf.at[tp], r.local_sem.at[4]),
    ]
    for copy in local[:3]:
        copy.start()

    half = ROPE // 2
    base, step = r.first_turn[pl.ds(sp, 1), :], r.row_turn[...]
    base_cos, base_sin = base[:, :half], base[:, half:]
    step_cos, step_sin = step[:, :half], step[:, half:]
    cosine = base_cos * step_cos - base_sin * step_sin
    sine = base_sin * step_cos + base_cos * step_sin
    key_rot = turned(jnp.transpose(r.rope_key[...].astype(F32)), cosine, sine)
    lat = jnp.concatenate([norm_rows(r.latent[...], r.lat_gain[...]), key_rot, key_rot], axis=1)
    r.latbuf[0] = lat.astype(BF16).reshape(r.latbuf.shape[1:])
    query = r.queries[...].astype(F32)
    one = NOPE + ROPE
    parts = [query[:, h * one : h * one + NOPE] for h in range(2)]
    parts += [turned(query[:, h * one + NOPE : (h + 1) * one], cosine, sine) for h in range(2)]
    own_rows_at = pl.ds(pl.multiple_of(x * rows, rows), rows)
    r.qbuf[:, own_rows_at] = jnp.transpose(jnp.concatenate(parts, axis=1)).astype(BF16)
    pl.semaphore_wait(barrier, len(peers))

    def ring(src_slot, dst_slot, chunk, to):
        src = r.latbuf.at[src_slot, core, chunk]
        dst = r.latbuf.at[dst_slot, core, chunk]
        return remote(src, dst, r.ring_send.at[dst_slot, chunk], r.ring_recv.at[dst_slot, chunk], to)

    def pair(slot, chunk, side):
        ref = r.latbuf.at[slot, side, chunk]
        return remote(ref, ref, r.pair_send.at[slot, chunk], r.pair_recv.at[slot, chunk], partner)

    def q_piece(k, half):
        channels = r.qbuf.shape[0]
        at = pl.ds(0, channels) if half is None else pl.ds(half * (channels // 2), channels // 2)
        return r.qbuf.at[at, pl.ds(pl.multiple_of(lax.rem(x + k, NX) * rows, rows), rows)]

    gq = Gather4(q_piece, r.gq_send, r.gq_recv, 0, along_x(1), along_x(3))

    def weight_copies(k):
        to = lax.rem(x + k, NX)
        return [
            remote(r.gustage.at[to], r.gubuf.at[far, x], r.wx_send.at[k, 0], r.wx_recv.at[k, 0], along_x(k)),
            remote(r.dn.at[to], r.dnbuf.at[z, x], r.wx_send.at[k, 1], r.wx_recv.at[k, 1], along_x(k)),
        ]

    def ow_copy(i):
        k, other = i // 2, i % 2
        to = along_y(k, other)
        src = r.owstage.at[:, pl.ds(pl.multiple_of(to[1] * cols, cols), cols)]
        return remote(src, r.owbuf.at[tp], r.ow_send.at[i], r.ow_recv.at[i], to)

    for chunk in range(CHUNKS):
        ring(0, 1, chunk, up).start()
        ring(0, far + 1, chunk, down).start()
    gq.start()

    gain = column(r.ffn_gain[pl.ds(sp, 1), :])
    gate, upward = r.gate[...].astype(F32) * gain, r.upward[...].astype(F32) * gain
    for i in range(NX):
        lo, mid_lo, hi = i * UNIT, i * UNIT + 128, (i + 1) * UNIT
        tiles = [gate[:, lo:mid_lo], gate[:, mid_lo:hi], upward[:, mid_lo:hi], upward[:, lo:mid_lo]]
        r.gustage[i] = jnp.concatenate(tiles, axis=1).astype(BF16)
    local[3].start()
    for k in (1, 3):
        for copy in weight_copies(k):
            copy.start()
    for h in range(2):
        at = 2 * h * NOPE
        r.wk[:, h * NOPE : (h + 1) * NOPE] = r.kv_weight[:, at : at + NOPE]
        value_weight = r.kv_weight[:, at + NOPE : at + NOPE + VDIM].astype(F32)
        r.wv[h * VDIM : (h + 1) * VDIM, :] = jnp.transpose(value_weight).astype(BF16)
    local[0].wait()
    gain = column(r.out_gain[...])

    def scale_ow(j, carry):
        at = pl.ds(pl.multiple_of(j * cols, cols), cols)
        r.owstage[:, at] = (r.owstage[:, at].astype(F32) * gain).astype(BF16)
        return carry

    lax.fori_loop(0, NT, scale_ow, 0)
    local[4].start()
    for i in range(1, NT):
        ow_copy(i).start()

    r.stat_m[...] = jnp.full(r.stat_m.shape, LOWEST, F32)
    r.stat_l[...] = jnp.zeros(r.stat_l.shape, F32)
    r.acc[...] = jnp.zeros(r.acc.shape, F32)

    def keys_of(slot):
        lat = r.latbuf[slot].reshape(rows, r.latbuf.shape[-1])
        wide = r.wk.shape[0]
        compressed, both_rot = lat[:, :wide], lat[:, wide:]
        lane = lax.broadcasted_iota(jnp.int32, both_rot.shape, 1)
        keys = wide_dot(compressed, r.wk[...]).astype(BF16)
        values = nt_dot(r.wv[...], compressed).astype(BF16)
        out = []
        for h in range(2):
            own_half = lane < ROPE if h == 0 else lane >= ROPE
            key_rot = jnp.where(own_half, both_rot.astype(F32), 0.0).astype(BF16)
            key = jnp.concatenate([keys[:, h * NOPE : (h + 1) * NOPE], key_rot], axis=1)
            out.append((key, values[h * VDIM : (h + 1) * VDIM]))
        return out

    def attend(heads_here, first, count, diagonal):
        for h, (key, _) in enumerate(heads_here):
            at = pl.ds(first, count)
            query = jnp.concatenate(
                [r.qbuf[h * NOPE : (h + 1) * NOPE, at], r.qbuf[2 * NOPE :, at]], axis=0
            )
            r.scores[h, :, :count] = wide_dot(key, query)
        for h, (_, value) in enumerate(heads_here):
            for b in range(count // 128):
                here = pl.ds(b * 128, 128)
                at = pl.ds(first + b * 128, 128)
                if not isinstance(first, int):
                    at = pl.ds(pl.multiple_of(first + b * 128, 128), 128)
                scores = r.scores[h, :, here] * factor
                if diagonal:
                    key_at = x * rows + lax.broadcasted_iota(jnp.int32, scores.shape, 0)
                    query_at = first + b * 128 + lax.broadcasted_iota(jnp.int32, scores.shape, 1)
                    allowed = key_at <= query_at
                    scores = jnp.where(allowed, scores, LOWEST)
                old = r.stat_m[h, :, at]
                new = jnp.maximum(old, jnp.max(scores, axis=0, keepdims=True))
                weights = jnp.exp2(scores - new)
                if diagonal:
                    weights = jnp.where(allowed, weights, 0.0)
                shrink = jnp.exp2(old - new)
                r.stat_m[h, :, at] = new
                r.stat_a[h, :, here] = shrink
                r.stat_l[h, :, at] = r.stat_l[h, :, at] * shrink + jnp.sum(
                    weights, axis=0, keepdims=True
                )
                r.weights[h, :, here] = weights.astype(BF16)
            at = pl.ds(first, count)
            r.acc[h, :, at] = r.acc[h, :, at] * r.stat_a[h, :, :count] + wide_dot(
                value, r.weights[h, :, :count]
            )

    def piece(slot):
        attend(keys_of(slot), 0, NX * rows, False)

    def diagonal_part(heads_here, k):
        attend(heads_here, pl.multiple_of(lax.rem(x + k, NX) * rows, rows), rows, True)

    def arrive(slot, forward_to, to):
        for chunk in range(CHUNKS):
            ring(0, slot, chunk, to).wait_recv()
            if forward_to is not None:
                ring(slot, forward_to, chunk, to).start()
            pair(slot, chunk, core).start()

    def use(slot, needed):
        for chunk in range(CHUNKS):
            pair(slot, chunk, 1 - core).wait_recv()

        @pl.when(needed)
        def _():
            piece(slot)

    def both(d):
        def one(i, carry):
            slot = jnp.where(i == 0, d, far + d)
            source = jnp.where(i == 0, z - d, z + d - nz)
            use(slot, source >= 0)
            return carry

        return one

    def hop_refs(of, way, part, z_from, z_to):
        if part == 1:
            return r.dnbuf.at[of], r.dnbuf.at[of]
        return r.gubuf.at[place(of, z_from)], r.gubuf.at[place(of, z_to)]

    def hop(d, way, part):
        of = lax.rem(z - (d - 1) + nz, nz) if way == 0 else lax.rem(z + d - 1, nz)
        to = up if way == 0 else down
        src, dst = hop_refs(of, way, part, z, to[0] // NX)
        return remote(src, dst, r.hop_send.at[d, way, part], r.hop_recv.at[d, way, part], to)

    def hop_in(d, way, part):
        of = lax.rem(z - d + nz, nz) if way == 0 else lax.rem(z + d, nz)
        to = up if way == 0 else down
        src, dst = hop_refs(of, way, part, z, z)
        return remote(src, dst, r.hop_send.at[d, way, part], r.hop_recv.at[d, way, part], to)

    def in_hop(d):
        return [(way, part) for part in range(2) for way in range(2) if d < far or way == part]

    def first_hop(k, way, part):
        to = up if way == 0 else down
        src, dst = hop_refs(z, way, part, z, to[0] // NX)
        block = lax.rem(x + k, NX)
        send, recv = r.first_send.at[k, way, part], r.first_recv.at[k, way, part]
        return remote(src.at[block], dst.at[block], send, recv, to)

    def first_in(k, way, part):
        to = up if way == 0 else down
        of = lax.rem(z + nz - 1, nz) if way == 0 else lax.rem(z + 1, nz)
        ref = hop_refs(of, way, part, z, z)[0].at[lax.rem(x + k, NX)]
        return remote(ref, ref, r.first_send.at[k, way, part], r.first_recv.at[k, way, part], to)

    def start_first(k):
        if k == 0:
            local[1].wait()
            local[3].wait()
        else:
            for copy in weight_copies(NX - k):
                copy.wait_recv()
        for way, part in in_hop(1):
            first_hop(k, way, part).start()

    def hop_on(d, only=None):
        for way, part in in_hop(d):
            if only is not None and part != only:
                continue
            if d == 1:
                for k in range(NX):
                    first_in(k, way, part).wait_recv()
            else:
                hop_in(d, way, part).wait_recv()
            if d < far and (way, part) in in_hop(d + 1):
                hop(d + 1, way, part).start()

    def hop_latent(d):
        arrive(d, d + 1 if d < far else None, up)
        if d < far:
            arrive(far + d, far + d + 1 if d < far - 1 else None, down)

    own_keys = keys_of(0)
    diagonal_part(own_keys, 0)
    hop_latent(1)
    gq.near(0)
    gq.near(1)
    for copy in weight_copies(2):
        copy.start()
    diagonal_part(own_keys, 3)
    diagonal_part(own_keys, 1)
    hop_latent(2)
    gq.far(0)
    gq.far(1)
    diagonal_part(own_keys, 2)
    if far > 2:
        lax.fori_loop(0, 2, both(1), 0)
        hop_latent(3)
    start_first(0)
    start_first(1)
    start_first(3)
    for d in range(2, far - 1):
        lax.fori_loop(0, 2, both(d), 0)
    start_first(2)
    if far > 3:
        hop_latent(4)
    lax.fori_loop(0, 2, both(far - 1), 0)
    use(far, z - far >= 0)

    for b in range(NX):
        at = pl.ds(b * rows, rows)
        for h in range(2):
            total = r.stat_l[h, :, at]
            inverse = jnp.where(total > 0.0, 1.0 / jnp.where(total > 0.0, total, 1.0), 0.0)
            r.osend[b, h * VDIM : (h + 1) * VDIM] = (r.acc[h, :, at] * inverse).astype(BF16)
            r.ssend[b, h : h + 1] = r.stat_m[h, :, at]
            r.ssend[b, 2 + h : 3 + h] = total

    def o_copy(k, h):
        to = lax.rem(x + k, NX)
        head = pl.ds(h * VDIM, VDIM)
        return remote(
            r.osend.at[to, head], r.orecv.at[k, head], r.o_send.at[k, h], r.o_recv.at[k, h], along_x(k)
        )

    def s_copy(k):
        to = lax.rem(x + k, NX)
        return remote(r.ssend.at[to], r.srecv.at[k], r.s_send.at[k], r.s_recv.at[k], along_x(k))

    for k in (2, 1, 3):
        s_copy(k).start()
    for h in range(2):
        for k in (2, 1, 3):
            o_copy(k, h).start()
    for k in range(1, NX):
        s_copy(k).wait_recv()
    width = 2 * VDIM
    stats = [r.ssend[x]] + [r.srecv[k] for k in range(1, NX)]

    def swap(piece, send, recv, index):
        k, half = ((0, None), (3, None), (1, None), (2, 0), (2, 1))[index]
        mine, theirs = piece(core)(k, half), piece(1 - core)(k, half)
        out = functools.partial(remote, mine, mine, send.at[index], recv.at[index], partner)
        come = functools.partial(remote, theirs, theirs, send.at[index], recv.at[index], partner)
        return out, come

    def att_piece(h, own_core):
        def ref(k, half):
            of = lax.rem(y + k, NY) * NC + own_core
            where = pl.ds(pl.multiple_of(of * width + h * VDIM, VDIM), VDIM)
            at = pl.ds(0, rows) if half is None else pl.ds(half * (rows // 2), rows // 2)
            return r.att.at[at, where]

        return ref

    heads = []
    for h in range(2):
        for k in range(1, NX):
            o_copy(k, h).wait_recv()
        outs = [r.osend[x, h * VDIM : (h + 1) * VDIM]] + [
            r.orecv[k, h * VDIM : (h + 1) * VDIM] for k in range(1, NX)
        ]
        top = functools.reduce(jnp.maximum, [s[h : h + 1] for s in stats])
        shares = [s[2 + h : 3 + h] * jnp.exp2(s[h : h + 1] - top) for s in stats]
        inverse = 1.0 / sum(shares)
        mixed = sum(o.astype(F32) * (w * inverse) for o, w in zip(outs, shares))
        at = pl.ds(pl.multiple_of(tp * width + h * VDIM, VDIM), VDIM)
        r.att[:, at] = jnp.transpose(mixed).astype(BF16)
        piece_of = functools.partial(att_piece, h)
        g = Gather4(piece_of(core), r.ga_send, r.ga_recv, h, along_y(1), along_y(3))
        swaps = [swap(piece_of, r.sa_send.at[h], r.sa_recv.at[h], i) for i in range(5)]
        g.start()
        swaps[0][0]().start()
        heads.append((g, swaps))
    hop_on(1, 0)
    for way in range(2):
        for g, swaps in heads:
            g.near(way)
            swaps[1 + way][0]().start()
    hop_on(1, 1)
    for half in range(2):
        for g, swaps in heads:
            g.far(half)
            swaps[3 + half][0]().start()
    for i in range(1, NT):
        ow_copy(i).wait_recv()
    local[4].wait()
    local[2].wait()
    for g, swaps in heads:
        for out, come in swaps:
            come().wait_recv()

    att = r.att[...]
    att_wide = att.astype(F32)
    scale = lax.rsqrt(jnp.mean(att_wide * att_wide, axis=1, keepdims=True) + EPSILON)
    attn_sum = wide_dot(att, r.owbuf[...].reshape(att.shape[1], cols)) * scale
    middle = (r.residbuf[...].astype(F32) + attn_sum).astype(BF16)
    r.mid[x, :, channels(tp)] = middle

    def sq_copy(i):
        ref = r.sq_part.at[tp]
        return remote(ref, ref, r.sq_send.at[i], r.sq_recv.at[i], along_y(i // 2, i % 2))

    def sx_copy(k):
        ref = r.sq_row.at[x]
        return remote(ref, ref, r.sx_send.at[k], r.sx_recv.at[k], along_x(k))

    def squares_start():
        wide = middle.astype(F32)
        squares = jnp.sum(wide * wide, axis=1, keepdims=True)
        r.sq_part[tp] = jnp.transpose(jnp.broadcast_to(squares, (rows, 128)))[:8]
        for i in range(1, NT):
            sq_copy(i).start()

    def squares_on():
        for i in range(1, NT):
            sq_copy(i).wait_recv()
        r.sq_row[x] = sum(r.sq_part[i] for i in range(NT))
        for k in range(1, NX):
            sx_copy(k).start()

    def squares_end():
        for k in range(1, NX):
            sx_copy(k).wait_recv()
        for b in range(NX):
            r.row_scale[b] = column(lax.rsqrt(r.sq_row[b, :1] / dim + EPSILON))


    def mid_piece(axis, at_x, at_y, own_core, first):
        def ref(k, half):
            of_x = lax.rem(x + at_x + (k if axis == 0 else 0), NX)
            of_y = lax.rem(y + at_y + (k if axis == 1 else 0), NY)
            where = channels(of_y * NC + own_core)
            quarter = rows // 4
            at = pl.ds(first * 2 * quarter, 2 * quarter)
            if half is not None:
                at = pl.ds((first * 2 + half) * quarter, quarter)
            return r.mid.at[of_x, at, where]

        return ref

    def plane_ring(index, axis, at_x, at_y, first):
        piece_of = functools.partial(lambda c: mid_piece(axis, at_x, at_y, c, first))
        plus, minus = (along_x(1), along_x(3)) if axis == 0 else (along_y(1), along_y(3))
        g = Gather4(piece_of(core), r.gm_send, r.gm_recv, index, plus, minus)
        return g, [swap(piece_of, r.sm_send.at[index], r.sm_recv.at[index], i) for i in range(5)]

    offsets = (0, 3, 1, 2)
    first_rings = [plane_ring(0, 0, 0, 0, 0), plane_ring(1, 1, 0, 0, 1)]
    second_rings = [
        [plane_ring(2 + i, 1, k, 0, 0), plane_ring(6 + i, 0, 0, k, 1)] for i, k in enumerate(offsets)
    ]
    for g, s in first_rings:
        g.start()
        s[0][0]().start()
    for g, s in second_rings[0]:
        g.start()
    squares_start()
    for way in range(2):
        for i, (g, s) in enumerate(first_rings):
            g.near(way)
            second_rings[1 + way][i][0].start()
            s[1 + way][0]().start()
    hop_on(2, 0)
    for way in range(2):
        for g, s in second_rings[0]:
            g.near(way)
            s[1 + way][0]().start()
    hop_on(2, 1)
    squares_on()
    for i, (g, s) in enumerate(first_rings):
        for half in range(2):
            g.far(half)
            s[3 + half][0]().start()
        second_rings[3][i][0].start()
    for j in range(1, 4):
        for way in range(2):
            for g, s in second_rings[j]:
                g.near(way)
                s[1 + way][0]().start()
        for half in range(2):
            for g, s in second_rings[j - 1]:
                g.far(half)
                s[3 + half][0]().start()
        if j == 1 and far > 3:
            hop_on(3, 0)
        if j == 2 and far > 3:
            hop_on(3, 1)
    for half in range(2):
        for g, s in second_rings[3]:
            g.far(half)
            s[3 + half][0]().start()
    rings = first_rings + [pair_of for both_of in second_rings for pair_of in both_of]
    for i, (g, s) in enumerate(rings):
        for j, (out, come) in enumerate(s):
            if j > 0 or i < 2:
                come().wait_recv()

    def ahead(j):
        return jnp.where(j == 0, 2, jnp.where(j == 1, 1, jnp.where(j == 2, 3, 0)))

    def early(j, carry):
        b = lax.rem(x + ahead(j), NX)

        r.gu_sum[b] = wide_dot(r.mid[b, :, cols:], r.gubuf[1:].reshape(dim - cols, 2 * UNIT))
        return carry

    squares_end()
    lax.fori_loop(0, EARLY, early, 0)
    hop_on(far)

    def mixer(j):
        b = lax.rem(x + ahead(j), NX)

        @pl.when(j < EARLY)
        def _():
            r.gu_sum[b] += wide_dot(r.mid[b, :, :cols], r.gubuf[0].reshape(cols, 2 * UNIT))

        @pl.when(j >= EARLY)
        def _():
            r.gu_sum[b] = wide_dot(r.mid[b], r.gubuf[...].reshape(dim, 2 * UNIT))

        gu = r.gu_sum[b]
        gu = gu * r.row_scale[b]
        gate, mixed_tile, upward = gu[:, :128], gu[:, 128:256], gu[:, 256:]
        first = gate / (1.0 + jnp.exp(-gate)) * upward
        second = (mixed_tile / (1.0 + jnp.exp(-mixed_tile)))[:, :64] * mixed_tile[:, 64:]
        hidden = jnp.concatenate([first, second], axis=1).astype(BF16)
        n = r.dnbuf.shape[-1]
        for zz in range(nz):
            w = jnp.concatenate([r.dnbuf[zz, i] for i in range(NX)], axis=1)
            terms = wide_dot(hidden, w).astype(BF16).reshape(NY, NC, share, NX * n)
            for c in range(NC):
                r.part[c, b, :, :, zz * NX * n : (zz + 1) * NX * n] = terms[:, c]
        core_copy(j).start()

    def core_copy(j):
        b = lax.rem(x + ahead(j), NX)
        return remote(r.part.at[1 - core, b], r.pairbuf.at[b], r.pc_send.at[j], r.pc_recv.at[j], partner)

    def core_sum(j):
        b = lax.rem(x + ahead(j), NX)
        core_copy(j).wait_recv()
        for i in range(NY):
            ref = r.part.at[core, b, i]
            ref[...] = (ref[...].astype(F32) + r.pairbuf[b, i].astype(F32)).astype(BF16)

    depth = r.part.shape[-1] // 2

    def block(axis, of_x, of_y, first):
        def ref(k, half):
            bx = lax.rem(of_x + (k if axis == 0 else 0), NX)
            by = lax.rem(of_y + (k if axis == 1 else 0), NY)
            at = pl.ds(first * depth, depth)
            if half is not None:
                at = pl.ds(first * depth + half * (depth // 2), depth // 2)
            return r.part.at[core, bx, by, :, at]

        return ref

    def scatter(index, axis, of_x, of_y, first):
        plus, minus = (along_x(1), along_x(3)) if axis == 0 else (along_y(1), along_y(3))
        return Scatter4(
            block(axis, of_x, of_y, first),
            r.half_in.at[index],
            r.whole_in.at[index],
            r.rs_send,
            r.rs_recv,
            index,
            plus,
            minus,
        )

    def first_along_y(j):
        return scatter(j, 1, x + ahead(j), y, 0)

    def first_along_x(j):
        return scatter(4 + j, 0, x, y + ahead(j), 1)

    def stage(j, carry):
        mixer(j)

        @pl.when(j >= 1)
        def _():
            core_sum(j - 1)
            first_along_y(j - 1).start()

        @pl.when(j == 1)
        def _():
            for i in range(NY):
                first_along_x(i).start()

        return carry

    lax.fori_loop(0, NX, stage, 0)
    steps = [[first_along_y(j), first_along_x(j)] for j in range(NX)]
    ends = [scatter(8, 0, x, y, 0), scatter(9, 1, x, y, 1)]
    for h in range(2):
        first_along_x(0).near(h)
        first_along_y(0).near(h)
    core_sum(NX - 1)
    first_along_y(NX - 1).start()
    for j in range(1, NX):
        for h in range(2):
            first_along_x(j).near(h)
            first_along_y(j).near(h)
    for j, both_of in enumerate(steps):
        for s in both_of:
            s.finish()
        for s in ends:
            if j == 0:
                s.start()
            if j == 1:
                s.near(1)
            if j == 2:
                s.near(0)
    own_rows = pl.ds(pl.multiple_of(tp * share, share), share)
    for first, s in enumerate(ends):
        at = slice(first * depth, (first + 1) * depth)
        r.out[:, at] = s.total()

    for t in range(NT):
        r.middle[:, t * cols : (t + 1) * cols] = r.mid[x, own_rows, channels(t)]

    for k in range(1, NX):
        for h in range(2):
            o_copy(k, h).wait_send()
        s_copy(k).wait_send()
        for copy in weight_copies(k):
            copy.wait_send()
    for i in range(1, NT):
        ow_copy(i).wait_send()
    for slot in range(1, nz):
        for chunk in range(CHUNKS):
            ring(0, slot, chunk, up).wait_send()
            pair(slot, chunk, core).wait_send()
    for way, part in in_hop(1):
        for k in range(NX):
            first_hop(k, way, part).wait_send()
    for d in range(2, far + 1):
        for way, part in in_hop(d):
            hop(d, way, part).wait_send()
    gq.done()
    for g, swaps in heads:
        g.done()
        for out, come in swaps:
            out().wait_send()
    for i, (g, s) in enumerate(rings):
        g.done()
        for j, (out, come) in enumerate(s):
            if j > 0 or i < 2:
                out().wait_send()
    for i in range(1, NT):
        sq_copy(i).wait_send()
    for k in range(1, NX):
        sx_copy(k).wait_send()
    for j in range(NX):
        core_copy(j).wait_send()
    for both_of in [*steps, ends]:
        for s in both_of:
            s.done()


def layer(inputs, whole):
    nz = lax.axis_size("sp") // NX
    vmem = pl.BlockSpec(memory_space=pltpu.VMEM)
    anywhere = pl.BlockSpec(memory_space=pl.ANY)
    rows, wide = inputs["latent"].shape
    depth = inputs["gate"].shape[0]
    n = inputs["dn"].shape[-1]
    dim = inputs["resid"].shape[1]
    share = rows // NT
    cols = dim // NT
    lat = (NC, CHUNKS, rows // NC // CHUNKS, wide + 2 * ROPE)
    gu, dn = (NX, depth, 2 * UNIT), (NX, UNIT, n)
    heads = 2 * VDIM
    buffers = {
        "latbuf": ((nz, *lat), BF16),
        "qbuf": ((2 * (NOPE + ROPE), NX * rows), BF16),
        "scores": ((2, rows, NX * rows), F32),
        "weights": ((2, rows, NX * rows), BF16),
        "stat_a": ((2, 1, NX * rows), F32),
        "wk": ((wide, 2 * NOPE), BF16),
        "wv": ((heads, wide), BF16),
        "gustage": (gu, BF16),
        "owstage": ((heads, dim), BF16),
        "acc": ((2, VDIM, NX * rows), F32),
        "stat_m": ((2, 1, NX * rows), F32),
        "stat_l": ((2, 1, NX * rows), F32),
        "osend": ((NX, 2 * VDIM, rows), BF16),
        "orecv": ((NX, 2 * VDIM, rows), BF16),
        "ssend": ((NX, 8, rows), F32),
        "srecv": ((NX, 8, rows), F32),
        "gubuf": ((nz, *gu), BF16),
        "dnbuf": ((nz, *dn), BF16),
        "owbuf": ((NT, heads, cols), BF16),
        "residbuf": ((rows, cols), BF16),
        "att": ((rows, NT * 2 * VDIM), BF16),
        "mid": ((NX, rows, dim), BF16),
        "part": ((NC, NX, NY, share, dim), BF16),
        "row_scale": ((NX, rows, 1), F32),
        "gu_sum": ((NX, rows, 2 * UNIT), F32),
        "sq_part": ((NT, 8, rows), F32),
        "sq_row": ((NX, 8, rows), F32),
        "pairbuf": ((NX, NY, share, dim), BF16),
        "half_in": ((10, 2, share, dim // 4), BF16),
        "whole_in": ((10, 2, share, dim // 2), BF16),
    }
    semaphores = {
        "local_sem": (5,),
        "ring_send": (nz, CHUNKS),
        "ring_recv": (nz, CHUNKS),
        "pair_send": (nz, CHUNKS),
        "pair_recv": (nz, CHUNKS),
        "gq_send": (1, 4),
        "gq_recv": (1, 4),
        "wx_send": (NX, 2),
        "wx_recv": (NX, 2),
        "ow_send": (NT,),
        "ow_recv": (NT,),
        "first_send": (NX, 2, 2),
        "first_recv": (NX, 2, 2),
        "hop_send": (nz, 2, 2),
        "hop_recv": (nz, 2, 2),
        "o_send": (NX, 2),
        "o_recv": (NX, 2),
        "s_send": (NX,),
        "s_recv": (NX,),
        "ga_send": (2, 4),
        "ga_recv": (2, 4),
        "sa_send": (2, 5),
        "sa_recv": (2, 5),
        "gm_send": (10, 4),
        "gm_recv": (10, 4),
        "sm_send": (10, 5),
        "sm_recv": (10, 5),
        "sq_send": (NT,),
        "sq_recv": (NT,),
        "sx_send": (NX,),
        "sx_recv": (NX,),
        "pc_send": (NX,),
        "pc_recv": (NX,),
        "rs_send": (10, 4),
        "rs_recv": (10, 4),
    }
    names = [*inputs, "out", "middle", *buffers, *semaphores]
    return pl.pallas_call(
        functools.partial(layer_kernel, nz, names),
        out_shape=(
            jax.ShapeDtypeStruct((share, dim), F32),
            jax.ShapeDtypeStruct((share, dim), BF16),
        ),
        in_specs=[anywhere if name in whole else vmem for name in inputs],
        out_specs=(vmem, vmem),
        scratch_shapes=[pltpu.VMEM(*b) for b in buffers.values()]
        + [pltpu.SemaphoreType.DMA(s) for s in semaphores.values()],
        compiler_params=pltpu.CompilerParams(
            collective_id=0, has_side_effects=True, vmem_limit_bytes=62 * 1024 * 1024
        ),
    )(*inputs.values())


def body(
    resid,
    queries,
    latent,
    rope_key,
    lat_gain,
    kv_weight,
    out_gain,
    out_weight,
    ffn_gain,
    gate_weight,
    up_weight,
    down_weight,
):
    rows = latent.shape[0]
    half = ROPE // 2
    frequency = THETA ** (-np.arange(half) / half)

    def turns(places):
        angle = places[:, None] * frequency
        return jnp.asarray(np.concatenate([np.cos(angle), np.sin(angle)], axis=1), F32)

    inputs = {
        "latent": latent,
        "rope_key": rope_key.T,
        "queries": queries,
        "lat_gain": lat_gain[None, :],
        "kv_weight": kv_weight,
        "gate": gate_weight,
        "upward": up_weight,
        "ffn_gain": ffn_gain.reshape(-1, gate_weight.shape[0]),
        "out_gain": out_gain[None, :],
        "first_turn": turns(np.arange(lax.axis_size("sp")) * rows),
        "row_turn": turns(np.arange(rows)),
        "dn": down_weight.reshape(NX, UNIT, down_weight.shape[1]),
        "ow": out_weight,
        "resid": resid,
    }
    ffn_sum, middle = layer(inputs, ("dn", "ow", "resid"))
    return (middle.astype(F32) + ffn_sum).astype(BF16)


def solution(mesh):
    placed = (
        P("sp", None),
        P("sp", "tp"),
        P("sp", None),
        P("sp", None),
        P(),
        P(None, "tp"),
        P("tp"),
        P("tp", None),
        P(),
        P("sp", "tp"),
        P("sp", "tp"),
        P("tp", "sp"),
    )
    return jax.shard_map(
        body, mesh=mesh, in_specs=placed, out_specs=P(("sp", "tp"), None), check_vma=False
    )
```

```python
import functools
import math

import jax
import jax.numpy as jnp
import numpy as np
from jax import lax
from jax.experimental import pallas as pl
from jax.experimental.pallas import tpu as pltpu
from jax.sharding import PartitionSpec as P

NOPE = 128
ROPE = 64
VDIM = 128
NX = 4
NY = 4
NC = 2
NT = NY * NC
CHUNKS = 4
EARLY = 1
UNIT = 192

EPSILON = 1e-06
THETA = 10000.0
LOWEST = -1e30
MESH = pl.DeviceIdType.MESH
F32 = jnp.float32
BF16 = jnp.bfloat16


def norm_rows(values, gain):
    wide = values.astype(F32)
    return wide * lax.rsqrt(jnp.mean(wide * wide, axis=-1, keepdims=True) + EPSILON) * gain


def column(row):
    return jnp.transpose(jnp.broadcast_to(row, (128, row.shape[1])))[:, :1]


def turned(values, cosine, sine):
    half = values.shape[-1] // 2
    first, second = values[:, :half], values[:, half:]
    return jnp.concatenate(
        [first * cosine - second * sine, first * sine + second * cosine], axis=1
    )


def nt_dot(a, b):
    return lax.dot_general(a, b, (((1,), (1,)), ((), ())), preferred_element_type=F32)


def wide_dot(a, b):
    return jnp.dot(a, b, preferred_element_type=F32)


class Refs:
    def __init__(self, names, values):
        self.__dict__.update(zip(names, values, strict=True))


def remote(src, dst, send, recv, to):
    return pltpu.make_async_remote_copy(
        src_ref=src, dst_ref=dst, send_sem=send, recv_sem=recv, device_id=to, device_id_type=MESH
    )


class Gather4:
    def __init__(self, piece, send, recv, index, plus, minus):
        self.piece, self.send, self.recv, self.index = piece, send, recv, index
        self.plus, self.minus = plus, minus

    def copy(self, way, k, half):
        to = self.plus if way in (0, 2) else self.minus
        ref = self.piece(k, half)
        return remote(ref, ref, self.send.at[self.index, way], self.recv.at[self.index, way], to)

    def start(self):
        self.copy(0, 0, None).start()
        self.copy(1, 0, None).start()

    def near(self, way):
        self.copy(way, 3 if way == 0 else 1, None).wait_recv()
        self.copy(way + 2, 3 if way == 0 else 1, way).start()

    def far(self, half):
        self.copy(half + 2, 2, half).wait_recv()

    def done(self):
        self.copy(0, 0, None).wait_send()
        self.copy(1, 0, None).wait_send()
        self.copy(2, 3, 0).wait_send()
        self.copy(3, 1, 1).wait_send()


class Scatter4:
    def __init__(self, block, half_in, whole_in, send, recv, index, plus, minus):
        self.block, self.half_in, self.whole_in = block, half_in, whole_in
        self.send, self.recv, self.index = send, recv, index
        self.plus, self.minus = plus, minus

    def half(self, h):
        to = self.minus if h == 0 else self.plus
        return remote(
            self.block(2, h), self.half_in.at[h], self.send.at[self.index, h], self.recv.at[self.index, h], to
        )

    def whole(self, h):
        to, k = (self.minus, 3) if h == 0 else (self.plus, 1)
        return remote(
            self.block(k, None),
            self.whole_in.at[h],
            self.send.at[self.index, 2 + h],
            self.recv.at[self.index, 2 + h],
            to,
        )

    def start(self):
        self.half(0).start()
        self.half(1).start()

    def near(self, h):
        self.half(h).wait_recv()
        ref = self.block(3 if h == 0 else 1, h)
        ref[...] = (ref[...].astype(F32) + self.half_in[h].astype(F32)).astype(BF16)
        self.whole(h).start()

    def total(self):
        self.whole(0).wait_recv()
        self.whole(1).wait_recv()
        ref = self.block(0, None)
        return ref[...].astype(F32) + self.whole_in[0].astype(F32) + self.whole_in[1].astype(F32)

    def finish(self):
        self.block(0, None)[...] = self.total().astype(BF16)

    def done(self):
        for h in range(2):
            self.half(h).wait_send()
            self.whole(h).wait_send()


def layer_kernel(nz, names, *values):
    r = Refs(names, values)
    sp, tp = lax.axis_index("sp"), lax.axis_index("tp")
    z, x = sp // NX, lax.rem(sp, NX)
    y, core = tp // NC, lax.rem(tp, NC)
    up = (lax.rem(z + 1, nz) * NX + x, tp)
    down = (lax.rem(z + nz - 1, nz) * NX + x, tp)
    partner = (sp, tp + 1 - 2 * core)
    rows = r.latent.shape[0]
    far = nz // 2
    factor = (1.0 / math.sqrt(NOPE + ROPE)) * math.log2(math.e)
    dim = r.resid.shape[1]
    cols = dim // NT
    share = rows // NT

    def along_x(k):
        return (z * NX + lax.rem(x + k, NX), tp)

    def along_y(k, other=0):
        to_core = core if other == 0 else 1 - core
        return (sp, lax.rem(y + k, NY) * NC + to_core)

    peers = [up, down, partner]
    peers += [along_x(k) for k in range(1, NX)]
    peers += [along_y(k) for k in range(1, NY)]
    peers += [along_y(k, 1) for k in range(1, NY)]
    barrier = pltpu.get_barrier_semaphore()
    for peer in peers:
        pl.semaphore_signal(barrier, inc=1, device_id=peer, device_id_type=MESH)

    own_cols = pl.ds(pl.multiple_of(tp * cols, cols), cols)

    def place(t, at_z):
        return lax.rem(t - at_z + far + nz, nz)

    def channels(t):
        return pl.ds(pl.multiple_of(place(t, z) * cols, cols), cols)

    local = [
        pltpu.make_async_copy(r.ow, r.owstage, r.local_sem.at[0]),
        pltpu.make_async_copy(r.dn.at[x], r.dnbuf.at[z, x], r.local_sem.at[1]),
        pltpu.make_async_copy(r.resid.at[:, own_cols], r.residbuf, r.local_sem.at[2]),
        pltpu.make_async_copy(r.gustage.at[x], r.gubuf.at[far, x], r.local_sem.at[3]),
        pltpu.make_async_copy(r.owstage.at[:, own_cols], r.owbuf.at[tp], r.local_sem.at[4]),
    ]
    for copy in local[:3]:
        copy.start()

    half = ROPE // 2
    base, step = r.first_turn[pl.ds(sp, 1), :], r.row_turn[...]
    base_cos, base_sin = base[:, :half], base[:, half:]
    step_cos, step_sin = step[:, :half], step[:, half:]
    cosine = base_cos * step_cos - base_sin * step_sin
    sine = base_sin * step_cos + base_cos * step_sin
    key_rot = turned(jnp.transpose(r.rope_key[...].astype(F32)), cosine, sine)
    lat = jnp.concatenate([norm_rows(r.latent[...], r.lat_gain[...]), key_rot, key_rot], axis=1)
    r.latbuf[0] = lat.astype(BF16).reshape(r.latbuf.shape[1:])
    query = r.queries[...].astype(F32)
    one = NOPE + ROPE
    parts = [query[:, h * one : h * one + NOPE] for h in range(2)]
    parts += [turned(query[:, h * one + NOPE : (h + 1) * one], cosine, sine) for h in range(2)]
    own_rows_at = pl.ds(pl.multiple_of(x * rows, rows), rows)
    r.qbuf[:, own_rows_at] = jnp.transpose(jnp.concatenate(parts, axis=1)).astype(BF16)
    pl.semaphore_wait(barrier, len(peers))

    def ring(src_slot, dst_slot, chunk, to):
        src = r.latbuf.at[src_slot, core, chunk]
        dst = r.latbuf.at[dst_slot, core, chunk]
        return remote(src, dst, r.ring_send.at[dst_slot, chunk], r.ring_recv.at[dst_slot, chunk], to)

    def pair(slot, chunk, side):
        ref = r.latbuf.at[slot, side, chunk]
        return remote(ref, ref, r.pair_send.at[slot, chunk], r.pair_recv.at[slot, chunk], partner)

    def q_piece(k, half):
        channels = r.qbuf.shape[0]
        at = pl.ds(0, channels) if half is None else pl.ds(half * (channels // 2), channels // 2)
        return r.qbuf.at[at, pl.ds(pl.multiple_of(lax.rem(x + k, NX) * rows, rows), rows)]

    gq = Gather4(q_piece, r.gq_send, r.gq_recv, 0, along_x(1), along_x(3))

    def weight_copies(k):
        to = lax.rem(x + k, NX)
        return [
            remote(r.gustage.at[to], r.gubuf.at[far, x], r.wx_send.at[k, 0], r.wx_recv.at[k, 0], along_x(k)),
            remote(r.dn.at[to], r.dnbuf.at[z, x], r.wx_send.at[k, 1], r.wx_recv.at[k, 1], along_x(k)),
        ]

    def ow_copy(i):
        k, other = i // 2, i % 2
        to = along_y(k, other)
        src = r.owstage.at[:, pl.ds(pl.multiple_of(to[1] * cols, cols), cols)]
        return remote(src, r.owbuf.at[tp], r.ow_send.at[i], r.ow_recv.at[i], to)

    for chunk in range(CHUNKS):
        ring(0, 1, chunk, up).start()
        ring(0, far + 1, chunk, down).start()
    gq.start()

    gain = column(r.ffn_gain[pl.ds(sp, 1), :])
    gate, upward = r.gate[...].astype(F32) * gain, r.upward[...].astype(F32) * gain
    for i in range(NX):
        lo, mid_lo, hi = i * UNIT, i * UNIT + 128, (i + 1) * UNIT
        tiles = [gate[:, lo:mid_lo], gate[:, mid_lo:hi], upward[:, mid_lo:hi], upward[:, lo:mid_lo]]
        r.gustage[i] = jnp.concatenate(tiles, axis=1).astype(BF16)
    local[3].start()
    for k in (1, 3):
        for copy in weight_copies(k):
            copy.start()
    for h in range(2):
        at = 2 * h * NOPE
        r.wk[:, h * NOPE : (h + 1) * NOPE] = r.kv_weight[:, at : at + NOPE]
        value_weight = r.kv_weight[:, at + NOPE : at + NOPE + VDIM].astype(F32)
        r.wv[h * VDIM : (h + 1) * VDIM, :] = jnp.transpose(value_weight).astype(BF16)
    local[0].wait()
    gain = column(r.out_gain[...])

    def scale_ow(j, carry):
        at = pl.ds(pl.multiple_of(j * cols, cols), cols)
        r.owstage[:, at] = (r.owstage[:, at].astype(F32) * gain).astype(BF16)
        return carry

    lax.fori_loop(0, NT, scale_ow, 0)
    local[4].start()
    for i in range(1, NT):
        ow_copy(i).start()

    r.stat_m[...] = jnp.full(r.stat_m.shape, LOWEST, F32)
    r.stat_l[...] = jnp.zeros(r.stat_l.shape, F32)
    r.acc[...] = jnp.zeros(r.acc.shape, F32)

    def keys_of(slot):
        lat = r.latbuf[slot].reshape(rows, r.latbuf.shape[-1])
        wide = r.wk.shape[0]
        compressed, both_rot = lat[:, :wide], lat[:, wide:]
        lane = lax.broadcasted_iota(jnp.int32, both_rot.shape, 1)
        keys = wide_dot(compressed, r.wk[...]).astype(BF16)
        values = nt_dot(r.wv[...], compressed).astype(BF16)
        out = []
        for h in range(2):
            own_half = lane < ROPE if h == 0 else lane >= ROPE
            key_rot = jnp.where(own_half, both_rot.astype(F32), 0.0).astype(BF16)
            key = jnp.concatenate([keys[:, h * NOPE : (h + 1) * NOPE], key_rot], axis=1)
            out.append((key, values[h * VDIM : (h + 1) * VDIM]))
        return out

    def attend(heads_here, first, count, diagonal):
        for h, (key, _) in enumerate(heads_here):
            at = pl.ds(first, count)
            query = jnp.concatenate(
                [r.qbuf[h * NOPE : (h + 1) * NOPE, at], r.qbuf[2 * NOPE :, at]], axis=0
            )
            r.scores[h, :, :count] = wide_dot(key, query)
        for h, (_, value) in enumerate(heads_here):
            for b in range(count // 128):
                here = pl.ds(b * 128, 128)
                at = pl.ds(first + b * 128, 128)
                if not isinstance(first, int):
                    at = pl.ds(pl.multiple_of(first + b * 128, 128), 128)
                scores = r.scores[h, :, here] * factor
                if diagonal:
                    key_at = x * rows + lax.broadcasted_iota(jnp.int32, scores.shape, 0)
                    query_at = first + b * 128 + lax.broadcasted_iota(jnp.int32, scores.shape, 1)
                    allowed = key_at <= query_at
                    scores = jnp.where(allowed, scores, LOWEST)
                old = r.stat_m[h, :, at]
                new = jnp.maximum(old, jnp.max(scores, axis=0, keepdims=True))
                weights = jnp.exp2(scores - new)
                if diagonal:
                    weights = jnp.where(allowed, weights, 0.0)
                shrink = jnp.exp2(old - new)
                r.stat_m[h, :, at] = new
                r.stat_a[h, :, here] = shrink
                r.stat_l[h, :, at] = r.stat_l[h, :, at] * shrink + jnp.sum(
                    weights, axis=0, keepdims=True
                )
                r.weights[h, :, here] = weights.astype(BF16)
            at = pl.ds(first, count)
            r.acc[h, :, at] = r.acc[h, :, at] * r.stat_a[h, :, :count] + wide_dot(
                value, r.weights[h, :, :count]
            )

    def piece(slot):
        attend(keys_of(slot), 0, NX * rows, False)

    def diagonal_part(heads_here, k):
        attend(heads_here, pl.multiple_of(lax.rem(x + k, NX) * rows, rows), rows, True)

    def arrive(slot, forward_to, to):
        for chunk in range(CHUNKS):
            ring(0, slot, chunk, to).wait_recv()
            if forward_to is not None:
                ring(slot, forward_to, chunk, to).start()
            pair(slot, chunk, core).start()

    def use(slot, needed):
        for chunk in range(CHUNKS):
            pair(slot, chunk, 1 - core).wait_recv()

        @pl.when(needed)
        def _():
            piece(slot)

    def both(d):
        def one(i, carry):
            slot = jnp.where(i == 0, d, far + d)
            source = jnp.where(i == 0, z - d, z + d - nz)
            use(slot, source >= 0)
            return carry

        return one

    def hop_refs(of, way, part, z_from, z_to):
        if part == 1:
            return r.dnbuf.at[of], r.dnbuf.at[of]
        return r.gubuf.at[place(of, z_from)], r.gubuf.at[place(of, z_to)]

    def hop(d, way, part):
        of = lax.rem(z - (d - 1) + nz, nz) if way == 0 else lax.rem(z + d - 1, nz)
        to = up if way == 0 else down
        src, dst = hop_refs(of, way, part, z, to[0] // NX)
        return remote(src, dst, r.hop_send.at[d, way, part], r.hop_recv.at[d, way, part], to)

    def hop_in(d, way, part):
        of = lax.rem(z - d + nz, nz) if way == 0 else lax.rem(z + d, nz)
        to = up if way == 0 else down
        src, dst = hop_refs(of, way, part, z, z)
        return remote(src, dst, r.hop_send.at[d, way, part], r.hop_recv.at[d, way, part], to)

    def in_hop(d):
        return [(way, part) for part in range(2) for way in range(2) if d < far or way == part]

    def first_hop(k, way, part):
        to = up if way == 0 else down
        src, dst = hop_refs(z, way, part, z, to[0] // NX)
        block = lax.rem(x + k, NX)
        send, recv = r.first_send.at[k, way, part], r.first_recv.at[k, way, part]
        return remote(src.at[block], dst.at[block], send, recv, to)

    def first_in(k, way, part):
        to = up if way == 0 else down
        of = lax.rem(z + nz - 1, nz) if way == 0 else lax.rem(z + 1, nz)
        ref = hop_refs(of, way, part, z, z)[0].at[lax.rem(x + k, NX)]
        return remote(ref, ref, r.first_send.at[k, way, part], r.first_recv.at[k, way, part], to)

    def start_first(k):
        if k == 0:
            local[1].wait()
            local[3].wait()
        else:
            for copy in weight_copies(NX - k):
                copy.wait_recv()
        for way, part in in_hop(1):
            first_hop(k, way, part).start()

    def hop_on(d, only=None):
        for way, part in in_hop(d):
            if only is not None and part != only:
                continue
            if d == 1:
                for k in range(NX):
                    first_in(k, way, part).wait_recv()
            else:
                hop_in(d, way, part).wait_recv()
            if d < far and (way, part) in in_hop(d + 1):
                hop(d + 1, way, part).start()

    def hop_latent(d):
        arrive(d, d + 1 if d < far else None, up)
        if d < far:
            arrive(far + d, far + d + 1 if d < far - 1 else None, down)

    own_keys = keys_of(0)
    diagonal_part(own_keys, 0)
    hop_latent(1)
    gq.near(0)
    gq.near(1)
    for copy in weight_copies(2):
        copy.start()
    diagonal_part(own_keys, 3)
    diagonal_part(own_keys, 1)
    hop_latent(2)
    gq.far(0)
    gq.far(1)
    diagonal_part(own_keys, 2)
    if far > 2:
        lax.fori_loop(0, 2, both(1), 0)
        hop_latent(3)
    start_first(0)
    for d in range(2, far - 1):
        lax.fori_loop(0, 2, both(d), 0)
    start_first(1)
    start_first(3)
    if far > 3:
        hop_latent(4)
    lax.fori_loop(0, 2, both(far - 1), 0)
    use(far, z - far >= 0)
    start_first(2)

    for b in range(NX):
        at = pl.ds(b * rows, rows)
        for h in range(2):
            total = r.stat_l[h, :, at]
            inverse = jnp.where(total > 0.0, 1.0 / jnp.where(total > 0.0, total, 1.0), 0.0)
            r.osend[b, h * VDIM : (h + 1) * VDIM] = (r.acc[h, :, at] * inverse).astype(BF16)
            r.ssend[b, h : h + 1] = r.stat_m[h, :, at]
            r.ssend[b, 2 + h : 3 + h] = total

    def o_copy(k, h):
        to = lax.rem(x + k, NX)
        head = pl.ds(h * VDIM, VDIM)
        return remote(
            r.osend.at[to, head], r.orecv.at[k, head], r.o_send.at[k, h], r.o_recv.at[k, h], along_x(k)
        )

    def s_copy(k):
        to = lax.rem(x + k, NX)
        return remote(r.ssend.at[to], r.srecv.at[k], r.s_send.at[k], r.s_recv.at[k], along_x(k))

    for k in (2, 1, 3):
        s_copy(k).start()
    for h in range(2):
        for k in (2, 1, 3):
            o_copy(k, h).start()
    for k in range(1, NX):
        s_copy(k).wait_recv()
    width = 2 * VDIM
    stats = [r.ssend[x]] + [r.srecv[k] for k in range(1, NX)]

    def swap(piece, send, recv, index):
        k, half = ((0, None), (3, None), (1, None), (2, 0), (2, 1))[index]
        mine, theirs = piece(core)(k, half), piece(1 - core)(k, half)
        out = functools.partial(remote, mine, mine, send.at[index], recv.at[index], partner)
        come = functools.partial(remote, theirs, theirs, send.at[index], recv.at[index], partner)
        return out, come

    def att_piece(h, own_core):
        def ref(k, half):
            of = lax.rem(y + k, NY) * NC + own_core
            where = pl.ds(pl.multiple_of(of * width + h * VDIM, VDIM), VDIM)
            at = pl.ds(0, rows) if half is None else pl.ds(half * (rows // 2), rows // 2)
            return r.att.at[at, where]

        return ref

    heads = []
    for h in range(2):
        for k in range(1, NX):
            o_copy(k, h).wait_recv()
        outs = [r.osend[x, h * VDIM : (h + 1) * VDIM]] + [
            r.orecv[k, h * VDIM : (h + 1) * VDIM] for k in range(1, NX)
        ]
        top = functools.reduce(jnp.maximum, [s[h : h + 1] for s in stats])
        shares = [s[2 + h : 3 + h] * jnp.exp2(s[h : h + 1] - top) for s in stats]
        inverse = 1.0 / sum(shares)
        mixed = sum(o.astype(F32) * (w * inverse) for o, w in zip(outs, shares))
        at = pl.ds(pl.multiple_of(tp * width + h * VDIM, VDIM), VDIM)
        r.att[:, at] = jnp.transpose(mixed).astype(BF16)
        piece_of = functools.partial(att_piece, h)
        g = Gather4(piece_of(core), r.ga_send, r.ga_recv, h, along_y(1), along_y(3))
        swaps = [swap(piece_of, r.sa_send.at[h], r.sa_recv.at[h], i) for i in range(5)]
        g.start()
        swaps[0][0]().start()
        heads.append((g, swaps))
    hop_on(1, 0)
    for way in range(2):
        for g, swaps in heads:
            g.near(way)
            swaps[1 + way][0]().start()
    hop_on(1, 1)
    for half in range(2):
        for g, swaps in heads:
            g.far(half)
            swaps[3 + half][0]().start()
    for i in range(1, NT):
        ow_copy(i).wait_recv()
    local[4].wait()
    local[2].wait()
    for g, swaps in heads:
        for out, come in swaps:
            come().wait_recv()

    att = r.att[...]
    att_wide = att.astype(F32)
    scale = lax.rsqrt(jnp.mean(att_wide * att_wide, axis=1, keepdims=True) + EPSILON)
    attn_sum = wide_dot(att, r.owbuf[...].reshape(att.shape[1], cols)) * scale
    middle = (r.residbuf[...].astype(F32) + attn_sum).astype(BF16)
    r.mid[x, :, channels(tp)] = middle

    def sq_copy(i):
        ref = r.sq_part.at[tp]
        return remote(ref, ref, r.sq_send.at[i], r.sq_recv.at[i], along_y(i // 2, i % 2))

    def sx_copy(k):
        ref = r.sq_row.at[x]
        return remote(ref, ref, r.sx_send.at[k], r.sx_recv.at[k], along_x(k))

    def squares_start():
        wide = middle.astype(F32)
        squares = jnp.sum(wide * wide, axis=1, keepdims=True)
        r.sq_part[tp] = jnp.transpose(jnp.broadcast_to(squares, (rows, 128)))[:8]
        for i in range(1, NT):
            sq_copy(i).start()

    def squares_on():
        for i in range(1, NT):
            sq_copy(i).wait_recv()
        r.sq_row[x] = sum(r.sq_part[i] for i in range(NT))
        for k in range(1, NX):
            sx_copy(k).start()

    def squares_end():
        for k in range(1, NX):
            sx_copy(k).wait_recv()
        for b in range(NX):
            r.row_scale[b] = column(lax.rsqrt(r.sq_row[b, :1] / dim + EPSILON))


    def mid_piece(axis, at_x, at_y, own_core, first):
        def ref(k, half):
            of_x = lax.rem(x + at_x + (k if axis == 0 else 0), NX)
            of_y = lax.rem(y + at_y + (k if axis == 1 else 0), NY)
            where = channels(of_y * NC + own_core)
            quarter = rows // 4
            at = pl.ds(first * 2 * quarter, 2 * quarter)
            if half is not None:
                at = pl.ds((first * 2 + half) * quarter, quarter)
            return r.mid.at[of_x, at, where]

        return ref

    def plane_ring(index, axis, at_x, at_y, first):
        piece_of = functools.partial(lambda c: mid_piece(axis, at_x, at_y, c, first))
        plus, minus = (along_x(1), along_x(3)) if axis == 0 else (along_y(1), along_y(3))
        g = Gather4(piece_of(core), r.gm_send, r.gm_recv, index, plus, minus)
        return g, [swap(piece_of, r.sm_send.at[index], r.sm_recv.at[index], i) for i in range(5)]

    offsets = (0, 3, 1, 2)
    first_rings = [plane_ring(0, 0, 0, 0, 0), plane_ring(1, 1, 0, 0, 1)]
    second_rings = [
        [plane_ring(2 + i, 1, k, 0, 0), plane_ring(6 + i, 0, 0, k, 1)] for i, k in enumerate(offsets)
    ]
    for g, s in first_rings:
        g.start()
        s[0][0]().start()
    for g, s in second_rings[0]:
        g.start()
    squares_start()
    for way in range(2):
        for i, (g, s) in enumerate(first_rings):
            g.near(way)
            second_rings[1 + way][i][0].start()
            s[1 + way][0]().start()
    hop_on(2, 0)
    for way in range(2):
        for g, s in second_rings[0]:
            g.near(way)
            s[1 + way][0]().start()
    hop_on(2, 1)
    squares_on()
    for i, (g, s) in enumerate(first_rings):
        for half in range(2):
            g.far(half)
            s[3 + half][0]().start()
        second_rings[3][i][0].start()
    for j in range(1, 4):
        for way in range(2):
            for g, s in second_rings[j]:
                g.near(way)
                s[1 + way][0]().start()
        for half in range(2):
            for g, s in second_rings[j - 1]:
                g.far(half)
                s[3 + half][0]().start()
        if j == 1 and far > 3:
            hop_on(3, 0)
        if j == 2 and far > 3:
            hop_on(3, 1)
    for half in range(2):
        for g, s in second_rings[3]:
            g.far(half)
            s[3 + half][0]().start()
    rings = first_rings + [pair_of for both_of in second_rings for pair_of in both_of]
    for i, (g, s) in enumerate(rings):
        for j, (out, come) in enumerate(s):
            if j > 0 or i < 2:
                come().wait_recv()

    def ahead(j):
        return jnp.where(j == 0, 2, jnp.where(j == 1, 1, jnp.where(j == 2, 3, 0)))

    def early(j, carry):
        b = lax.rem(x + ahead(j), NX)

        r.gu_sum[b] = wide_dot(r.mid[b, :, cols:], r.gubuf[1:].reshape(dim - cols, 2 * UNIT))
        return carry

    squares_end()
    lax.fori_loop(0, EARLY, early, 0)
    hop_on(far)

    def mixer(j):
        b = lax.rem(x + ahead(j), NX)

        @pl.when(j < EARLY)
        def _():
            r.gu_sum[b] += wide_dot(r.mid[b, :, :cols], r.gubuf[0].reshape(cols, 2 * UNIT))

        @pl.when(j >= EARLY)
        def _():
            r.gu_sum[b] = wide_dot(r.mid[b], r.gubuf[...].reshape(dim, 2 * UNIT))

        gu = r.gu_sum[b]
        gu = gu * r.row_scale[b]
        gate, mixed_tile, upward = gu[:, :128], gu[:, 128:256], gu[:, 256:]
        first = gate / (1.0 + jnp.exp(-gate)) * upward
        second = (mixed_tile / (1.0 + jnp.exp(-mixed_tile)))[:, :64] * mixed_tile[:, 64:]
        hidden = jnp.concatenate([first, second], axis=1).astype(BF16)
        n = r.dnbuf.shape[-1]
        for zz in range(nz):
            w = jnp.concatenate([r.dnbuf[zz, i] for i in range(NX)], axis=1)
            terms = wide_dot(hidden, w).astype(BF16).reshape(NY, NC, share, NX * n)
            for c in range(NC):
                r.part[c, b, :, :, zz * NX * n : (zz + 1) * NX * n] = terms[:, c]
        core_copy(j).start()

    def core_copy(j):
        b = lax.rem(x + ahead(j), NX)
        return remote(r.part.at[1 - core, b], r.pairbuf.at[b], r.pc_send.at[j], r.pc_recv.at[j], partner)

    def core_sum(j):
        b = lax.rem(x + ahead(j), NX)
        core_copy(j).wait_recv()
        for i in range(NY):
            ref = r.part.at[core, b, i]
            ref[...] = (ref[...].astype(F32) + r.pairbuf[b, i].astype(F32)).astype(BF16)

    depth = r.part.shape[-1] // 2

    def block(axis, of_x, of_y, first):
        def ref(k, half):
            bx = lax.rem(of_x + (k if axis == 0 else 0), NX)
            by = lax.rem(of_y + (k if axis == 1 else 0), NY)
            at = pl.ds(first * depth, depth)
            if half is not None:
                at = pl.ds(first * depth + half * (depth // 2), depth // 2)
            return r.part.at[core, bx, by, :, at]

        return ref

    def scatter(index, axis, of_x, of_y, first):
        plus, minus = (along_x(1), along_x(3)) if axis == 0 else (along_y(1), along_y(3))
        return Scatter4(
            block(axis, of_x, of_y, first),
            r.half_in.at[index],
            r.whole_in.at[index],
            r.rs_send,
            r.rs_recv,
            index,
            plus,
            minus,
        )

    def first_along_y(j):
        return scatter(j, 1, x + ahead(j), y, 0)

    def first_along_x(j):
        return scatter(4 + j, 0, x, y + ahead(j), 1)

    def stage(j, carry):
        mixer(j)

        @pl.when(j >= 1)
        def _():
            core_sum(j - 1)
            first_along_y(j - 1).start()

        @pl.when(j == 1)
        def _():
            for i in range(NY):
                first_along_x(i).start()

        return carry

    lax.fori_loop(0, NX, stage, 0)
    steps = [[first_along_y(j), first_along_x(j)] for j in range(NX)]
    ends = [scatter(8, 0, x, y, 0), scatter(9, 1, x, y, 1)]
    for h in range(2):
        first_along_x(0).near(h)
        first_along_y(0).near(h)
    core_sum(NX - 1)
    first_along_y(NX - 1).start()
    for j in range(1, NX - 1):
        for h in range(2):
            first_along_x(j).near(h)
            first_along_y(j).near(h)
    for both_of, s in zip(steps[0], ends, strict=True):
        both_of.finish()
        s.start()
    for h in range(2):
        first_along_x(NX - 1).near(h)
        first_along_y(NX - 1).near(h)
    for j in range(1, NX):
        for both_of, s in zip(steps[j], ends, strict=True):
            both_of.finish()
            if j < NX - 1:
                s.near(1 if j == 1 else 0)
    own_rows = pl.ds(pl.multiple_of(tp * share, share), share)
    for first, s in enumerate(ends):
        at = slice(first * depth, (first + 1) * depth)
        r.out[:, at] = s.total()

    for t in range(NT):
        r.middle[:, t * cols : (t + 1) * cols] = r.mid[x, own_rows, channels(t)]

    for k in range(1, NX):
        for h in range(2):
            o_copy(k, h).wait_send()
        s_copy(k).wait_send()
        for copy in weight_copies(k):
            copy.wait_send()
    for i in range(1, NT):
        ow_copy(i).wait_send()
    for slot in range(1, nz):
        for chunk in range(CHUNKS):
            ring(0, slot, chunk, up).wait_send()
            pair(slot, chunk, core).wait_send()
    for way, part in in_hop(1):
        for k in range(NX):
            first_hop(k, way, part).wait_send()
    for d in range(2, far + 1):
        for way, part in in_hop(d):
            hop(d, way, part).wait_send()
    gq.done()
    for g, swaps in heads:
        g.done()
        for out, come in swaps:
            out().wait_send()
    for i, (g, s) in enumerate(rings):
        g.done()
        for j, (out, come) in enumerate(s):
            if j > 0 or i < 2:
                out().wait_send()
    for i in range(1, NT):
        sq_copy(i).wait_send()
    for k in range(1, NX):
        sx_copy(k).wait_send()
    for j in range(NX):
        core_copy(j).wait_send()
    for both_of in [*steps, ends]:
        for s in both_of:
            s.done()


def layer(inputs, whole):
    nz = lax.axis_size("sp") // NX
    vmem = pl.BlockSpec(memory_space=pltpu.VMEM)
    anywhere = pl.BlockSpec(memory_space=pl.ANY)
    rows, wide = inputs["latent"].shape
    depth = inputs["gate"].shape[0]
    n = inputs["dn"].shape[-1]
    dim = inputs["resid"].shape[1]
    share = rows // NT
    cols = dim // NT
    lat = (NC, CHUNKS, rows // NC // CHUNKS, wide + 2 * ROPE)
    gu, dn = (NX, depth, 2 * UNIT), (NX, UNIT, n)
    heads = 2 * VDIM
    buffers = {
        "latbuf": ((nz, *lat), BF16),
        "qbuf": ((2 * (NOPE + ROPE), NX * rows), BF16),
        "scores": ((2, rows, NX * rows), F32),
        "weights": ((2, rows, NX * rows), BF16),
        "stat_a": ((2, 1, NX * rows), F32),
        "wk": ((wide, 2 * NOPE), BF16),
        "wv": ((heads, wide), BF16),
        "gustage": (gu, BF16),
        "owstage": ((heads, dim), BF16),
        "acc": ((2, VDIM, NX * rows), F32),
        "stat_m": ((2, 1, NX * rows), F32),
        "stat_l": ((2, 1, NX * rows), F32),
        "osend": ((NX, 2 * VDIM, rows), BF16),
        "orecv": ((NX, 2 * VDIM, rows), BF16),
        "ssend": ((NX, 8, rows), F32),
        "srecv": ((NX, 8, rows), F32),
        "gubuf": ((nz, *gu), BF16),
        "dnbuf": ((nz, *dn), BF16),
        "owbuf": ((NT, heads, cols), BF16),
        "residbuf": ((rows, cols), BF16),
        "att": ((rows, NT * 2 * VDIM), BF16),
        "mid": ((NX, rows, dim), BF16),
        "part": ((NC, NX, NY, share, dim), BF16),
        "row_scale": ((NX, rows, 1), F32),
        "gu_sum": ((NX, rows, 2 * UNIT), F32),
        "sq_part": ((NT, 8, rows), F32),
        "sq_row": ((NX, 8, rows), F32),
        "pairbuf": ((NX, NY, share, dim), BF16),
        "half_in": ((10, 2, share, dim // 4), BF16),
        "whole_in": ((10, 2, share, dim // 2), BF16),
    }
    semaphores = {
        "local_sem": (5,),
        "ring_send": (nz, CHUNKS),
        "ring_recv": (nz, CHUNKS),
        "pair_send": (nz, CHUNKS),
        "pair_recv": (nz, CHUNKS),
        "gq_send": (1, 4),
        "gq_recv": (1, 4),
        "wx_send": (NX, 2),
        "wx_recv": (NX, 2),
        "ow_send": (NT,),
        "ow_recv": (NT,),
        "first_send": (NX, 2, 2),
        "first_recv": (NX, 2, 2),
        "hop_send": (nz, 2, 2),
        "hop_recv": (nz, 2, 2),
        "o_send": (NX, 2),
        "o_recv": (NX, 2),
        "s_send": (NX,),
        "s_recv": (NX,),
        "ga_send": (2, 4),
        "ga_recv": (2, 4),
        "sa_send": (2, 5),
        "sa_recv": (2, 5),
        "gm_send": (10, 4),
        "gm_recv": (10, 4),
        "sm_send": (10, 5),
        "sm_recv": (10, 5),
        "sq_send": (NT,),
        "sq_recv": (NT,),
        "sx_send": (NX,),
        "sx_recv": (NX,),
        "pc_send": (NX,),
        "pc_recv": (NX,),
        "rs_send": (10, 4),
        "rs_recv": (10, 4),
    }
    names = [*inputs, "out", "middle", *buffers, *semaphores]
    return pl.pallas_call(
        functools.partial(layer_kernel, nz, names),
        out_shape=(
            jax.ShapeDtypeStruct((share, dim), F32),
            jax.ShapeDtypeStruct((share, dim), BF16),
        ),
        in_specs=[anywhere if name in whole else vmem for name in inputs],
        out_specs=(vmem, vmem),
        scratch_shapes=[pltpu.VMEM(*b) for b in buffers.values()]
        + [pltpu.SemaphoreType.DMA(s) for s in semaphores.values()],
        compiler_params=pltpu.CompilerParams(
            collective_id=0, has_side_effects=True, vmem_limit_bytes=62 * 1024 * 1024
        ),
    )(*inputs.values())


def body(
    resid,
    queries,
    latent,
    rope_key,
    lat_gain,
    kv_weight,
    out_gain,
    out_weight,
    ffn_gain,
    gate_weight,
    up_weight,
    down_weight,
):
    rows = latent.shape[0]
    half = ROPE // 2
    frequency = THETA ** (-np.arange(half) / half)

    def turns(places):
        angle = places[:, None] * frequency
        return jnp.asarray(np.concatenate([np.cos(angle), np.sin(angle)], axis=1), F32)

    inputs = {
        "latent": latent,
        "rope_key": rope_key.T,
        "queries": queries,
        "lat_gain": lat_gain[None, :],
        "kv_weight": kv_weight,
        "gate": gate_weight,
        "upward": up_weight,
        "ffn_gain": ffn_gain.reshape(-1, gate_weight.shape[0]),
        "out_gain": out_gain[None, :],
        "first_turn": turns(np.arange(lax.axis_size("sp")) * rows),
        "row_turn": turns(np.arange(rows)),
        "dn": down_weight.reshape(NX, UNIT, down_weight.shape[1]),
        "ow": out_weight,
        "resid": resid,
    }
    ffn_sum, middle = layer(inputs, ("dn", "ow", "resid"))
    return (middle.astype(F32) + ffn_sum).astype(BF16)


def solution(mesh):
    placed = (
        P("sp", None),
        P("sp", "tp"),
        P("sp", None),
        P("sp", None),
        P(),
        P(None, "tp"),
        P("tp"),
        P("tp", None),
        P(),
        P("sp", "tp"),
        P("sp", "tp"),
        P("tp", "sp"),
    )
    return jax.shard_map(
        body, mesh=mesh, in_specs=placed, out_specs=P(("sp", "tp"), None), check_vma=False
    )
```

```python
import functools
import math

import jax
import jax.numpy as jnp
import numpy as np
from jax import lax
from jax.experimental import pallas as pl
from jax.experimental.pallas import tpu as pltpu
from jax.sharding import PartitionSpec as P

NOPE = 128
ROPE = 64
VDIM = 128
NX = 4
NY = 4
NC = 2
NT = NY * NC
CHUNKS = 4
EARLY = 1
UNIT = 192

EPSILON = 1e-06
THETA = 10000.0
LOWEST = -1e30
MESH = pl.DeviceIdType.MESH
F32 = jnp.float32
BF16 = jnp.bfloat16


def norm_rows(values, gain):
    wide = values.astype(F32)
    return wide * lax.rsqrt(jnp.mean(wide * wide, axis=-1, keepdims=True) + EPSILON) * gain


def column(row):
    return jnp.transpose(jnp.broadcast_to(row, (128, row.shape[1])))[:, :1]


def turned(values, cosine, sine):
    half = values.shape[-1] // 2
    first, second = values[:, :half], values[:, half:]
    return jnp.concatenate(
        [first * cosine - second * sine, first * sine + second * cosine], axis=1
    )


def nt_dot(a, b):
    return lax.dot_general(a, b, (((1,), (1,)), ((), ())), preferred_element_type=F32)


def wide_dot(a, b):
    return jnp.dot(a, b, preferred_element_type=F32)


class Refs:
    def __init__(self, names, values):
        self.__dict__.update(zip(names, values, strict=True))


def remote(src, dst, send, recv, to):
    return pltpu.make_async_remote_copy(
        src_ref=src, dst_ref=dst, send_sem=send, recv_sem=recv, device_id=to, device_id_type=MESH
    )


class Gather4:
    def __init__(self, piece, send, recv, index, plus, minus):
        self.piece, self.send, self.recv, self.index = piece, send, recv, index
        self.plus, self.minus = plus, minus

    def copy(self, way, k, half):
        to = self.plus if way in (0, 2) else self.minus
        ref = self.piece(k, half)
        return remote(ref, ref, self.send.at[self.index, way], self.recv.at[self.index, way], to)

    def start(self):
        self.copy(0, 0, None).start()
        self.copy(1, 0, None).start()

    def near(self, way):
        self.copy(way, 3 if way == 0 else 1, None).wait_recv()
        self.copy(way + 2, 3 if way == 0 else 1, way).start()

    def far(self, half):
        self.copy(half + 2, 2, half).wait_recv()

    def done(self):
        self.copy(0, 0, None).wait_send()
        self.copy(1, 0, None).wait_send()
        self.copy(2, 3, 0).wait_send()
        self.copy(3, 1, 1).wait_send()


class Scatter4:
    def __init__(self, block, half_in, whole_in, send, recv, index, plus, minus):
        self.block, self.half_in, self.whole_in = block, half_in, whole_in
        self.send, self.recv, self.index = send, recv, index
        self.plus, self.minus = plus, minus

    def half(self, h):
        to = self.minus if h == 0 else self.plus
        return remote(
            self.block(2, h), self.half_in.at[h], self.send.at[self.index, h], self.recv.at[self.index, h], to
        )

    def whole(self, h):
        to, k = (self.minus, 3) if h == 0 else (self.plus, 1)
        return remote(
            self.block(k, None),
            self.whole_in.at[h],
            self.send.at[self.index, 2 + h],
            self.recv.at[self.index, 2 + h],
            to,
        )

    def start(self):
        self.half(0).start()
        self.half(1).start()

    def near(self, h):
        self.half(h).wait_recv()
        ref = self.block(3 if h == 0 else 1, h)
        ref[...] = (ref[...].astype(F32) + self.half_in[h].astype(F32)).astype(BF16)
        self.whole(h).start()

    def total(self):
        self.whole(0).wait_recv()
        self.whole(1).wait_recv()
        ref = self.block(0, None)
        return ref[...].astype(F32) + self.whole_in[0].astype(F32) + self.whole_in[1].astype(F32)

    def finish(self):
        self.block(0, None)[...] = self.total().astype(BF16)

    def done(self):
        for h in range(2):
            self.half(h).wait_send()
            self.whole(h).wait_send()


def layer_kernel(nz, names, *values):
    r = Refs(names, values)
    sp, tp = lax.axis_index("sp"), lax.axis_index("tp")
    z, x = sp // NX, lax.rem(sp, NX)
    y, core = tp // NC, lax.rem(tp, NC)
    up = (lax.rem(z + 1, nz) * NX + x, tp)
    down = (lax.rem(z + nz - 1, nz) * NX + x, tp)
    partner = (sp, tp + 1 - 2 * core)
    rows = r.latent.shape[0]
    far = nz // 2
    factor = (1.0 / math.sqrt(NOPE + ROPE)) * math.log2(math.e)
    dim = r.resid.shape[1]
    cols = dim // NT
    share = rows // NT

    def along_x(k):
        return (z * NX + lax.rem(x + k, NX), tp)

    def along_y(k, other=0):
        to_core = core if other == 0 else 1 - core
        return (sp, lax.rem(y + k, NY) * NC + to_core)

    peers = [up, down, partner]
    peers += [along_x(k) for k in range(1, NX)]
    peers += [along_y(k) for k in range(1, NY)]
    peers += [along_y(k, 1) for k in range(1, NY)]
    barrier = pltpu.get_barrier_semaphore()
    for peer in peers:
        pl.semaphore_signal(barrier, inc=1, device_id=peer, device_id_type=MESH)

    own_cols = pl.ds(pl.multiple_of(tp * cols, cols), cols)

    def place(t, at_z):
        return lax.rem(t - at_z + far + nz, nz)

    def channels(t):
        return pl.ds(pl.multiple_of(place(t, z) * cols, cols), cols)

    local = [
        pltpu.make_async_copy(r.ow, r.owstage, r.local_sem.at[0]),
        pltpu.make_async_copy(r.dn.at[x], r.dnbuf.at[z, x], r.local_sem.at[1]),
        pltpu.make_async_copy(r.resid.at[:, own_cols], r.residbuf, r.local_sem.at[2]),
        pltpu.make_async_copy(r.gustage.at[x], r.gubuf.at[far, x], r.local_sem.at[3]),
        pltpu.make_async_copy(r.owstage.at[:, own_cols], r.owbuf.at[tp], r.local_sem.at[4]),
        pltpu.make_async_copy(r.gate, r.gate_here, r.local_sem.at[5]),
        pltpu.make_async_copy(r.upward, r.up_here, r.local_sem.at[6]),
        pltpu.make_async_copy(r.kv_weight, r.kv_here, r.local_sem.at[7]),
    ]
    for copy in local[5:] + local[:3]:
        copy.start()

    half = ROPE // 2
    base, step = r.first_turn[pl.ds(sp, 1), :], r.row_turn[...]
    base_cos, base_sin = base[:, :half], base[:, half:]
    step_cos, step_sin = step[:, :half], step[:, half:]
    cosine = base_cos * step_cos - base_sin * step_sin
    sine = base_sin * step_cos + base_cos * step_sin
    key_rot = turned(jnp.transpose(r.rope_key[...].astype(F32)), cosine, sine)
    lat = jnp.concatenate([norm_rows(r.latent[...], r.lat_gain[...]), key_rot, key_rot], axis=1)
    r.latbuf[0] = lat.astype(BF16).reshape(r.latbuf.shape[1:])
    query = r.queries[...].astype(F32)
    one = NOPE + ROPE
    parts = [query[:, h * one : h * one + NOPE] for h in range(2)]
    parts += [turned(query[:, h * one + NOPE : (h + 1) * one], cosine, sine) for h in range(2)]
    own_rows_at = pl.ds(pl.multiple_of(x * rows, rows), rows)
    r.qbuf[:, own_rows_at] = jnp.transpose(jnp.concatenate(parts, axis=1)).astype(BF16)
    pl.semaphore_wait(barrier, len(peers))

    def ring(src_slot, dst_slot, chunk, to):
        src = r.latbuf.at[src_slot, core, chunk]
        dst = r.latbuf.at[dst_slot, core, chunk]
        return remote(src, dst, r.ring_send.at[dst_slot, chunk], r.ring_recv.at[dst_slot, chunk], to)

    def pair(slot, chunk, side):
        ref = r.latbuf.at[slot, side, chunk]
        return remote(ref, ref, r.pair_send.at[slot, chunk], r.pair_recv.at[slot, chunk], partner)

    def q_piece(k, half):
        channels = r.qbuf.shape[0]
        at = pl.ds(0, channels) if half is None else pl.ds(half * (channels // 2), channels // 2)
        return r.qbuf.at[at, pl.ds(pl.multiple_of(lax.rem(x + k, NX) * rows, rows), rows)]

    gq = Gather4(q_piece, r.gq_send, r.gq_recv, 0, along_x(1), along_x(3))

    def weight_copies(k):
        to = lax.rem(x + k, NX)
        return [
            remote(r.gustage.at[to], r.gubuf.at[far, x], r.wx_send.at[k, 0], r.wx_recv.at[k, 0], along_x(k)),
            remote(r.dn.at[to], r.dnbuf.at[z, x], r.wx_send.at[k, 1], r.wx_recv.at[k, 1], along_x(k)),
        ]

    def ow_copy(i):
        k, other = i // 2, i % 2
        to = along_y(k, other)
        src = r.owstage.at[:, pl.ds(pl.multiple_of(to[1] * cols, cols), cols)]
        return remote(src, r.owbuf.at[tp], r.ow_send.at[i], r.ow_recv.at[i], to)

    for chunk in range(CHUNKS):
        ring(0, 1, chunk, up).start()
        ring(0, far + 1, chunk, down).start()
    gq.start()

    gain = column(r.ffn_gain[pl.ds(sp, 1), :])
    for copy in local[5:]:
        copy.wait()
    gate, upward = r.gate_here[...].astype(F32) * gain, r.up_here[...].astype(F32) * gain
    for i in range(NX):
        lo, mid_lo, hi = i * UNIT, i * UNIT + 128, (i + 1) * UNIT
        tiles = [gate[:, lo:mid_lo], gate[:, mid_lo:hi], upward[:, mid_lo:hi], upward[:, lo:mid_lo]]
        r.gustage[i] = jnp.concatenate(tiles, axis=1).astype(BF16)
    local[3].start()
    for k in (1, 3):
        for copy in weight_copies(k):
            copy.start()
    for h in range(2):
        at = 2 * h * NOPE
        r.wk[:, h * NOPE : (h + 1) * NOPE] = r.kv_here[:, at : at + NOPE]
        value_weight = r.kv_here[:, at + NOPE : at + NOPE + VDIM].astype(F32)
        r.wv[h * VDIM : (h + 1) * VDIM, :] = jnp.transpose(value_weight).astype(BF16)
    local[0].wait()
    gain = column(r.out_gain[...])

    def scale_ow(j, carry):
        at = pl.ds(pl.multiple_of(j * cols, cols), cols)
        r.owstage[:, at] = (r.owstage[:, at].astype(F32) * gain).astype(BF16)
        return carry

    lax.fori_loop(0, NT, scale_ow, 0)
    local[4].start()
    for i in range(1, NT):
        ow_copy(i).start()

    r.stat_m[...] = jnp.full(r.stat_m.shape, LOWEST, F32)
    r.stat_l[...] = jnp.zeros(r.stat_l.shape, F32)
    r.acc[...] = jnp.zeros(r.acc.shape, F32)

    def keys_of(slot):
        lat = r.latbuf[slot].reshape(rows, r.latbuf.shape[-1])
        wide = r.wk.shape[0]
        compressed, both_rot = lat[:, :wide], lat[:, wide:]
        lane = lax.broadcasted_iota(jnp.int32, both_rot.shape, 1)
        keys = wide_dot(compressed, r.wk[...]).astype(BF16)
        values = nt_dot(r.wv[...], compressed).astype(BF16)
        out = []
        for h in range(2):
            own_half = lane < ROPE if h == 0 else lane >= ROPE
            key_rot = jnp.where(own_half, both_rot.astype(F32), 0.0).astype(BF16)
            key = jnp.concatenate([keys[:, h * NOPE : (h + 1) * NOPE], key_rot], axis=1)
            out.append((key, values[h * VDIM : (h + 1) * VDIM]))
        return out

    def attend(heads_here, first, count, diagonal):
        for h, (key, _) in enumerate(heads_here):
            at = pl.ds(first, count)
            query = jnp.concatenate(
                [r.qbuf[h * NOPE : (h + 1) * NOPE, at], r.qbuf[2 * NOPE :, at]], axis=0
            )
            r.scores[h, :, :count] = wide_dot(key, query)
        for h, (_, value) in enumerate(heads_here):
            for b in range(count // 128):
                here = pl.ds(b * 128, 128)
                at = pl.ds(first + b * 128, 128)
                if not isinstance(first, int):
                    at = pl.ds(pl.multiple_of(first + b * 128, 128), 128)
                scores = r.scores[h, :, here] * factor
                if diagonal:
                    key_at = x * rows + lax.broadcasted_iota(jnp.int32, scores.shape, 0)
                    query_at = first + b * 128 + lax.broadcasted_iota(jnp.int32, scores.shape, 1)
                    allowed = key_at <= query_at
                    scores = jnp.where(allowed, scores, LOWEST)
                old = r.stat_m[h, :, at]
                new = jnp.maximum(old, jnp.max(scores, axis=0, keepdims=True))
                weights = jnp.exp2(scores - new)
                if diagonal:
                    weights = jnp.where(allowed, weights, 0.0)
                shrink = jnp.exp2(old - new)
                r.stat_m[h, :, at] = new
                r.stat_a[h, :, here] = shrink
                r.stat_l[h, :, at] = r.stat_l[h, :, at] * shrink + jnp.sum(
                    weights, axis=0, keepdims=True
                )
                r.weights[h, :, here] = weights.astype(BF16)
            at = pl.ds(first, count)
            r.acc[h, :, at] = r.acc[h, :, at] * r.stat_a[h, :, :count] + wide_dot(
                value, r.weights[h, :, :count]
            )

    def piece(slot):
        attend(keys_of(slot), 0, NX * rows, False)

    def diagonal_part(heads_here, k):
        attend(heads_here, pl.multiple_of(lax.rem(x + k, NX) * rows, rows), rows, True)

    def arrive(slot, forward_to, to):
        for chunk in range(CHUNKS):
            ring(0, slot, chunk, to).wait_recv()
            if forward_to is not None:
                ring(slot, forward_to, chunk, to).start()
            pair(slot, chunk, core).start()

    def use(slot, needed):
        for chunk in range(CHUNKS):
            pair(slot, chunk, 1 - core).wait_recv()

        @pl.when(needed)
        def _():
            piece(slot)

    def both(d):
        def one(i, carry):
            slot = jnp.where(i == 0, d, far + d)
            source = jnp.where(i == 0, z - d, z + d - nz)
            use(slot, source >= 0)
            return carry

        return one

    def hop_refs(of, way, part, z_from, z_to):
        if part == 1:
            return r.dnbuf.at[of], r.dnbuf.at[of]
        return r.gubuf.at[place(of, z_from)], r.gubuf.at[place(of, z_to)]

    def hop(d, way, part):
        of = lax.rem(z - (d - 1) + nz, nz) if way == 0 else lax.rem(z + d - 1, nz)
        to = up if way == 0 else down
        src, dst = hop_refs(of, way, part, z, to[0] // NX)
        return remote(src, dst, r.hop_send.at[d, way, part], r.hop_recv.at[d, way, part], to)

    def hop_in(d, way, part):
        of = lax.rem(z - d + nz, nz) if way == 0 else lax.rem(z + d, nz)
        to = up if way == 0 else down
        src, dst = hop_refs(of, way, part, z, z)
        return remote(src, dst, r.hop_send.at[d, way, part], r.hop_recv.at[d, way, part], to)

    def in_hop(d):
        return [(way, part) for part in range(2) for way in range(2) if d < far or way == part]

    def first_hop(k, way, part):
        to = up if way == 0 else down
        src, dst = hop_refs(z, way, part, z, to[0] // NX)
        block = lax.rem(x + k, NX)
        send, recv = r.first_send.at[k, way, part], r.first_recv.at[k, way, part]
        return remote(src.at[block], dst.at[block], send, recv, to)

    def first_in(k, way, part):
        to = up if way == 0 else down
        of = lax.rem(z + nz - 1, nz) if way == 0 else lax.rem(z + 1, nz)
        ref = hop_refs(of, way, part, z, z)[0].at[lax.rem(x + k, NX)]
        return remote(ref, ref, r.first_send.at[k, way, part], r.first_recv.at[k, way, part], to)

    def start_first(k):
        if k == 0:
            local[1].wait()
            local[3].wait()
        else:
            for copy in weight_copies(NX - k):
                copy.wait_recv()
        for way, part in in_hop(1):
            first_hop(k, way, part).start()

    def hop_on(d, only=None):
        for way, part in in_hop(d):
            if only is not None and part != only:
                continue
            if d == 1:
                for k in range(NX):
                    first_in(k, way, part).wait_recv()
            else:
                hop_in(d, way, part).wait_recv()
            if d < far and (way, part) in in_hop(d + 1):
                hop(d + 1, way, part).start()

    def hop_latent(d):
        arrive(d, d + 1 if d < far else None, up)
        if d < far:
            arrive(far + d, far + d + 1 if d < far - 1 else None, down)

    own_keys = keys_of(0)
    diagonal_part(own_keys, 0)
    hop_latent(1)
    gq.near(0)
    gq.near(1)
    for copy in weight_copies(2):
        copy.start()
    diagonal_part(own_keys, 3)
    diagonal_part(own_keys, 1)
    hop_latent(2)
    gq.far(0)
    gq.far(1)
    diagonal_part(own_keys, 2)
    if far > 2:
        lax.fori_loop(0, 2, both(1), 0)
        hop_latent(3)
    start_first(0)
    for d in range(2, far - 1):
        lax.fori_loop(0, 2, both(d), 0)
    start_first(1)
    start_first(3)
    if far > 3:
        hop_latent(4)
    lax.fori_loop(0, 2, both(far - 1), 0)
    use(far, z - far >= 0)
    start_first(2)

    for b in range(NX):
        at = pl.ds(b * rows, rows)
        for h in range(2):
            total = r.stat_l[h, :, at]
            inverse = jnp.where(total > 0.0, 1.0 / jnp.where(total > 0.0, total, 1.0), 0.0)
            r.osend[b, h * VDIM : (h + 1) * VDIM] = (r.acc[h, :, at] * inverse).astype(BF16)
            r.ssend[b, h : h + 1] = r.stat_m[h, :, at]
            r.ssend[b, 2 + h : 3 + h] = total

    def o_copy(k, h):
        to = lax.rem(x + k, NX)
        head = pl.ds(h * VDIM, VDIM)
        return remote(
            r.osend.at[to, head], r.orecv.at[k, head], r.o_send.at[k, h], r.o_recv.at[k, h], along_x(k)
        )

    def s_copy(k):
        to = lax.rem(x + k, NX)
        return remote(r.ssend.at[to], r.srecv.at[k], r.s_send.at[k], r.s_recv.at[k], along_x(k))

    for k in (2, 1, 3):
        s_copy(k).start()
    for h in range(2):
        for k in (2, 1, 3):
            o_copy(k, h).start()
    for k in range(1, NX):
        s_copy(k).wait_recv()
    width = 2 * VDIM
    stats = [r.ssend[x]] + [r.srecv[k] for k in range(1, NX)]

    def swap(piece, send, recv, index):
        k, half = ((0, None), (3, None), (1, None), (2, 0), (2, 1))[index]
        mine, theirs = piece(core)(k, half), piece(1 - core)(k, half)
        out = functools.partial(remote, mine, mine, send.at[index], recv.at[index], partner)
        come = functools.partial(remote, theirs, theirs, send.at[index], recv.at[index], partner)
        return out, come

    def att_piece(h, own_core):
        def ref(k, half):
            of = lax.rem(y + k, NY) * NC + own_core
            where = pl.ds(pl.multiple_of(of * width + h * VDIM, VDIM), VDIM)
            at = pl.ds(0, rows) if half is None else pl.ds(half * (rows // 2), rows // 2)
            return r.att.at[at, where]

        return ref

    heads = []
    for h in range(2):
        for k in range(1, NX):
            o_copy(k, h).wait_recv()
        outs = [r.osend[x, h * VDIM : (h + 1) * VDIM]] + [
            r.orecv[k, h * VDIM : (h + 1) * VDIM] for k in range(1, NX)
        ]
        top = functools.reduce(jnp.maximum, [s[h : h + 1] for s in stats])
        shares = [s[2 + h : 3 + h] * jnp.exp2(s[h : h + 1] - top) for s in stats]
        inverse = 1.0 / sum(shares)
        mixed = sum(o.astype(F32) * (w * inverse) for o, w in zip(outs, shares))
        at = pl.ds(pl.multiple_of(tp * width + h * VDIM, VDIM), VDIM)
        r.att[:, at] = jnp.transpose(mixed).astype(BF16)
        piece_of = functools.partial(att_piece, h)
        g = Gather4(piece_of(core), r.ga_send, r.ga_recv, h, along_y(1), along_y(3))
        swaps = [swap(piece_of, r.sa_send.at[h], r.sa_recv.at[h], i) for i in range(5)]
        g.start()
        swaps[0][0]().start()
        heads.append((g, swaps))
    hop_on(1, 0)
    for way in range(2):
        for g, swaps in heads:
            g.near(way)
            swaps[1 + way][0]().start()
    hop_on(1, 1)
    for half in range(2):
        for g, swaps in heads:
            g.far(half)
            swaps[3 + half][0]().start()
    for i in range(1, NT):
        ow_copy(i).wait_recv()
    local[4].wait()
    local[2].wait()
    for g, swaps in heads:
        for out, come in swaps:
            come().wait_recv()

    att = r.att[...]
    att_wide = att.astype(F32)
    scale = lax.rsqrt(jnp.mean(att_wide * att_wide, axis=1, keepdims=True) + EPSILON)
    attn_sum = wide_dot(att, r.owbuf[...].reshape(att.shape[1], cols)) * scale
    middle = (r.residbuf[...].astype(F32) + attn_sum).astype(BF16)
    r.mid[x, :, channels(tp)] = middle

    def sq_copy(i):
        ref = r.sq_part.at[tp]
        return remote(ref, ref, r.sq_send.at[i], r.sq_recv.at[i], along_y(i // 2, i % 2))

    def sx_copy(k):
        ref = r.sq_row.at[x]
        return remote(ref, ref, r.sx_send.at[k], r.sx_recv.at[k], along_x(k))

    def squares_start():
        wide = middle.astype(F32)
        squares = jnp.sum(wide * wide, axis=1, keepdims=True)
        r.sq_part[tp] = jnp.transpose(jnp.broadcast_to(squares, (rows, 128)))[:8]
        for i in range(1, NT):
            sq_copy(i).start()

    def squares_on():
        for i in range(1, NT):
            sq_copy(i).wait_recv()
        r.sq_row[x] = sum(r.sq_part[i] for i in range(NT))
        for k in range(1, NX):
            sx_copy(k).start()

    def squares_end():
        for k in range(1, NX):
            sx_copy(k).wait_recv()
        for b in range(NX):
            r.row_scale[b] = column(lax.rsqrt(r.sq_row[b, :1] / dim + EPSILON))


    def mid_piece(axis, at_x, at_y, own_core, first):
        def ref(k, half):
            of_x = lax.rem(x + at_x + (k if axis == 0 else 0), NX)
            of_y = lax.rem(y + at_y + (k if axis == 1 else 0), NY)
            where = channels(of_y * NC + own_core)
            quarter = rows // 4
            at = pl.ds(first * 2 * quarter, 2 * quarter)
            if half is not None:
                at = pl.ds((first * 2 + half) * quarter, quarter)
            return r.mid.at[of_x, at, where]

        return ref

    def plane_ring(index, axis, at_x, at_y, first):
        piece_of = functools.partial(lambda c: mid_piece(axis, at_x, at_y, c, first))
        plus, minus = (along_x(1), along_x(3)) if axis == 0 else (along_y(1), along_y(3))
        g = Gather4(piece_of(core), r.gm_send, r.gm_recv, index, plus, minus)
        return g, [swap(piece_of, r.sm_send.at[index], r.sm_recv.at[index], i) for i in range(5)]

    offsets = (0, 3, 1, 2)
    first_rings = [plane_ring(0, 0, 0, 0, 0), plane_ring(1, 1, 0, 0, 1)]
    second_rings = [
        [plane_ring(2 + i, 1, k, 0, 0), plane_ring(6 + i, 0, 0, k, 1)] for i, k in enumerate(offsets)
    ]
    for g, s in first_rings:
        g.start()
        s[0][0]().start()
    for g, s in second_rings[0]:
        g.start()
    squares_start()
    for way in range(2):
        for i, (g, s) in enumerate(first_rings):
            g.near(way)
            second_rings[1 + way][i][0].start()
            s[1 + way][0]().start()
    hop_on(2, 0)
    for way in range(2):
        for g, s in second_rings[0]:
            g.near(way)
            s[1 + way][0]().start()
    hop_on(2, 1)
    squares_on()
    for i, (g, s) in enumerate(first_rings):
        for half in range(2):
            g.far(half)
            s[3 + half][0]().start()
        second_rings[3][i][0].start()
    for j in range(1, 4):
        for way in range(2):
            for g, s in second_rings[j]:
                g.near(way)
                s[1 + way][0]().start()
        for half in range(2):
            for g, s in second_rings[j - 1]:
                g.far(half)
                s[3 + half][0]().start()
        if j == 1 and far > 3:
            hop_on(3, 0)
        if j == 2 and far > 3:
            hop_on(3, 1)
    for half in range(2):
        for g, s in second_rings[3]:
            g.far(half)
            s[3 + half][0]().start()
    rings = first_rings + [pair_of for both_of in second_rings for pair_of in both_of]
    for i, (g, s) in enumerate(rings):
        for j, (out, come) in enumerate(s):
            if j > 0 or i < 2:
                come().wait_recv()

    def ahead(j):
        return jnp.where(j == 0, 2, jnp.where(j == 1, 1, jnp.where(j == 2, 3, 0)))

    def early(j, carry):
        b = lax.rem(x + ahead(j), NX)

        r.gu_sum[b] = wide_dot(r.mid[b, :, cols:], r.gubuf[1:].reshape(dim - cols, 2 * UNIT))
        return carry

    squares_end()
    lax.fori_loop(0, EARLY, early, 0)
    hop_on(far)

    def mixer(j):
        b = lax.rem(x + ahead(j), NX)

        @pl.when(j < EARLY)
        def _():
            r.gu_sum[b] += wide_dot(r.mid[b, :, :cols], r.gubuf[0].reshape(cols, 2 * UNIT))

        @pl.when(j >= EARLY)
        def _():
            r.gu_sum[b] = wide_dot(r.mid[b], r.gubuf[...].reshape(dim, 2 * UNIT))

        gu = r.gu_sum[b]
        gu = gu * r.row_scale[b]
        gate, mixed_tile, upward = gu[:, :128], gu[:, 128:256], gu[:, 256:]
        first = gate / (1.0 + jnp.exp(-gate)) * upward
        second = (mixed_tile / (1.0 + jnp.exp(-mixed_tile)))[:, :64] * mixed_tile[:, 64:]
        hidden = jnp.concatenate([first, second], axis=1).astype(BF16)
        n = r.dnbuf.shape[-1]
        for zz in range(nz):
            w = jnp.concatenate([r.dnbuf[zz, i] for i in range(NX)], axis=1)
            terms = wide_dot(hidden, w).astype(BF16).reshape(NY, NC, share, NX * n)
            for c in range(NC):
                r.part[c, b, :, :, zz * NX * n : (zz + 1) * NX * n] = terms[:, c]
        core_copy(j).start()

    def core_copy(j):
        b = lax.rem(x + ahead(j), NX)
        return remote(r.part.at[1 - core, b], r.pairbuf.at[b], r.pc_send.at[j], r.pc_recv.at[j], partner)

    def core_sum(j):
        b = lax.rem(x + ahead(j), NX)
        core_copy(j).wait_recv()
        for i in range(NY):
            ref = r.part.at[core, b, i]
            ref[...] = (ref[...].astype(F32) + r.pairbuf[b, i].astype(F32)).astype(BF16)

    depth = r.part.shape[-1] // 2

    def block(axis, of_x, of_y, first):
        def ref(k, half):
            bx = lax.rem(of_x + (k if axis == 0 else 0), NX)
            by = lax.rem(of_y + (k if axis == 1 else 0), NY)
            at = pl.ds(first * depth, depth)
            if half is not None:
                at = pl.ds(first * depth + half * (depth // 2), depth // 2)
            return r.part.at[core, bx, by, :, at]

        return ref

    def scatter(index, axis, of_x, of_y, first):
        plus, minus = (along_x(1), along_x(3)) if axis == 0 else (along_y(1), along_y(3))
        return Scatter4(
            block(axis, of_x, of_y, first),
            r.half_in.at[index],
            r.whole_in.at[index],
            r.rs_send,
            r.rs_recv,
            index,
            plus,
            minus,
        )

    def first_along_y(j):
        return scatter(j, 1, x + ahead(j), y, 0)

    def first_along_x(j):
        return scatter(4 + j, 0, x, y + ahead(j), 1)

    def stage(j, carry):
        mixer(j)

        @pl.when(j >= 1)
        def _():
            core_sum(j - 1)
            first_along_y(j - 1).start()

        @pl.when(j == 1)
        def _():
            for i in range(NY):
                first_along_x(i).start()

        return carry

    lax.fori_loop(0, NX, stage, 0)
    steps = [[first_along_y(j), first_along_x(j)] for j in range(NX)]
    ends = [scatter(8, 0, x, y, 0), scatter(9, 1, x, y, 1)]
    for h in range(2):
        first_along_x(0).near(h)
        first_along_y(0).near(h)
    core_sum(NX - 1)
    first_along_y(NX - 1).start()
    for j in range(1, NX - 1):
        for h in range(2):
            first_along_x(j).near(h)
            first_along_y(j).near(h)
    for both_of, s in zip(steps[0], ends, strict=True):
        both_of.finish()
        s.start()
    for h in range(2):
        first_along_x(NX - 1).near(h)
        first_along_y(NX - 1).near(h)
    for j in range(1, NX):
        for both_of, s in zip(steps[j], ends, strict=True):
            both_of.finish()
            if j < NX - 1:
                s.near(1 if j == 1 else 0)
    own_rows = pl.ds(pl.multiple_of(tp * share, share), share)
    for first, s in enumerate(ends):
        at = slice(first * depth, (first + 1) * depth)
        r.out[:, at] = s.total()

    for t in range(NT):
        r.middle[:, t * cols : (t + 1) * cols] = r.mid[x, own_rows, channels(t)]

    for k in range(1, NX):
        for h in range(2):
            o_copy(k, h).wait_send()
        s_copy(k).wait_send()
        for copy in weight_copies(k):
            copy.wait_send()
    for i in range(1, NT):
        ow_copy(i).wait_send()
    for slot in range(1, nz):
        for chunk in range(CHUNKS):
            ring(0, slot, chunk, up).wait_send()
            pair(slot, chunk, core).wait_send()
    for way, part in in_hop(1):
        for k in range(NX):
            first_hop(k, way, part).wait_send()
    for d in range(2, far + 1):
        for way, part in in_hop(d):
            hop(d, way, part).wait_send()
    gq.done()
    for g, swaps in heads:
        g.done()
        for out, come in swaps:
            out().wait_send()
    for i, (g, s) in enumerate(rings):
        g.done()
        for j, (out, come) in enumerate(s):
            if j > 0 or i < 2:
                out().wait_send()
    for i in range(1, NT):
        sq_copy(i).wait_send()
    for k in range(1, NX):
        sx_copy(k).wait_send()
    for j in range(NX):
        core_copy(j).wait_send()
    for both_of in [*steps, ends]:
        for s in both_of:
            s.done()


def layer(inputs, whole):
    nz = lax.axis_size("sp") // NX
    vmem = pl.BlockSpec(memory_space=pltpu.VMEM)
    anywhere = pl.BlockSpec(memory_space=pl.ANY)
    rows, wide = inputs["latent"].shape
    depth = inputs["gate"].shape[0]
    n = inputs["dn"].shape[-1]
    dim = inputs["resid"].shape[1]
    share = rows // NT
    cols = dim // NT
    lat = (NC, CHUNKS, rows // NC // CHUNKS, wide + 2 * ROPE)
    gu, dn = (NX, depth, 2 * UNIT), (NX, UNIT, n)
    heads = 2 * VDIM
    buffers = {
        "latbuf": ((nz, *lat), BF16),
        "qbuf": ((2 * (NOPE + ROPE), NX * rows), BF16),
        "scores": ((2, rows, NX * rows), F32),
        "weights": ((2, rows, NX * rows), BF16),
        "stat_a": ((2, 1, NX * rows), F32),
        "wk": ((wide, 2 * NOPE), BF16),
        "wv": ((heads, wide), BF16),
        "gate_here": (inputs["gate"].shape, BF16),
        "up_here": (inputs["upward"].shape, BF16),
        "kv_here": (inputs["kv_weight"].shape, BF16),
        "gustage": (gu, BF16),
        "owstage": ((heads, dim), BF16),
        "acc": ((2, VDIM, NX * rows), F32),
        "stat_m": ((2, 1, NX * rows), F32),
        "stat_l": ((2, 1, NX * rows), F32),
        "osend": ((NX, 2 * VDIM, rows), BF16),
        "orecv": ((NX, 2 * VDIM, rows), BF16),
        "ssend": ((NX, 8, rows), F32),
        "srecv": ((NX, 8, rows), F32),
        "gubuf": ((nz, *gu), BF16),
        "dnbuf": ((nz, *dn), BF16),
        "owbuf": ((NT, heads, cols), BF16),
        "residbuf": ((rows, cols), BF16),
        "att": ((rows, NT * 2 * VDIM), BF16),
        "mid": ((NX, rows, dim), BF16),
        "part": ((NC, NX, NY, share, dim), BF16),
        "row_scale": ((NX, rows, 1), F32),
        "gu_sum": ((NX, rows, 2 * UNIT), F32),
        "sq_part": ((NT, 8, rows), F32),
        "sq_row": ((NX, 8, rows), F32),
        "pairbuf": ((NX, NY, share, dim), BF16),
        "half_in": ((10, 2, share, dim // 4), BF16),
        "whole_in": ((10, 2, share, dim // 2), BF16),
    }
    semaphores = {
        "local_sem": (8,),
        "ring_send": (nz, CHUNKS),
        "ring_recv": (nz, CHUNKS),
        "pair_send": (nz, CHUNKS),
        "pair_recv": (nz, CHUNKS),
        "gq_send": (1, 4),
        "gq_recv": (1, 4),
        "wx_send": (NX, 2),
        "wx_recv": (NX, 2),
        "ow_send": (NT,),
        "ow_recv": (NT,),
        "first_send": (NX, 2, 2),
        "first_recv": (NX, 2, 2),
        "hop_send": (nz, 2, 2),
        "hop_recv": (nz, 2, 2),
        "o_send": (NX, 2),
        "o_recv": (NX, 2),
        "s_send": (NX,),
        "s_recv": (NX,),
        "ga_send": (2, 4),
        "ga_recv": (2, 4),
        "sa_send": (2, 5),
        "sa_recv": (2, 5),
        "gm_send": (10, 4),
        "gm_recv": (10, 4),
        "sm_send": (10, 5),
        "sm_recv": (10, 5),
        "sq_send": (NT,),
        "sq_recv": (NT,),
        "sx_send": (NX,),
        "sx_recv": (NX,),
        "pc_send": (NX,),
        "pc_recv": (NX,),
        "rs_send": (10, 4),
        "rs_recv": (10, 4),
    }
    names = [*inputs, "out", "middle", *buffers, *semaphores]
    return pl.pallas_call(
        functools.partial(layer_kernel, nz, names),
        out_shape=(
            jax.ShapeDtypeStruct((share, dim), F32),
            jax.ShapeDtypeStruct((share, dim), BF16),
        ),
        in_specs=[anywhere if name in whole else vmem for name in inputs],
        out_specs=(vmem, vmem),
        scratch_shapes=[pltpu.VMEM(*b) for b in buffers.values()]
        + [pltpu.SemaphoreType.DMA(s) for s in semaphores.values()],
        compiler_params=pltpu.CompilerParams(
            collective_id=0, has_side_effects=True, vmem_limit_bytes=62 * 1024 * 1024
        ),
    )(*inputs.values())


def body(
    resid,
    queries,
    latent,
    rope_key,
    lat_gain,
    kv_weight,
    out_gain,
    out_weight,
    ffn_gain,
    gate_weight,
    up_weight,
    down_weight,
):
    rows = latent.shape[0]
    half = ROPE // 2
    frequency = THETA ** (-np.arange(half) / half)

    def turns(places):
        angle = places[:, None] * frequency
        return jnp.asarray(np.concatenate([np.cos(angle), np.sin(angle)], axis=1), F32)

    inputs = {
        "latent": latent,
        "rope_key": rope_key.T,
        "queries": queries,
        "lat_gain": lat_gain[None, :],
        "kv_weight": kv_weight,
        "gate": gate_weight,
        "upward": up_weight,
        "ffn_gain": ffn_gain.reshape(-1, gate_weight.shape[0]),
        "out_gain": out_gain[None, :],
        "first_turn": turns(np.arange(lax.axis_size("sp")) * rows),
        "row_turn": turns(np.arange(rows)),
        "dn": down_weight.reshape(NX, UNIT, down_weight.shape[1]),
        "ow": out_weight,
        "resid": resid,
    }
    ffn_sum, middle = layer(inputs, ("dn", "ow", "resid", "gate", "upward", "kv_weight"))
    return (middle.astype(F32) + ffn_sum).astype(BF16)


def solution(mesh):
    placed = (
        P("sp", None),
        P("sp", "tp"),
        P("sp", None),
        P("sp", None),
        P(),
        P(None, "tp"),
        P("tp"),
        P("tp", None),
        P(),
        P("sp", "tp"),
        P("sp", "tp"),
        P("tp", "sp"),
    )
    return jax.shard_map(
        body, mesh=mesh, in_specs=placed, out_specs=P(("sp", "tp"), None), check_vma=False
    )
```
